128 devices in a mesh: rep: 2 (over x_hi), fs: 4 (over x_lo, core), tp: 16 (over z, y).
Axes of the slice: x: 4 (x_hi: 2, x_lo: 2; x = x_hi * 2 + x_lo), y: 4, z: 4, core: 2. Of those that a mesh axis runs over, the one named last changes fastest.
Arguments:
- inputs: bfloat16 [4096, 4096], P(('rep', 'fs', 'tp')), may hold values from -6 to 6
- w_gate: bfloat16 [4096, 11008], P('fs', 'tp'), may hold values from -0.09375 to 0.09375
- w_up: bfloat16 [4096, 11008], P('fs', 'tp'), may hold values from -0.09375 to 0.09375
- w_down: bfloat16 [11008, 4096], P('tp', 'fs'), may hold values from -0.0546875 to 0.0546875
- d_out: bfloat16 [4096, 4096], P(('rep', 'fs', 'tp')), may hold values from -24 to 24
Outputs:
- grad_inputs: bfloat16 [4096, 4096], P(('rep', 'fs', 'tp'))
- grad_gate: float32 [4096, 11008], P('fs', 'tp')
- grad_up: float32 [4096, 11008], P('fs', 'tp')
- grad_down: float32 [11008, 4096], P('tp', 'fs')
The draws below stay inside these ranges and needn't reach their ends.
All inputs are finite; a program needn't handle non-finite values.
Results may differ from the reference program's by a relative error of at most 0.00185.
Values may be sent and summed in bfloat16 or wider, within the bound.
No kernel may reach another device: no remote copies, remote signals or barrier semaphores. Data moves between devices by JAX's collectives and lax.ppermute only.
A program may use at most 192 MiB of HBM per device.

```python
import jax
import jax.numpy as jnp
from jax import lax

D = 4096
FF = 11008
TOKENS = 4096


def raised(array, key, source, target, shards_of, factor):
    owner, partner = [(jnp.arange(array.shape[dim]) // (array.shape[dim] // shards_of)).reshape([-1 if axis == dim else 1 for axis in range(array.ndim)]) for dim in (source, target)]
    chosen = jax.random.permutation(key, shards_of)[partner]
    strong = (owner == chosen) | (owner == (partner + shards_of // 2) % shards_of)
    return jnp.where(strong, factor * array, array)


def shard_levels(key, extent, split, least, top_value):
    factor_of, own = 1.0, jax.random.fold_in(key, 6)
    for dim, blocks in split:
        heights = jnp.exp(jax.random.uniform(jax.random.fold_in(own, dim), (blocks,), jnp.float32, least / len(split), top_value / len(split)))
        factor_of = factor_of * jnp.repeat(heights, extent[dim] // blocks).reshape([-1 if axis == dim else 1 for axis in range(len(extent))])
    return factor_of


def centred(stream_key, dims, deviation, reach, pieces=(), kind=jnp.bfloat16):
    array = jax.random.normal(stream_key, dims, jnp.float32) * deviation
    if len(pieces) > 0:
        array = shard_levels(stream_key, dims, pieces, -0.22, 0.18) * array
    return jnp.clip(array, min=-reach, max=reach).astype(kind)


def bell_draw_with(key, extent, scale, reach, pieces, heavy, kind=jnp.bfloat16):
    drawn = scale * jax.random.normal(key, extent, jnp.float32)
    if pieces:
        drawn = drawn * shard_levels(key, extent, pieces, -0.22, 0.18)
    return jnp.clip(raised(drawn, jax.random.fold_in(key, 3), *heavy), -reach, reach).astype(kind)


def setup_inputs(seed: int = 0) -> dict:
    seeds = jax.random.split(jax.random.key(seed), 6)
    inputs = centred(seeds[0], (TOKENS, D), 1.0, 6.0, ((0, 128),))
    w_gate = centred(seeds[1], (D, FF), D ** -0.5, 0.09375, ((0, 4), (1, 16)))
    w_up = centred(seeds[2], (D, FF), D ** -0.5, 0.09375, ((0, 4), (1, 16)))
    w_down = centred(seeds[3], (FF, D), FF ** -0.5, 0.0546875, ((0, 16), (1, 4)))
    d_out = bell_draw_with(seeds[4], (TOKENS, D), 1.0, 24.0, ((0, 128),), (0, 1, 128, 5.5))
    return dict(inputs=inputs, w_gate=w_gate, w_up=w_up, w_down=w_down, d_out=d_out)


def stored(values):
    return lax.optimization_barrier(values.astype(jnp.bfloat16)).astype(jnp.float32)


def reference(inputs, w_gate, w_up, w_down, d_out):
    gate_val = stored(jnp.dot(inputs, w_gate, preferred_element_type=jnp.float32))
    up_val = stored(jnp.dot(inputs, w_up, preferred_element_type=jnp.float32))
    back_val = stored(jnp.dot(d_out, w_down.T, preferred_element_type=jnp.float32))
    sigma = jax.nn.sigmoid(gate_val)
    active = gate_val * sigma
    hidden = (active * up_val).astype(jnp.bfloat16)
    d_gate = (back_val * up_val * sigma * (1.0 + gate_val * (1.0 - sigma))).astype(jnp.bfloat16)
    d_up = (back_val * active).astype(jnp.bfloat16)
    grad_inputs = jnp.dot(d_gate, w_gate.T, preferred_element_type=jnp.float32)
    grad_inputs = grad_inputs + jnp.dot(d_up, w_up.T, preferred_element_type=jnp.float32)
    grad_inputs = grad_inputs.astype(jnp.bfloat16)
    grad_gate = jnp.dot(inputs.T, d_gate, preferred_element_type=jnp.float32)
    grad_up = jnp.dot(inputs.T, d_up, preferred_element_type=jnp.float32)
    grad_down = jnp.dot(hidden.T, d_out, preferred_element_type=jnp.float32)
    return grad_inputs, grad_gate, grad_up, grad_down
```

```python
import jax
import jax.numpy as jnp
from jax import lax
from jax.sharding import PartitionSpec as P


AXES = ("rep", "fs", "tp")
BF, F32, F16 = jnp.bfloat16, jnp.float32, jnp.float16
W_MAX = 0.09375


def index_of(x, c, z, y):
    x, z, y = x % 4, z % 4, y % 4
    return (x // 2) * 64 + ((x % 2) * 2 + c) * 16 + z * 4 + y


def moved(array, dx=0, flip=0, dz=0, dy=0):
    pairs = []
    for x in range(4):
        for c in range(2):
            for z in range(4):
                for y in range(4):
                    pairs.append((index_of(x + dx, c ^ flip, z + dz, y + dy), index_of(x, c, z, y)))
    return lax.ppermute(array, AXES, pairs)


def dot(a, b, ca, cb):
    return lax.dot_general(a, b, (((ca,), (cb,)), ((), ())), preferred_element_type=F32)


def block(inputs, w_gate, w_up, w_down, d_out):
    fs, tp = lax.axis_index("fs"), lax.axis_index("tp")
    z, y = tp // 4, tp % 4
    rows, width = inputs.shape
    depth, units = w_gate.shape
    tokens = rows * 16

    def relative(a):
        parts = [a[:, i * depth:(i + 1) * depth] for i in range(4)]
        out = []
        for k in range(4):
            v = parts[k]
            for f in range(1, 4):
                v = jnp.where(fs == f, parts[f ^ k], v)
            out.append(v)
        return jnp.concatenate(out, axis=1)

    x_own, d_own = relative(inputs), relative(d_out)

    wg, wu = w_gate.T, w_up.T
    half = units // 2
    wa = jnp.concatenate([wg, w_down[:half]], axis=0)
    wb = jnp.concatenate([wu, w_down[half:]], axis=0)
    wa2, wb2 = moved(wa, dx=1), moved(wb, dx=-1)

    xz = jnp.concatenate([x_own] + [moved(x_own, dz=d) for d in (1, 2, 3)], axis=0)
    dy_ = jnp.concatenate([d_own] + [moved(d_own, dy=d) for d in (1, 2, 3)], axis=0)
    wa1, wb1 = moved(wa, flip=1), moved(wb, flip=1)
    xq = [xz] + [moved(xz, dy=d) for d in (1, 2, 3)]
    dq = [dy_] + [moved(dy_, dz=d) for d in (1, 2, 3)]
    wa3, wb3 = moved(wa2, flip=1), moved(wb2, flip=1)

    def lane(a):
        return jnp.stack([a[:, :depth], a[:, 2 * depth:3 * depth]])
    def cross(a):
        return jnp.stack([a[:, depth:2 * depth], a[:, 3 * depth:]])
    mine = jnp.stack([lane(x_own), lane(d_own)], axis=1)
    sib = moved(jnp.stack([cross(x_own), cross(d_own)], axis=1), flip=1)
    both = jnp.stack([mine, sib], axis=2)
    near, far = both[1], both[0]
    got = jnp.stack([moved(near, dx=1), moved(near, dx=-1), moved(far, dx=2)])
    cols = lax.all_gather(got.reshape(12, rows, depth), "tp", axis=0)

    x_all = jnp.concatenate([xq[b][a * rows:(a + 1) * rows] for a in range(4) for b in range(4)], axis=0)
    d_all = jnp.concatenate(dq, axis=0)
    sib_cols = moved(jnp.stack([x_all[:, depth:2 * depth], d_all[:, depth:2 * depth]]), flip=1)

    was, wbs = (wa, wa1, wa2, wa3), (wb, wb1, wb2, wb3)
    gate = up = back_a = back_b = 0.0
    for k in range(4):
        xk, dk = x_all[:, k * depth:(k + 1) * depth], d_all[:, k * depth:(k + 1) * depth]
        gate = gate + dot(was[k][:units], xk, 1, 1)
        up = up + dot(wbs[k][:units], xk, 1, 1)
        back_a = back_a + dot(was[k][units:], dk, 1, 1)
        back_b = back_b + dot(wbs[k][units:], dk, 1, 1)

    def stored(v):
        return lax.reduce_precision(v, 8, 7)

    gate, up, back = stored(gate), stored(up), stored(jnp.concatenate([back_a, back_b], axis=0))
    sigma = jax.nn.sigmoid(gate)
    active = gate * sigma
    hidden = (active * up).astype(BF)
    d_gate = (back * up * sigma * (1.0 + gate * (1.0 - sigma))).astype(BF)
    d_up = (back * active).astype(BF)
    acts = jnp.concatenate([d_gate, d_up, hidden], axis=0)

    r = lax.broadcasted_iota(jnp.int32, (tokens, tokens), 0)
    a = lax.broadcasted_iota(jnp.int32, (tokens, tokens), 1)
    target = ((z + r // (4 * rows)) % 4) * (4 * rows) + ((y + (r // rows) % 4) % 4) * rows + r % rows
    order = (a == target).astype(BF)
    acts_t = dot(acts, order, 1, 0).astype(BF)

    am, ap = moved(acts_t, dx=1), moved(acts_t, dx=-1)
    acts_s = moved(acts, flip=1)
    h3 = 3 * units // 2
    oa, ob = moved(am[:h3], dx=1), moved(ap[h3:], dx=-1)
    sm, sp = moved(am, flip=1), moved(ap, flip=1)
    soa, sob = moved(oa, flip=1), moved(ob, flip=1)
    ao, so = jnp.concatenate([oa, ob], axis=0), jnp.concatenate([soa, sob], axis=0)

    norm = jnp.sum(jnp.abs(acts[:2 * units].astype(F32)), axis=0) * (1.02 * W_MAX)
    expo = jnp.ceil(jnp.log2(jnp.maximum(norm, 1e-30)))[:, None]
    scale = jnp.exp2(14.0 - expo)
    g = [dot(d_gate, was[k][:units], 0, 0) + dot(d_up, wbs[k][:units], 0, 0) for k in range(4)]
    ga, gb = jnp.concatenate(g[:2], axis=1), jnp.concatenate(g[2:], axis=1)
    wide = ga.shape[1]
    tail = jnp.broadcast_to(expo, (tokens, 128))

    def packed(v):
        v = jnp.concatenate([v * scale, tail], axis=1).astype(F16)
        return v.reshape(4, 4, rows, wide + 128)

    def unpacked(v):
        v = v.astype(F32)
        return v[..., :wide] * jnp.exp2(v[..., wide:wide + 1] - 14.0)

    qa, qb = packed(ga), packed(gb)
    acc_a = ga.reshape(4, 4, rows, wide)[0]
    acc_b = gb.reshape(4, 4, rows, wide)[:, 0]
    ra = [moved(qa[d], dz=-d) for d in (1, 2, 3)]
    rb = [moved(qb[:, d], dy=-d) for d in (1, 2, 3)]
    acc_a = acc_a + unpacked(ra[0]) + unpacked(ra[1]) + unpacked(ra[2])
    acc_b = acc_b + unpacked(rb[0]) + unpacked(rb[1]) + unpacked(rb[2])
    fa = acc_a[0] + moved(acc_a[1], dy=-1) + moved(acc_a[2], dy=-2) + moved(acc_a[3], dy=-3)
    fb = acc_b[0] + moved(acc_b[1], dz=-1) + moved(acc_b[2], dz=-2) + moved(acc_b[3], dz=-3)
    grad_inputs = relative(jnp.concatenate([fa, fb], axis=1).astype(BF))

    def col(g, arr, ln):
        return cols[:, (g * 2 + arr) * 2 + ln].reshape(tokens, depth)

    near_acts = [acts, acts_s]
    near_x = [x_all[:, :depth], sib_cols[0]]
    near_d = [d_all[:, :depth], sib_cols[1]]
    mid_acts = [am, sm, ap, sp]
    mid_x = [col(0, 0, 0), col(0, 0, 1), col(1, 0, 0), col(1, 0, 1)]
    mid_d = [col(0, 1, 0), col(0, 1, 1), col(1, 1, 0), col(1, 1, 1)]
    far_acts = [ao, so]
    far_x = [col(2, 0, 0), col(2, 0, 1)]
    far_d = [col(2, 1, 0), col(2, 1, 1)]
    gu = gd = 0.0
    for al, xl, dl in ((near_acts, near_x, near_d), (mid_acts, mid_x, mid_d), (far_acts, far_x, far_d)):
        av = jnp.concatenate(al, axis=1)
        gu = gu + dot(av[:2 * units], jnp.concatenate(xl, axis=0), 1, 0)
        gd = gd + dot(av[2 * units:], jnp.concatenate(dl, axis=0), 1, 0)
    return grad_inputs, gu[:units].T, gu[units:].T, gd


def solution(mesh):
    tok = P(AXES, None)
    return jax.shard_map(
        block,
        mesh=mesh,
        in_specs=(tok, P("fs", "tp"), P("fs", "tp"), P("tp", "fs"), tok),
        out_specs=(tok, P("fs", "tp"), P("fs", "tp"), P("tp", "fs")),
        check_vma=False,
    )
```

```python
import functools

import jax
import jax.numpy as jnp
from jax import lax
from jax.experimental import pallas as pl
from jax.experimental.pallas import tpu as pltpu
from jax.sharding import PartitionSpec as P


AXES = ("rep", "fs", "tp")
BF, F32, F16 = jnp.bfloat16, jnp.float32, jnp.float16
W_MAX = 0.09375
ANY = pl.BlockSpec(memory_space=pl.ANY)
VMEM = pl.BlockSpec(memory_space=pltpu.VMEM)
LIMIT = 56 * 1024 * 1024

ROWS, DEPTH, UNITS = 32, 1024, 688
TOK, WIDE = 16 * ROWS, 4 * DEPTH
CUT = 336
LOW = 1040
HALF = 2 * DEPTH
TAIL = 128


def index_of(x, c, z, y):
    x, z, y = x % 4, z % 4, y % 4
    return (x // 2) * 64 + ((x % 2) * 2 + c) * 16 + z * 4 + y


def moved(array, dx=0, flip=0, dz=0, dy=0):
    pairs = []
    for x in range(4):
        for c in range(2):
            for z in range(4):
                for y in range(4):
                    pairs.append((index_of(x + dx, c ^ flip, z + dz, y + dy), index_of(x, c, z, y)))
    return lax.ppermute(array, AXES, pairs)


def dot(a, b, ca, cb):
    return lax.dot_general(a, b, (((ca,), (cb,)), ((), ())), preferred_element_type=F32)


def place():
    tp = lax.axis_index("tp")
    return tp // 4, tp % 4


def call(body, out_shape, scratch, flops, ins, outs, args, nbytes):
    return pl.pallas_call(
        body,
        out_shape=out_shape,
        in_specs=ins,
        out_specs=outs,
        scratch_shapes=scratch,
        compiler_params=pltpu.CompilerParams(vmem_limit_bytes=LIMIT),
        cost_estimate=pl.CostEstimate(flops=flops, bytes_accessed=nbytes, transcendentals=0),
    )(*args)


X_FROM = ((0, 0, 4, 0), (1, 0, 4, 1), (2, 0, 4, 3), (3, 0, 2, 2), (4, 2, 2, 2))


def forward_kernel(*refs):
    xs, ds, was, wbs = refs[:5], refs[5:10], refs[10:14], refs[14:18]
    acts, x_own, d_own, side = refs[18:22]
    x, d, wa, wb, gate, up, back, sx, sd, sw, so = refs[22:]
    z, y = place()
    x_copies, d_copies = [], []
    n = 0
    for i, first, count, off in X_FROM:
        for j in range(count):
            zz = lax.rem(z + first + j, 4)
            yy = lax.rem(y + off, 4)
            row = pl.multiple_of((zz * 4 + yy) * ROWS, ROWS)
            x_copies.append(pltpu.make_async_copy(xs[i].at[pl.ds(j * ROWS, ROWS)], x.at[pl.ds(row, ROWS)], sx.at[n]))
            zz = lax.rem(z + off, 4)
            yy = lax.rem(y + first + j, 4)
            row = pl.multiple_of((zz * 4 + yy) * ROWS, ROWS)
            d_copies.append(pltpu.make_async_copy(ds[i].at[pl.ds(j * ROWS, ROWS)], d.at[pl.ds(row, ROWS)], sd.at[n]))
            n += 1
    w_copies = [
        (pltpu.make_async_copy(was[k], wa.at[k], sw.at[2 * k]), pltpu.make_async_copy(wbs[k], wb.at[k], sw.at[2 * k + 1]))
        for k in range(4)
    ]
    for c in x_copies:
        c.start()
    for c in w_copies[0]:
        c.start()
    for c in d_copies:
        c.start()
    for k in range(1, 4):
        for c in w_copies[k]:
            c.start()
    for c in x_copies + d_copies:
        c.wait()
    outs = [
        pltpu.make_async_copy(x.at[:, pl.ds(0, DEPTH)], x_own, so.at[0]),
        pltpu.make_async_copy(d.at[:, pl.ds(0, DEPTH)], d_own, so.at[1]),
        pltpu.make_async_copy(x.at[:, pl.ds(DEPTH, DEPTH)], side.at[0], so.at[2]),
        pltpu.make_async_copy(d.at[:, pl.ds(DEPTH, DEPTH)], side.at[1], so.at[3]),
    ]
    for c in outs:
        c.start()
    for k in range(4):
        for c in w_copies[k]:
            c.wait()

        def tile(j, _):
            t = pl.ds(pl.multiple_of(j * 256, 256), 256)
            xk, dk = x[t, k * DEPTH:(k + 1) * DEPTH], d[t, k * DEPTH:(k + 1) * DEPTH]
            for into, rows, w, v in (
                (gate, slice(0, UNITS), wa[k, :UNITS], xk),
                (up, slice(0, UNITS), wb[k, :UNITS], xk),
                (back, slice(0, CUT), wa[k, UNITS:], dk),
                (back, slice(CUT, UNITS), wb[k, UNITS:], dk),
            ):
                part = dot(w, v, 1, 1)
                into[rows, t] = part if k == 0 else into[rows, t] + part
            return 0

        lax.fori_loop(0, 2, tile, 0)

    def act(i, _):
        r = pl.ds(pl.multiple_of(i * 16, 16), 16)
        g = gate[r, :].astype(BF).astype(F32)
        u = up[r, :].astype(BF).astype(F32)
        b = back[r, :].astype(BF).astype(F32)
        sigma = 1.0 / (1.0 + jnp.exp(-g))
        active = g * sigma
        acts[pl.ds(pl.multiple_of(i * 16, 16), 16), :] = (b * u * sigma * (1.0 + g * (1.0 - sigma))).astype(BF)
        acts[pl.ds(pl.multiple_of(UNITS + i * 16, 16), 16), :] = (b * active).astype(BF)
        acts[pl.ds(pl.multiple_of(2 * UNITS + i * 16, 16), 16), :] = (active * u).astype(BF)
        return 0

    lax.fori_loop(0, UNITS // 16, act, 0)
    for c in outs:
        c.wait()


def forward(xs, ds, was, wbs):
    shape = jax.ShapeDtypeStruct
    return call(
        forward_kernel,
        (shape((3 * UNITS, TOK), BF), shape((TOK, DEPTH), BF), shape((TOK, DEPTH), BF), shape((2, TOK, DEPTH), BF)),
        [
            pltpu.VMEM((TOK, WIDE), BF), pltpu.VMEM((TOK, WIDE), BF),
            pltpu.VMEM((4, UNITS + CUT, DEPTH), BF), pltpu.VMEM((4, 2 * UNITS - CUT, DEPTH), BF),
            pltpu.VMEM((UNITS, TOK), F32), pltpu.VMEM((UNITS, TOK), F32), pltpu.VMEM((UNITS, TOK), F32),
            pltpu.SemaphoreType.DMA((16,)), pltpu.SemaphoreType.DMA((16,)),
            pltpu.SemaphoreType.DMA((8,)), pltpu.SemaphoreType.DMA((4,)),
        ],
        2 * TOK * WIDE * UNITS * 3,
        [ANY] * 18,
        (VMEM, ANY, ANY, ANY),
        (*xs, *ds, *was, *wbs),
        30 << 20,
    )


def input_kernel(*refs):
    acts, was, wbs = refs[0], refs[1:5], refs[5:9]
    qa, qb, oa, ob = refs[9:13]
    wa, wb, tg, tu, total, scale, expo, sw = refs[13:]
    z, y = place()
    copies = [
        (pltpu.make_async_copy(was[k].at[pl.ds(0, UNITS)], wa.at[k], sw.at[2 * k]),
         pltpu.make_async_copy(wbs[k].at[pl.ds(0, UNITS)], wb.at[k], sw.at[2 * k + 1]))
        for k in range(4)
    ]
    for pair in copies:
        for c in pair:
            c.start()
    tg[...] = acts[:UNITS, :].T
    tu[...] = acts[UNITS:2 * UNITS, :].T
    norm = jnp.sum(jnp.abs(tg[...].astype(F32)), axis=1, keepdims=True)
    norm = norm + jnp.sum(jnp.abs(tu[...].astype(F32)), axis=1, keepdims=True)
    e = jnp.ceil(jnp.log2(jnp.maximum(norm * (1.02 * W_MAX), 1e-30)))
    scale[...] = jnp.broadcast_to(jnp.exp2(14.0 - e), (TOK, TAIL))
    expo[...] = jnp.broadcast_to(e, (TOK, TAIL))
    for k in range(4):
        for c in copies[k]:
            c.wait()

        def tile(j, _):
            n = pl.ds(pl.multiple_of(j * 256, 256), 256)
            total[:, n] = dot(tg[...], wa[k, :, n], 1, 0) + dot(tu[...], wb[k, :, n], 1, 0)
            return 0

        lax.fori_loop(0, DEPTH // 256, tile, 0)
        where = slice((k % 2) * DEPTH, (k % 2 + 1) * DEPTH)
        if k < 2:
            for s in range(4):
                r = pl.ds(pl.multiple_of(lax.rem(z + s, 4) * (4 * ROWS), 4 * ROWS), 4 * ROWS)
                if s == 0:
                    oa[:, where] = total[r, :]
                else:
                    qa[s - 1, :, where] = total[r, :] * scale[r, :1]
                    if k == 0:
                        qa[s - 1, :, HALF:] = expo[r, :]
        else:
            for s in range(4):
                for i in range(4):
                    r = pl.ds(pl.multiple_of((i * 4 + lax.rem(y + s, 4)) * ROWS, ROWS), ROWS)
                    to = slice(i * ROWS, (i + 1) * ROWS)
                    if s == 0:
                        ob[to, where] = total[r, :]
                    else:
                        qb[s - 1, to, where] = total[r, :] * scale[r, :1]
                        if k == 2:
                            qb[s - 1, to, HALF:] = expo[r, :]


def input_sums(acts, was, wbs):
    shape = jax.ShapeDtypeStruct
    q, o = shape((3, 4 * ROWS, HALF + TAIL), F32), shape((4 * ROWS, HALF), F32)
    return call(
        input_kernel,
        (q, q, o, o),
        [
            pltpu.VMEM((4, UNITS, DEPTH), BF), pltpu.VMEM((4, UNITS, DEPTH), BF),
            pltpu.VMEM((TOK, UNITS), BF), pltpu.VMEM((TOK, UNITS), BF),
            pltpu.VMEM((TOK, DEPTH), F32), pltpu.VMEM((TOK, TAIL), F32), pltpu.VMEM((TOK, TAIL), F32),
            pltpu.SemaphoreType.DMA((8,)),
        ],
        2 * TOK * WIDE * UNITS * 2,
        [VMEM] + [ANY] * 8,
        (VMEM,) * 4,
        (acts, *was, *wbs),
        22 << 20,
    )


def join_kernel(*refs):
    oa, ob, ra, rb, fa, fb = refs[0], refs[1], refs[2:5], refs[5:8], refs[8], refs[9]
    z, y = place()
    for own, got, to, at in ((oa, ra, fa, y), (ob, rb, fb, z)):
        for s in range(4):
            r = pl.ds(pl.multiple_of(lax.rem(at + s, 4) * ROWS, ROWS), ROWS)
            v = own[r, :]
            for g in got:
                v = v + g[r, :HALF] * jnp.exp2(g[r, HALF:HALF + 1] - 14.0)
            to[s] = v


def joined(oa, ob, ra, rb):
    out = jax.ShapeDtypeStruct((4, ROWS, HALF), F32)
    return call(join_kernel, (out, out), [], 1 << 20, [VMEM] * 8, (VMEM,) * 2, (oa, ob, *ra, *rb), 12 << 20)


def weight_kernel(picks, has_base, n_in, *refs):
    ins, outs = refs[:n_in], refs[n_in:n_in + 3]
    a, xc, dc, total, sa, sc, sb, so = refs[n_in + 3:]
    copies_a, copies_x, copies_d = [], [], []
    n = 0
    for g, (pieces, x_at, d_at) in enumerate(picks):
        for i, r0, r1 in pieces:
            copies_a.append(pltpu.make_async_copy(ins[i], a.at[pl.ds(r0, r1 - r0), pl.ds(g * TOK, TOK)], sa.at[n]))
            n += 1
        for (i, sub), buf, into, half in ((x_at, xc, copies_x, 0), (d_at, dc, copies_d, 1)):
            src = ins[i]
            if sub is not None:
                src = src.at[:, sub] if len(src.shape) == 4 else src.at[sub]
            into.append(pltpu.make_async_copy(src, buf.at[g], sc.at[2 * g + half]))
    base = []
    if has_base:
        base = [pltpu.make_async_copy(ins[n_in - 3 + i], total.at[i], sb.at[i]) for i in range(3)]
    for c in copies_a + copies_x + copies_d + base:
        c.start()
    for c in copies_a + copies_x:
        c.wait()
    done = []
    for i in range(3):
        if i == 2:
            for c in copies_d:
                c.wait()
        if has_base:
            base[i].wait()
        cols = dc if i == 2 else xc

        def tile(j, _):
            m = pl.ds(pl.multiple_of(j * 256, 256), 256)
            depth = len(picks) * TOK
            v = dot(a[i * UNITS:(i + 1) * UNITS, :], cols[..., m].reshape(depth, 256), 1, 0)
            total[i, :, m] = total[i, :, m] + v if has_base else v
            return 0

        lax.fori_loop(0, DEPTH // 256, tile, 0)
        done.append(pltpu.make_async_copy(total.at[i], outs[i], so.at[i]))
        done[-1].start()
    for c in done:
        c.wait()


def weight_sums(groups, base):
    ins, picks = [], []

    def slot(v):
        for i, w in enumerate(ins):
            if w is v:
                return i
        ins.append(v)
        return len(ins) - 1

    n_pieces = 0
    tiled = groups[0][1][0].ndim == 4
    for pieces, (xv, xi), (dv, di) in groups:
        row, marks = 0, []
        for p in pieces:
            marks.append((slot(p), row, row + p.shape[0]))
            row += p.shape[0]
            n_pieces += 1
        picks.append((marks, (slot(xv), xi), (slot(dv), di)))
    ins += list(base or [])
    n = len(groups)
    col = (n, 16, ROWS, DEPTH) if tiled else (n, TOK, DEPTH)
    out = jax.ShapeDtypeStruct((UNITS, DEPTH), F32)
    return call(
        functools.partial(weight_kernel, picks, base is not None, len(ins)),
        (out,) * 3,
        [
            pltpu.VMEM((3 * UNITS, n * TOK), BF), pltpu.VMEM(col, BF), pltpu.VMEM(col, BF),
            pltpu.VMEM((3, UNITS, DEPTH), F32),
            pltpu.SemaphoreType.DMA((n_pieces,)), pltpu.SemaphoreType.DMA((2 * n,)),
            pltpu.SemaphoreType.DMA((3,)), pltpu.SemaphoreType.DMA((3,)),
        ],
        2 * 3 * UNITS * DEPTH * n * TOK,
        [ANY] * len(ins),
        (ANY,) * 3,
        ins,
        n * (4 << 20) + (16 << 20),
    )


def block(inputs, w_gate, w_up, w_down, d_out):
    fs = lax.axis_index("fs")

    def relative(v):
        parts = [v[:, i * DEPTH:(i + 1) * DEPTH] for i in range(4)]
        out = []
        for k in range(4):
            w = parts[k]
            for f in range(1, 4):
                w = jnp.where(fs == f, parts[f ^ k], w)
            out.append(w)
        return out

    xp, dp = relative(inputs), relative(d_out)
    x_own, d_own = jnp.concatenate(xp, axis=1), jnp.concatenate(dp, axis=1)

    side = moved(jnp.stack([xp[1], dp[1], xp[3], dp[3]]), flip=1)
    far = jnp.stack([xp[0], side[0], dp[0], side[1]])
    near = jnp.stack([xp[2], side[2], dp[2], side[3]])
    got = jnp.stack([moved(near, dx=1), moved(near, dx=-1), moved(far, dx=2)])
    cols = lax.all_gather(got.reshape(12, ROWS, DEPTH), "tp", axis=0)

    wa = jnp.concatenate([w_gate.T, w_down[:CUT]], axis=0)
    wb = jnp.concatenate([w_up.T, w_down[CUT:]], axis=0)
    wa2, wb2 = moved(wa, dx=1), moved(wb, dx=-1)
    wa1, wb1 = moved(wa, flip=1), moved(wb, flip=1)
    wa3, wb3 = moved(wa2, flip=1), moved(wb2, flip=1)
    was, wbs = (wa, wa1, wa2, wa3), (wb, wb1, wb2, wb3)

    def spread(own, first, second):
        line = jnp.concatenate([own] + [moved(own, **{first: d}) for d in (1, 2, 3)], axis=0)
        up, down = moved(line, **{second: 1}), moved(line, **{second: -1})
        h = 2 * ROWS
        return line, up, down, moved(up[:h], **{second: 1}), moved(down[h:], **{second: -1})

    xs = spread(x_own, "dz", "dy")
    ds = spread(d_own, "dy", "dz")

    acts, x_cols, d_cols, cross = forward(xs, ds, was, wbs)

    am, ap = moved(acts, dx=1), moved(acts, dx=-1)
    acts_s, cross_s = moved(acts, flip=1), moved(cross, flip=1)
    oa, ob = moved(am[:LOW], dx=1), moved(ap[LOW:], dx=-1)
    sm, sp = moved(am, flip=1), moved(ap, flip=1)
    soa, sob = moved(oa, flip=1), moved(ob, flip=1)

    qa, qb, own_a, own_b = input_sums(acts, was, wbs)
    qa, qb = qa.astype(F16), qb.astype(F16)
    ra = [moved(qa[d - 1], dz=-d).astype(F32) for d in (1, 2, 3)]
    rb = [moved(qb[d - 1], dy=-d).astype(F32) for d in (1, 2, 3)]
    fa, fb = joined(own_a, own_b, ra, rb)
    fa = fa[0] + moved(fa[1], dy=-1) + moved(fa[2], dy=-2) + moved(fa[3], dy=-3)
    fb = fb[0] + moved(fb[1], dz=-1) + moved(fb[2], dz=-2) + moved(fb[3], dz=-3)
    grad_inputs = jnp.concatenate(relative(jnp.concatenate([fa, fb], axis=1).astype(BF)), axis=1)

    sums = weight_sums([([acts], (x_cols, None), (d_cols, None)), ([acts_s], (cross_s, 0), (cross_s, 1))], None)
    sums = weight_sums(
        [([am], (cols, 0), (cols, 2)), ([sm], (cols, 1), (cols, 3)),
         ([ap], (cols, 4), (cols, 6)), ([sp], (cols, 5), (cols, 7))], sums)
    sums = weight_sums([([oa, ob], (cols, 8), (cols, 10)), ([soa, sob], (cols, 9), (cols, 11))], sums)
    return grad_inputs, sums[0].T, sums[1].T, sums[2]


def solution(mesh):
    tok = P(AXES, None)
    return jax.shard_map(
        block,
        mesh=mesh,
        in_specs=(tok, P("fs", "tp"), P("fs", "tp"), P("tp", "fs"), tok),
        out_specs=(tok, P("fs", "tp"), P("fs", "tp"), P("tp", "fs")),
        check_vma=False,
    )
```

```python
import functools

import jax
import jax.numpy as jnp
from jax import lax
from jax.experimental import pallas as pl
from jax.experimental.pallas import tpu as pltpu
from jax.sharding import PartitionSpec as P


AXES = ("rep", "fs", "tp")
BF, F32, F16 = jnp.bfloat16, jnp.float32, jnp.float16
W_MAX = 0.09375
ANY = pl.BlockSpec(memory_space=pl.ANY)
VMEM = pl.BlockSpec(memory_space=pltpu.VMEM)
LIMIT = 56 * 1024 * 1024

ROWS, DEPTH, UNITS = 32, 1024, 688
TOK, WIDE = 16 * ROWS, 4 * DEPTH
CUT = 336
LOW = 1040
TAIL = 128


def index_of(x, c, z, y):
    x, z, y = x % 4, z % 4, y % 4
    return (x // 2) * 64 + ((x % 2) * 2 + c) * 16 + z * 4 + y


def moved(array, dx=0, flip=0, dz=0, dy=0):
    pairs = []
    for x in range(4):
        for c in range(2):
            for z in range(4):
                for y in range(4):
                    pairs.append((index_of(x + dx, c ^ flip, z + dz, y + dy), index_of(x, c, z, y)))
    return lax.ppermute(array, AXES, pairs)


def dot(a, b, ca, cb):
    return lax.dot_general(a, b, (((ca,), (cb,)), ((), ())), preferred_element_type=F32)


def place():
    tp = lax.axis_index("tp")
    return tp // 4, tp % 4


def call(body, out_shape, scratch, flops, ins, outs, args, nbytes):
    return pl.pallas_call(
        body,
        out_shape=out_shape,
        in_specs=ins,
        out_specs=outs,
        scratch_shapes=scratch,
        compiler_params=pltpu.CompilerParams(vmem_limit_bytes=LIMIT),
        cost_estimate=pl.CostEstimate(flops=flops, bytes_accessed=nbytes, transcendentals=0),
    )(*args)


D_FROM = ((0, 0, 4, 0), (1, 0, 4, 1), (2, 0, 4, 3), (3, 0, 2, 2), (4, 2, 2, 2))


def forward_kernel(*refs):
    x_in, ds, was, wbs = refs[0], refs[1:6], refs[6:10], refs[10:14]
    acts, side, x_own, d_own = refs[14:18]
    x, d, wa, wb, gate, up, back, act, sx, sd, sw, so = refs[18:]
    z, y = place()
    d_copies = []
    for i, first, count, off in D_FROM:
        for j in range(count):
            row = pl.multiple_of((lax.rem(z + off, 4) * 4 + lax.rem(y + first + j, 4)) * ROWS, ROWS)
            d_copies.append(
                pltpu.make_async_copy(ds[i].at[pl.ds(j * ROWS, ROWS)], d.at[pl.ds(row, ROWS)], sd.at[len(d_copies)]))
    x_copies = [
        pltpu.make_async_copy(x_in.at[:, pl.ds(k * DEPTH, DEPTH)], x.at[:, pl.ds(k * DEPTH, DEPTH)], sx.at[k])
        for k in range(4)
    ]
    w_copies = [
        (pltpu.make_async_copy(was[k], wa.at[k], sw.at[2 * k]), pltpu.make_async_copy(wbs[k], wb.at[k], sw.at[2 * k + 1]))
        for k in range(4)
    ]
    for c in (x_copies[0], *w_copies[0], *d_copies):
        c.start()
    for k in range(1, 4):
        for c in (x_copies[k], *w_copies[k]):
            c.start()
    outs = []
    for k in range(4):
        for c in (x_copies[k], *w_copies[k]):
            c.wait()

        def first(j, _):
            t = pl.ds(pl.multiple_of(j * 256, 256), 256)
            xk = x[t, k * DEPTH:(k + 1) * DEPTH]
            for into, w in ((gate, wa), (up, wb)):
                part = dot(w[k, :UNITS], xk, 1, 1)
                into[:, t] = part if k == 0 else into[:, t] + part
            return 0

        def second(j, _):
            t = pl.ds(pl.multiple_of(j * 256, 256), 256)
            dk = d[t, k * DEPTH:(k + 1) * DEPTH]
            for rows, w in ((slice(0, CUT), wa), (slice(CUT, UNITS), wb)):
                part = dot(w[k, UNITS:], dk, 1, 1)
                back[rows, t] = part if k == 0 else back[rows, t] + part
            return 0

        lax.fori_loop(0, 2, first, 0)
        if k == 0:
            for c in d_copies:
                c.wait()
        lax.fori_loop(0, 2, second, 0)
        if k == 1:
            for i, (v, to) in enumerate(((x, x_own), (d, d_own))):
                outs.append(pltpu.make_async_copy(v.at[:, pl.ds(0, DEPTH)], to, so.at[i]))
                for h in range(2):
                    outs.append(pltpu.make_async_copy(
                        v.at[:, pl.ds(DEPTH + h * TOK, TOK)],
                        side.at[pl.ds(3 * UNITS + (2 * i + h) * TOK, TOK)], so.at[2 + 2 * i + h]))
            for c in outs:
                c.start()

    def unit(i, _):
        r = pl.ds(pl.multiple_of(i * 16, 16), 16)
        g = gate[r, :].astype(BF).astype(F32)
        u = up[r, :].astype(BF).astype(F32)
        b = back[r, :].astype(BF).astype(F32)
        sigma = 1.0 / (1.0 + jnp.exp(-g))
        active = g * sigma
        act[r, :] = (b * u * sigma * (1.0 + g * (1.0 - sigma))).astype(BF)
        act[pl.ds(pl.multiple_of(UNITS + i * 16, 16), 16), :] = (b * active).astype(BF)
        act[pl.ds(pl.multiple_of(2 * UNITS + i * 16, 16), 16), :] = (active * u).astype(BF)
        return 0

    lax.fori_loop(0, UNITS // 16, unit, 0)
    outs.append(pltpu.make_async_copy(act, acts, so.at[6]))
    outs.append(pltpu.make_async_copy(act, side.at[pl.ds(0, 3 * UNITS)], so.at[7]))
    for c in outs[-2:]:
        c.start()
    for c in outs:
        c.wait()


def forward(x, ds, was, wbs):
    shape = jax.ShapeDtypeStruct
    return call(
        forward_kernel,
        (shape((3 * UNITS, TOK), BF), shape((3 * UNITS + 4 * TOK, TOK), BF), shape((TOK, DEPTH), BF), shape((TOK, DEPTH), BF)),
        [
            pltpu.VMEM((TOK, WIDE), BF), pltpu.VMEM((TOK, WIDE), BF),
            pltpu.VMEM((4, UNITS + CUT, DEPTH), BF), pltpu.VMEM((4, 2 * UNITS - CUT, DEPTH), BF),
            pltpu.VMEM((UNITS, TOK), F32), pltpu.VMEM((UNITS, TOK), F32), pltpu.VMEM((UNITS, TOK), F32),
            pltpu.VMEM((3 * UNITS, TOK), BF),
            pltpu.SemaphoreType.DMA((4,)), pltpu.SemaphoreType.DMA((16,)),
            pltpu.SemaphoreType.DMA((8,)), pltpu.SemaphoreType.DMA((8,)),
        ],
        2 * TOK * WIDE * UNITS * 3,
        [ANY] * 14,
        (ANY,) * 4,
        (x, *ds, *was, *wbs),
        34 << 20,
    )


def input_kernel(*refs):
    acts, was, wbs, out = refs[0], refs[1:5], refs[5:9], refs[9]
    wa, wb, tg, tu, scale, sw = refs[10:]
    copies = [
        (pltpu.make_async_copy(was[k].at[pl.ds(0, UNITS)], wa.at[k], sw.at[2 * k]),
         pltpu.make_async_copy(wbs[k].at[pl.ds(0, UNITS)], wb.at[k], sw.at[2 * k + 1]))
        for k in range(4)
    ]
    for pair in copies:
        for c in pair:
            c.start()
    tg[...] = acts[:UNITS, :].T
    tu[...] = acts[UNITS:2 * UNITS, :].T
    norm = jnp.sum(jnp.abs(tg[...].astype(F32)), axis=1, keepdims=True)
    norm = norm + jnp.sum(jnp.abs(tu[...].astype(F32)), axis=1, keepdims=True)
    e = jnp.ceil(jnp.log2(jnp.maximum(norm * (1.02 * W_MAX), 1e-30)))
    scale[...] = jnp.broadcast_to(jnp.exp2(14.0 - e), (TOK, TAIL))
    out[:, WIDE:] = jnp.broadcast_to(e, (TOK, TAIL))
    for k in range(4):
        for c in copies[k]:
            c.wait()

        def tile(j, _):
            n = pl.ds(pl.multiple_of(j * 256, 256), 256)
            m = pl.ds(pl.multiple_of(k * DEPTH + j * 256, 256), 256)
            v = dot(tg[...], wa[k, :, n], 1, 0) + dot(tu[...], wb[k, :, n], 1, 0)
            out[:, m] = v * scale[:, :1]
            return 0

        lax.fori_loop(0, DEPTH // 256, tile, 0)


def input_sums(acts, was, wbs):
    return call(
        input_kernel,
        jax.ShapeDtypeStruct((TOK, WIDE + TAIL), F32),
        [
            pltpu.VMEM((4, UNITS, DEPTH), BF), pltpu.VMEM((4, UNITS, DEPTH), BF),
            pltpu.VMEM((TOK, UNITS), BF), pltpu.VMEM((TOK, UNITS), BF),
            pltpu.VMEM((TOK, TAIL), F32),
            pltpu.SemaphoreType.DMA((8,)),
        ],
        2 * TOK * WIDE * UNITS * 2,
        [VMEM] + [ANY] * 8,
        VMEM,
        (acts, *was, *wbs),
        22 << 20,
    )


def weight_kernel(picks, has_base, n_in, *refs):
    ins, outs = refs[:n_in], refs[n_in:n_in + 3]
    a, xc, dc, total, sa, sc, sb, so = refs[n_in + 3:]
    copies_a, copies_x, copies_d = [], [], []
    n = 0
    for g, (pieces, x_at, d_at) in enumerate(picks):
        for i, r0, r1 in pieces:
            copies_a.append(pltpu.make_async_copy(
                ins[i].at[pl.ds(0, r1 - r0)], a.at[pl.ds(r0, r1 - r0), pl.ds(g * TOK, TOK)], sa.at[n]))
            n += 1
        for (i, sub), buf, into, half in ((x_at, xc, copies_x, 0), (d_at, dc, copies_d, 1)):
            if len(ins[i].shape) == 4:
                pairs = [(ins[i].at[:, sub], buf.at[g])]
            elif sub is None:
                pairs = [(ins[i], buf.at[g])]
            else:
                pairs = [(ins[i].at[pl.ds(sub + h * TOK, TOK)], buf.at[g, :, pl.ds(h * TOK, TOK)]) for h in range(2)]
            for h, (src, to) in enumerate(pairs):
                into.append(pltpu.make_async_copy(src, to, sc.at[4 * g + 2 * half + h]))
    base = []
    if has_base:
        base = [pltpu.make_async_copy(ins[n_in - 3 + i], total.at[i], sb.at[i]) for i in range(3)]
    for c in copies_a + copies_x + copies_d + base:
        c.start()
    for c in copies_a + copies_x:
        c.wait()
    done = []
    for i in range(3):
        if i == 2:
            for c in copies_d:
                c.wait()
        if has_base:
            base[i].wait()
        cols = dc if i == 2 else xc

        def tile(j, _):
            m = pl.ds(pl.multiple_of(j * 256, 256), 256)
            depth = len(picks) * TOK
            v = dot(a[i * UNITS:(i + 1) * UNITS, :], cols[..., m].reshape(depth, 256), 1, 0)
            total[i, :, m] = total[i, :, m] + v if has_base else v
            return 0

        lax.fori_loop(0, DEPTH // 256, tile, 0)
        done.append(pltpu.make_async_copy(total.at[i], outs[i], so.at[i]))
        done[-1].start()
    for c in done:
        c.wait()


def weight_sums(groups, base):
    ins, picks = [], []

    def slot(v):
        for i, w in enumerate(ins):
            if w is v:
                return i
        ins.append(v)
        return len(ins) - 1

    n_pieces = 0
    tiled = groups[0][2][0].ndim == 4
    for pieces, rows, (xv, xi), (dv, di) in groups:
        row, marks = 0, []
        for p, m in zip(pieces, rows):
            marks.append((slot(p), row, row + m))
            row += m
            n_pieces += 1
        picks.append((marks, (slot(xv), xi), (slot(dv), di)))
    ins += list(base or [])
    n = len(groups)
    col = (n, 16, ROWS, DEPTH) if tiled else (n, TOK, DEPTH)
    out = jax.ShapeDtypeStruct((UNITS, DEPTH), F32)
    return call(
        functools.partial(weight_kernel, picks, base is not None, len(ins)),
        (out,) * 3,
        [
            pltpu.VMEM((3 * UNITS, n * TOK), BF), pltpu.VMEM(col, BF), pltpu.VMEM(col, BF),
            pltpu.VMEM((3, UNITS, DEPTH), F32),
            pltpu.SemaphoreType.DMA((n_pieces,)), pltpu.SemaphoreType.DMA((4 * n,)),
            pltpu.SemaphoreType.DMA((3,)), pltpu.SemaphoreType.DMA((3,)),
        ],
        2 * 3 * UNITS * DEPTH * n * TOK,
        [ANY] * len(ins),
        (ANY,) * 3,
        ins,
        n * (4 << 20) + (16 << 20),
    )


def block(inputs, w_gate, w_up, w_down, d_out):
    fs = lax.axis_index("fs")

    def relative(v):
        parts = [v[:, i * DEPTH:(i + 1) * DEPTH] for i in range(4)]
        out = []
        for k in range(4):
            w = parts[k]
            for f in range(1, 4):
                w = jnp.where(fs == f, parts[f ^ k], w)
            out.append(w)
        return out

    xp, dp = relative(inputs), relative(d_out)
    x_own, d_own = jnp.concatenate(xp, axis=1), jnp.concatenate(dp, axis=1)

    x = lax.all_gather(x_own, "tp", axis=0, tiled=True)
    line = jnp.concatenate([d_own] + [moved(d_own, dy=d) for d in (1, 2, 3)], axis=0)
    up, down = moved(line, dz=1), moved(line, dz=-1)
    h = 2 * ROWS
    ds = (line, up, down, moved(up[:h], dz=1), moved(down[h:], dz=-1))

    side = moved(jnp.stack([xp[1], dp[1], xp[3], dp[3]]), flip=1)
    far = jnp.stack([xp[0], side[0], dp[0], side[1]])
    near = jnp.stack([xp[2], side[2], dp[2], side[3]])
    got = jnp.stack([moved(near, dx=1), moved(near, dx=-1), moved(far, dx=2)])
    cols = lax.all_gather(got.reshape(12, ROWS, DEPTH), "tp", axis=0)

    wa = jnp.concatenate([w_gate.T, w_down[:CUT]], axis=0)
    wb = jnp.concatenate([w_up.T, w_down[CUT:]], axis=0)
    wa2, wb2 = moved(wa, dx=1), moved(wb, dx=-1)
    wa1, wb1 = moved(wa, flip=1), moved(wb, flip=1)
    wa3, wb3 = moved(wa2, flip=1), moved(wb2, flip=1)
    was, wbs = (wa, wa1, wa2, wa3), (wb, wb1, wb2, wb3)

    acts, side, x_cols, d_cols = forward(x, ds, was, wbs)

    am, ap = moved(acts, dx=1), moved(acts, dx=-1)
    side = moved(side, flip=1)
    oa, ob = moved(am[:LOW], dx=1), moved(ap[LOW:], dx=-1)
    sm, sp = moved(am, flip=1), moved(ap, flip=1)
    soa, sob = moved(oa, flip=1), moved(ob, flip=1)

    packed = input_sums(acts, was, wbs).astype(F16)
    got = lax.all_to_all(packed, "tp", 0, 0, tiled=True)
    got = got.reshape(16, ROWS, WIDE + TAIL).astype(F32)
    back = jnp.exp2(got[:, :, WIDE:WIDE + 1] - 14.0)
    grad_inputs = jnp.sum(got[:, :, :WIDE] * back, axis=0).astype(BF)
    grad_inputs = jnp.concatenate(relative(grad_inputs), axis=1)

    full, cut = (3 * UNITS,), (LOW, 3 * UNITS - LOW)
    at = 3 * UNITS
    sums = weight_sums(
        [([acts], full, (x_cols, None), (d_cols, None)), ([side], full, (side, at), (side, at + 2 * TOK))], None)
    sums = weight_sums(
        [([am], full, (cols, 0), (cols, 2)), ([sm], full, (cols, 1), (cols, 3)),
         ([ap], full, (cols, 4), (cols, 6)), ([sp], full, (cols, 5), (cols, 7))], sums)
    sums = weight_sums(
        [([oa, ob], cut, (cols, 8), (cols, 10)), ([soa, sob], cut, (cols, 9), (cols, 11))], sums)
    return grad_inputs, sums[0].T, sums[1].T, sums[2]


def solution(mesh):
    tok = P(AXES, None)
    return jax.shard_map(
        block,
        mesh=mesh,
        in_specs=(tok, P("fs", "tp"), P("fs", "tp"), P("tp", "fs"), tok),
        out_specs=(tok, P("fs", "tp"), P("fs", "tp"), P("tp", "fs")),
        check_vma=False,
    )
```

```python
import functools

import jax
import jax.numpy as jnp
from jax import lax
from jax.experimental import pallas as pl
from jax.experimental.pallas import tpu as pltpu
from jax.sharding import PartitionSpec as P


AXES = ("rep", "fs", "tp")
BF, F32, F16 = jnp.bfloat16, jnp.float32, jnp.float16
W_MAX = 0.09375
ANY = pl.BlockSpec(memory_space=pl.ANY)
VMEM = pl.BlockSpec(memory_space=pltpu.VMEM)
LIMIT = 56 * 1024 * 1024

ROWS, DEPTH, UNITS = 32, 1024, 688
TOK, WIDE = 16 * ROWS, 4 * DEPTH
CUT = 336
LOW = 1040
HALF = 2 * DEPTH
TAIL = 128


def index_of(x, c, z, y):
    x, z, y = x % 4, z % 4, y % 4
    return (x // 2) * 64 + ((x % 2) * 2 + c) * 16 + z * 4 + y


def moved(array, dx=0, flip=0, dz=0, dy=0):
    pairs = []
    for x in range(4):
        for c in range(2):
            for z in range(4):
                for y in range(4):
                    pairs.append((index_of(x + dx, c ^ flip, z + dz, y + dy), index_of(x, c, z, y)))
    return lax.ppermute(array, AXES, pairs)


def dot(a, b, ca, cb):
    return lax.dot_general(a, b, (((ca,), (cb,)), ((), ())), preferred_element_type=F32)


def place():
    tp = lax.axis_index("tp")
    return tp // 4, tp % 4


def call(body, out_shape, scratch, flops, ins, outs, args, nbytes):
    return pl.pallas_call(
        body,
        out_shape=out_shape,
        in_specs=ins,
        out_specs=outs,
        scratch_shapes=scratch,
        compiler_params=pltpu.CompilerParams(vmem_limit_bytes=LIMIT),
        cost_estimate=pl.CostEstimate(flops=flops, bytes_accessed=nbytes, transcendentals=0),
    )(*args)


FROM = ((0, 0, 4, 0), (1, 0, 4, 1), (2, 0, 4, 3), (3, 0, 2, 2), (4, 2, 2, 2))


def forward_kernel(*refs):
    xs, ds, was, wbs = refs[:5], refs[5:10], refs[10:14], refs[14:18]
    acts, side, x_own, d_own = refs[18:22]
    x, d, wa, wb, gate, up, back, act, sx, sd, sw, so = refs[22:]
    z, y = place()
    x_copies, d_copies = [], []
    for i, first, count, off in FROM:
        for j in range(count):
            row = pl.multiple_of((lax.rem(z + first + j, 4) * 4 + lax.rem(y + off, 4)) * ROWS, ROWS)
            x_copies.append(
                pltpu.make_async_copy(xs[i].at[pl.ds(j * ROWS, ROWS)], x.at[pl.ds(row, ROWS)], sx.at[len(x_copies)]))
            row = pl.multiple_of((lax.rem(z + off, 4) * 4 + lax.rem(y + first + j, 4)) * ROWS, ROWS)
            d_copies.append(
                pltpu.make_async_copy(ds[i].at[pl.ds(j * ROWS, ROWS)], d.at[pl.ds(row, ROWS)], sd.at[len(d_copies)]))
    w_copies = [
        [pltpu.make_async_copy(was[k], wa.at[k], sw.at[2 * k]), pltpu.make_async_copy(wbs[k], wb.at[k], sw.at[2 * k + 1])]
        for k in range(4)
    ]
    stages = [x_copies + w_copies[0], d_copies, w_copies[1], w_copies[2], w_copies[3]]

    def begin(n):
        if n < len(stages):
            for c in stages[n]:
                c.start()

    def end(n):
        for c in stages[n]:
            c.wait()

    def first(k):
        xk = x[:, k * DEPTH:(k + 1) * DEPTH]
        for into, w in ((gate, wa), (up, wb)):
            part = dot(w[k, :UNITS], xk, 1, 1)
            into[...] = part if k == 0 else into[...] + part

    def second(k):
        dk = d[:, k * DEPTH:(k + 1) * DEPTH]
        for rows, w in ((slice(0, CUT), wa), (slice(CUT, UNITS), wb)):
            part = dot(w[k, UNITS:], dk, 1, 1)
            back[rows, :] = part if k == 0 else back[rows, :] + part

    begin(0)
    begin(1)
    end(0)
    begin(2)
    first(0)
    end(1)
    begin(3)
    second(0)
    end(2)
    begin(4)
    outs = []
    for i, (v, to) in enumerate(((x, x_own), (d, d_own))):
        outs.append(pltpu.make_async_copy(v.at[:, pl.ds(0, DEPTH)], to, so.at[i]))
        for h in range(2):
            outs.append(pltpu.make_async_copy(
                v.at[:, pl.ds(DEPTH + h * TOK, TOK)],
                side.at[pl.ds(3 * UNITS + (2 * i + h) * TOK, TOK)], so.at[2 + 2 * i + h]))
    for k in (1, 2, 3):
        if k > 1:
            end(k + 1)
        if k == 3:
            for c in outs:
                c.start()
        first(k)
        second(k)

    def unit(i, _):
        r = pl.ds(pl.multiple_of(i * 16, 16), 16)
        g = gate[r, :].astype(BF).astype(F32)
        u = up[r, :].astype(BF).astype(F32)
        b = back[r, :].astype(BF).astype(F32)
        sigma = 1.0 / (1.0 + jnp.exp(-g))
        active = g * sigma
        act[r, :] = (b * u * sigma * (1.0 + g * (1.0 - sigma))).astype(BF)
        act[pl.ds(pl.multiple_of(UNITS + i * 16, 16), 16), :] = (b * active).astype(BF)
        act[pl.ds(pl.multiple_of(2 * UNITS + i * 16, 16), 16), :] = (active * u).astype(BF)
        return 0

    lax.fori_loop(0, UNITS // 16, unit, 0)
    outs.append(pltpu.make_async_copy(act, acts, so.at[6]))
    outs.append(pltpu.make_async_copy(act, side.at[pl.ds(0, 3 * UNITS)], so.at[7]))
    for c in outs[-2:]:
        c.start()
    for c in outs:
        c.wait()


def forward(xs, ds, was, wbs):
    shape = jax.ShapeDtypeStruct
    return call(
        forward_kernel,
        (shape((3 * UNITS, TOK), BF), shape((3 * UNITS + 4 * TOK, TOK), BF), shape((TOK, DEPTH), BF), shape((TOK, DEPTH), BF)),
        [
            pltpu.VMEM((TOK, WIDE), BF), pltpu.VMEM((TOK, WIDE), BF),
            pltpu.VMEM((4, UNITS + CUT, DEPTH), BF), pltpu.VMEM((4, 2 * UNITS - CUT, DEPTH), BF),
            pltpu.VMEM((UNITS, TOK), F32), pltpu.VMEM((UNITS, TOK), F32), pltpu.VMEM((UNITS, TOK), F32),
            pltpu.VMEM((3 * UNITS, TOK), BF),
            pltpu.SemaphoreType.DMA((16,)), pltpu.SemaphoreType.DMA((16,)),
            pltpu.SemaphoreType.DMA((8,)), pltpu.SemaphoreType.DMA((8,)),
        ],
        2 * TOK * WIDE * UNITS * 3,
        [ANY] * 18,
        (ANY,) * 4,
        (*xs, *ds, *was, *wbs),
        34 << 20,
    )


def input_kernel(*refs):
    acts, was, wbs = refs[0], refs[1:5], refs[5:9]
    own, away = refs[9:11], refs[11:13]
    wa, wb, tg, tu, total, expo, sw, so, st = refs[13:]
    z, y = place()
    copies = [
        (pltpu.make_async_copy(was[k].at[pl.ds(0, UNITS)], wa.at[k], sw.at[2 * k]),
         pltpu.make_async_copy(wbs[k].at[pl.ds(0, UNITS)], wb.at[k], sw.at[2 * k + 1]))
        for k in range(4)
    ]
    for pair in copies[:2]:
        for c in pair:
            c.start()
    tg[...] = acts[:UNITS, :].T
    tu[...] = acts[UNITS:2 * UNITS, :].T
    norm = jnp.sum(jnp.abs(tg[...].astype(F32)), axis=1, keepdims=True)
    norm = norm + jnp.sum(jnp.abs(tu[...].astype(F32)), axis=1, keepdims=True)
    e = jnp.ceil(jnp.log2(jnp.maximum(norm * (1.02 * W_MAX), 1e-30)))
    expo[...] = jnp.broadcast_to(e, (TOK, TAIL))

    def puts(src, side, cols, sems):
        out, n = [], 0
        for s in range(4):
            for i in range(4):
                zz, yy = (lax.rem(z + s, 4), i) if side == 0 else (i, lax.rem(y + s, 4))
                r = pl.ds(pl.multiple_of((zz * 4 + yy) * ROWS, ROWS), ROWS)
                to = own[side] if s == 0 else away[side].at[s - 1]
                out.append(pltpu.make_async_copy(src.at[r], to.at[pl.ds(i * ROWS, ROWS), cols], sems.at[n]))
                n += 1
        return out

    tails = [c for side in range(2) for c in puts(expo, side, pl.ds(HALF, TAIL), st.at[side])]
    for c in tails:
        c.start()
    pending = [None, None]
    for k in range(4):
        for c in copies[k]:
            c.wait()
        if k + 2 < 4:
            for c in copies[k + 2]:
                c.start()
        if pending[k % 2]:
            for c in pending[k % 2]:
                c.wait()
        v = dot(tg[...], wa[k], 1, 0) + dot(tu[...], wb[k], 1, 0)
        total[k % 2] = v * jnp.exp2(14.0 - expo[:, :1])
        pending[k % 2] = puts(total.at[k % 2], k // 2, pl.ds((k % 2) * DEPTH, DEPTH), so.at[k % 2])
        for c in pending[k % 2]:
            c.start()
    for c in pending[0] + pending[1] + tails:
        c.wait()


def input_sums(acts, was, wbs):
    shape = jax.ShapeDtypeStruct
    own, away = shape((4 * ROWS, HALF + TAIL), F32), shape((3, 4 * ROWS, HALF + TAIL), F32)
    return call(
        input_kernel,
        (own, own, away, away),
        [
            pltpu.VMEM((4, UNITS, DEPTH), BF), pltpu.VMEM((4, UNITS, DEPTH), BF),
            pltpu.VMEM((TOK, UNITS), BF), pltpu.VMEM((TOK, UNITS), BF),
            pltpu.VMEM((2, TOK, DEPTH), F32), pltpu.VMEM((TOK, TAIL), F32),
            pltpu.SemaphoreType.DMA((8,)), pltpu.SemaphoreType.DMA((2, 16)), pltpu.SemaphoreType.DMA((2, 16)),
        ],
        2 * TOK * WIDE * UNITS * 2,
        [VMEM] + [ANY] * 8,
        (ANY,) * 4,
        (acts, *was, *wbs),
        22 << 20,
    )


def join_kernel(*refs):
    z, y = place()
    for got, to, at in ((refs[0:4], refs[8], y), (refs[4:8], refs[9], z)):
        for s in range(4):
            r = pl.ds(pl.multiple_of(lax.rem(at + s, 4) * ROWS, ROWS), ROWS)
            v = None
            for g in got:
                w = g[r, :HALF] * jnp.exp2(g[r, HALF:HALF + 1] - 14.0)
                v = w if v is None else v + w
            to[s] = v


def joined(own_a, own_b, ra, rb):
    out = jax.ShapeDtypeStruct((4, ROWS, HALF), F32)
    return call(
        join_kernel, (out, out), [], 1 << 30, [VMEM] * 8, (VMEM,) * 2, (own_a, *ra, own_b, *rb), 12 << 20)


def weight_kernel(picks, has_base, n_in, *refs):
    ins, outs = refs[:n_in], refs[n_in:n_in + 3]
    a, xc, dc, total, sa, sc, sb, so = refs[n_in + 3:]
    stages = [[], [], []]
    n = 0
    for g, (pieces, x_at, d_at) in enumerate(picks):
        for i, r0, r1 in pieces:
            for s in range(3):
                lo, hi = max(r0, s * UNITS), min(r1, (s + 1) * UNITS)
                if lo < hi:
                    stages[s].append(pltpu.make_async_copy(
                        ins[i].at[pl.ds(lo - r0, hi - lo)], a.at[pl.ds(lo, hi - lo), pl.ds(g * TOK, TOK)], sa.at[n]))
                    n += 1
        for (i, sub), buf, s in ((x_at, xc, 0), (d_at, dc, 2)):
            if len(ins[i].shape) == 4:
                pairs = [(ins[i].at[:, sub], buf.at[g])]
            elif sub is None:
                pairs = [(ins[i], buf.at[g])]
            else:
                pairs = [(ins[i].at[pl.ds(sub + h * TOK, TOK)], buf.at[g, :, pl.ds(h * TOK, TOK)]) for h in range(2)]
            for h, (src, to) in enumerate(pairs):
                stages[s].append(pltpu.make_async_copy(src, to, sc.at[4 * g + s + h]))
    if has_base:
        for s in range(3):
            stages[s].append(pltpu.make_async_copy(ins[n_in - 3 + s], total.at[s], sb.at[s]))

    def begin(s):
        for c in stages[s]:
            c.start()

    begin(0)
    begin(1)
    done = []
    for i in range(3):
        for c in stages[i]:
            c.wait()
        if i == 0:
            begin(2)
        cols = dc if i == 2 else xc
        v = dot(a[i * UNITS:(i + 1) * UNITS, :], cols[...].reshape(len(picks) * TOK, DEPTH), 1, 0)
        total[i] = total[i] + v if has_base else v
        done.append(pltpu.make_async_copy(total.at[i], outs[i], so.at[i]))
        done[-1].start()
    for c in done:
        c.wait()


def weight_sums(groups, base):
    ins, picks = [], []

    def slot(v):
        for i, w in enumerate(ins):
            if w is v:
                return i
        ins.append(v)
        return len(ins) - 1

    n_pieces = 0
    tiled = groups[0][2][0].ndim == 4
    for pieces, rows, (xv, xi), (dv, di) in groups:
        row, marks = 0, []
        for p, m in zip(pieces, rows):
            marks.append((slot(p), row, row + m))
            row += m
            n_pieces += 1
        picks.append((marks, (slot(xv), xi), (slot(dv), di)))
    ins += list(base or [])
    n = len(groups)
    col = (n, 16, ROWS, DEPTH) if tiled else (n, TOK, DEPTH)
    out = jax.ShapeDtypeStruct((UNITS, DEPTH), F32)
    return call(
        functools.partial(weight_kernel, picks, base is not None, len(ins)),
        (out,) * 3,
        [
            pltpu.VMEM((3 * UNITS, n * TOK), BF), pltpu.VMEM(col, BF), pltpu.VMEM(col, BF),
            pltpu.VMEM((3, UNITS, DEPTH), F32),
            pltpu.SemaphoreType.DMA((3 * n_pieces,)), pltpu.SemaphoreType.DMA((4 * n,)),
            pltpu.SemaphoreType.DMA((3,)), pltpu.SemaphoreType.DMA((3,)),
        ],
        2 * 3 * UNITS * DEPTH * n * TOK,
        [ANY] * len(ins),
        (ANY,) * 3,
        ins,
        n * (4 << 20) + (16 << 20),
    )


def block(inputs, w_gate, w_up, w_down, d_out):
    fs = lax.axis_index("fs")

    def relative(v):
        parts = [v[:, i * DEPTH:(i + 1) * DEPTH] for i in range(4)]
        out = []
        for k in range(4):
            w = parts[k]
            for f in range(1, 4):
                w = jnp.where(fs == f, parts[f ^ k], w)
            out.append(w)
        return out

    xp, dp = relative(inputs), relative(d_out)
    x_own, d_own = jnp.concatenate(xp, axis=1), jnp.concatenate(dp, axis=1)

    def spread(own, first, second):
        line = jnp.concatenate([own] + [moved(own, **{first: d}) for d in (1, 2, 3)], axis=0)
        up, down = moved(line, **{second: 1}), moved(line, **{second: -1})
        h = 2 * ROWS
        return (line, up, down, moved(up[:h], **{second: 1}), moved(down[h:], **{second: -1}))

    xs = spread(x_own, "dz", "dy")
    ds = spread(d_own, "dy", "dz")

    side = moved(jnp.stack([xp[1], dp[1], xp[3], dp[3]]), flip=1)
    far = jnp.stack([xp[0], side[0], dp[0], side[1]])
    near = jnp.stack([xp[2], side[2], dp[2], side[3]])
    got = jnp.stack([moved(near, dx=1), moved(near, dx=-1), moved(far, dx=2)])
    cols = lax.all_gather(got.reshape(12, ROWS, DEPTH), "tp", axis=0)

    wa = jnp.concatenate([w_gate.T, w_down[:CUT]], axis=0)
    wb = jnp.concatenate([w_up.T, w_down[CUT:]], axis=0)
    wa2, wb2 = moved(wa, dx=1), moved(wb, dx=-1)
    wa1, wb1 = moved(wa, flip=1), moved(wb, flip=1)
    wa3, wb3 = moved(wa2, flip=1), moved(wb2, flip=1)
    was, wbs = (wa, wa1, wa2, wa3), (wb, wb1, wb2, wb3)

    acts, side, x_cols, d_cols = forward(xs, ds, was, wbs)

    am, ap = moved(acts, dx=1), moved(acts, dx=-1)
    side = moved(side, flip=1)
    oa, ob = moved(am[:LOW], dx=1), moved(ap[LOW:], dx=-1)
    sm, sp = moved(am, flip=1), moved(ap, flip=1)
    soa, sob = moved(oa, flip=1), moved(ob, flip=1)

    own_a, own_b, qa, qb = input_sums(acts, was, wbs)
    qa, qb = qa.astype(F16), qb.astype(F16)
    ra = [moved(qa[d - 1], dz=-d).astype(F32) for d in (1, 2, 3)]
    rb = [moved(qb[d - 1], dy=-d).astype(F32) for d in (1, 2, 3)]
    fa, fb = joined(own_a, own_b, ra, rb)
    fa = fa[0] + moved(fa[1], dy=-1) + moved(fa[2], dy=-2) + moved(fa[3], dy=-3)
    fb = fb[0] + moved(fb[1], dz=-1) + moved(fb[2], dz=-2) + moved(fb[3], dz=-3)
    grad_inputs = jnp.concatenate(relative(jnp.concatenate([fa, fb], axis=1).astype(BF)), axis=1)

    full, cut = (3 * UNITS,), (LOW, 3 * UNITS - LOW)
    at = 3 * UNITS
    sums = weight_sums(
        [([acts], full, (x_cols, None), (d_cols, None)), ([side], full, (side, at), (side, at + 2 * TOK))], None)
    sums = weight_sums(
        [([am], full, (cols, 0), (cols, 2)), ([sm], full, (cols, 1), (cols, 3)),
         ([ap], full, (cols, 4), (cols, 6)), ([sp], full, (cols, 5), (cols, 7))], sums)
    sums = weight_sums(
        [([oa, ob], cut, (cols, 8), (cols, 10)), ([soa, sob], cut, (cols, 9), (cols, 11))], sums)
    return grad_inputs, sums[0].T, sums[1].T, sums[2]


def solution(mesh):
    tok = P(AXES, None)
    return jax.shard_map(
        block,
        mesh=mesh,
        in_specs=(tok, P("fs", "tp"), P("fs", "tp"), P("tp", "fs"), tok),
        out_specs=(tok, P("fs", "tp"), P("fs", "tp"), P("tp", "fs")),
        check_vma=False,
    )
```

```python
import functools

import jax
import jax.numpy as jnp
from jax import lax
from jax.experimental import pallas as pl
from jax.experimental.pallas import tpu as pltpu
from jax.sharding import PartitionSpec as P


AXES = ("rep", "fs", "tp")
BF, F32, F16 = jnp.bfloat16, jnp.float32, jnp.float16
W_MAX = 0.09375
ANY = pl.BlockSpec(memory_space=pl.ANY)
VMEM = pl.BlockSpec(memory_space=pltpu.VMEM)
LIMIT = 56 * 1024 * 1024

ROWS, DEPTH, UNITS = 32, 1024, 688
TOK, WIDE = 16 * ROWS, 4 * DEPTH
CUT = 336
LOW = 1040
HALF = 2 * DEPTH
TAIL = 128


def index_of(x, c, z, y):
    x, z, y = x % 4, z % 4, y % 4
    return (x // 2) * 64 + ((x % 2) * 2 + c) * 16 + z * 4 + y


def moved(array, dx=0, flip=0, dz=0, dy=0):
    pairs = []
    for x in range(4):
        for c in range(2):
            for z in range(4):
                for y in range(4):
                    pairs.append((index_of(x + dx, c ^ flip, z + dz, y + dy), index_of(x, c, z, y)))
    return lax.ppermute(array, AXES, pairs)


def dot(a, b, ca, cb):
    return lax.dot_general(a, b, (((ca,), (cb,)), ((), ())), preferred_element_type=F32)


def place():
    tp = lax.axis_index("tp")
    return tp // 4, tp % 4


def call(body, out_shape, scratch, flops, ins, outs, args, nbytes):
    return pl.pallas_call(
        body,
        out_shape=out_shape,
        in_specs=ins,
        out_specs=outs,
        scratch_shapes=scratch,
        compiler_params=pltpu.CompilerParams(vmem_limit_bytes=LIMIT),
        cost_estimate=pl.CostEstimate(flops=flops, bytes_accessed=nbytes, transcendentals=0),
    )(*args)


FROM = ((0, 0, 4, 0), (1, 0, 4, 1), (2, 0, 4, 3), (3, 0, 2, 2), (4, 2, 2, 2))


def forward_kernel(*refs):
    xs, ds, was, wbs = refs[:5], refs[5:10], refs[10:14], refs[14:18]
    acts, side, x_own, d_own = refs[18:22]
    v, w, sums, act, sx, sd, sw, so = refs[22:]
    z, y = place()
    x_copies, d_copies = [], []
    for i, first, count, off in FROM:
        for j in range(count):
            row = pl.multiple_of((lax.rem(z + first + j, 4) * 4 + lax.rem(y + off, 4)) * ROWS, ROWS)
            x_copies.append(
                pltpu.make_async_copy(xs[i].at[j], v.at[0, pl.ds(row, ROWS)], sx.at[len(x_copies)]))
            row = pl.multiple_of((lax.rem(z + off, 4) * 4 + lax.rem(y + first + j, 4)) * ROWS, ROWS)
            d_copies.append(
                pltpu.make_async_copy(ds[i].at[j], v.at[1, pl.ds(row, ROWS)], sd.at[len(d_copies)]))
    rest = UNITS - CUT
    w_copies = [
        [
            pltpu.make_async_copy(was[k].at[pl.ds(0, UNITS)], w.at[k, 0], sw.at[4 * k]),
            pltpu.make_async_copy(wbs[k].at[pl.ds(0, UNITS)], w.at[k, 1], sw.at[4 * k + 1]),
            pltpu.make_async_copy(was[k].at[pl.ds(UNITS, CUT)], w.at[k, 2, pl.ds(0, CUT)], sw.at[4 * k + 2]),
            pltpu.make_async_copy(wbs[k].at[pl.ds(UNITS, rest)], w.at[k, 2, pl.ds(CUT, rest)], sw.at[4 * k + 3]),
        ]
        for k in range(4)
    ]
    stages = [x_copies + w_copies[0][:2], d_copies + w_copies[0][2:], w_copies[1], w_copies[2], w_copies[3]]

    def begin(n):
        for c in stages[n]:
            c.start()

    def end(n):
        for c in stages[n]:
            c.wait()

    begin(0)
    begin(1)
    end(0)
    begin(2)
    for i in range(2):
        sums[i] = dot(w[0, i], v[0, :, :DEPTH], 1, 1)
    end(1)
    begin(3)
    sums[2] = dot(w[0, 2], v[1, :, :DEPTH], 1, 1)
    end(2)
    begin(4)
    outs = []
    for i, to in enumerate((x_own, d_own)):
        outs.append(pltpu.make_async_copy(v.at[i, :, pl.ds(0, DEPTH)], to, so.at[i]))
        for h in range(2):
            outs.append(pltpu.make_async_copy(
                v.at[i, :, pl.ds(DEPTH + h * TOK, TOK)],
                side.at[pl.ds(3 * UNITS + (2 * i + h) * TOK, TOK)], so.at[2 + 2 * i + h]))
    for k in (1, 2, 3):
        if k > 1:
            end(k + 1)
        if k == 3:
            for c in outs:
                c.start()

        def product(i, _):
            sums[i] = sums[i] + dot(w[k, i], v[i // 2, :, k * DEPTH:(k + 1) * DEPTH], 1, 1)
            return 0

        lax.fori_loop(0, 3, product, 0)

    def unit(i, _):
        r = pl.ds(pl.multiple_of(i * 16, 16), 16)
        g = sums[0, r, :].astype(BF).astype(F32)
        u = sums[1, r, :].astype(BF).astype(F32)
        b = sums[2, r, :].astype(BF).astype(F32)
        sigma = 1.0 / (1.0 + jnp.exp(-g))
        active = g * sigma
        act[r, :] = (b * u * sigma * (1.0 + g * (1.0 - sigma))).astype(BF)
        act[pl.ds(pl.multiple_of(UNITS + i * 16, 16), 16), :] = (b * active).astype(BF)
        act[pl.ds(pl.multiple_of(2 * UNITS + i * 16, 16), 16), :] = (active * u).astype(BF)
        return 0

    lax.fori_loop(0, UNITS // 16, unit, 0)
    outs.append(pltpu.make_async_copy(act, acts, so.at[6]))
    outs.append(pltpu.make_async_copy(act, side.at[pl.ds(0, 3 * UNITS)], so.at[7]))
    for c in outs[-2:]:
        c.start()
    for c in outs:
        c.wait()


def forward(xs, ds, was, wbs):
    shape = jax.ShapeDtypeStruct
    return call(
        forward_kernel,
        (shape((3 * UNITS, TOK), BF), shape((3 * UNITS + 4 * TOK, TOK), BF), shape((TOK, DEPTH), BF), shape((TOK, DEPTH), BF)),
        [
            pltpu.VMEM((2, TOK, WIDE), BF), pltpu.VMEM((4, 3, UNITS, DEPTH), BF), pltpu.VMEM((3, UNITS, TOK), F32),
            pltpu.VMEM((3 * UNITS, TOK), BF),
            pltpu.SemaphoreType.DMA((16,)), pltpu.SemaphoreType.DMA((16,)),
            pltpu.SemaphoreType.DMA((16,)), pltpu.SemaphoreType.DMA((8,)),
        ],
        2 * TOK * WIDE * UNITS * 3,
        [ANY] * 18,
        (ANY,) * 4,
        (*xs, *ds, *was, *wbs),
        34 << 20,
    )


def input_kernel(*refs):
    acts, was, wbs = refs[0], refs[1:5], refs[5:9]
    own, away = refs[9:11], refs[11:13]
    wa, wb, tg, tu, total, expo, sw, so, st = refs[13:]
    z, y = place()
    copies = [
        (pltpu.make_async_copy(was[k].at[pl.ds(0, UNITS)], wa.at[k], sw.at[2 * k]),
         pltpu.make_async_copy(wbs[k].at[pl.ds(0, UNITS)], wb.at[k], sw.at[2 * k + 1]))
        for k in range(4)
    ]
    for pair in copies[:2]:
        for c in pair:
            c.start()
    tg[...] = acts[:UNITS, :].T
    tu[...] = acts[UNITS:2 * UNITS, :].T
    norm = jnp.sum(jnp.abs(tg[...].astype(F32)), axis=1, keepdims=True)
    norm = norm + jnp.sum(jnp.abs(tu[...].astype(F32)), axis=1, keepdims=True)
    e = jnp.ceil(jnp.log2(jnp.maximum(norm * (1.02 * W_MAX), 1e-30)))
    expo[...] = jnp.broadcast_to(e, (TOK, TAIL))

    def puts(src, side, cols, sems):
        out, n = [], 0
        for s in range(4):
            for i in range(4):
                zz, yy = (lax.rem(z + s, 4), i) if side == 0 else (i, lax.rem(y + s, 4))
                r = pl.ds(pl.multiple_of((zz * 4 + yy) * ROWS, ROWS), ROWS)
                to = own[side] if s == 0 else away[side].at[s - 1]
                out.append(pltpu.make_async_copy(src.at[r], to.at[pl.ds(i * ROWS, ROWS), cols], sems.at[n]))
                n += 1
        return out

    tails = [c for side in range(2) for c in puts(expo, side, pl.ds(HALF, TAIL), st.at[side])]
    for c in tails:
        c.start()
    pending = [None, None]
    for k in range(4):
        for c in copies[k]:
            c.wait()
        if k + 2 < 4:
            for c in copies[k + 2]:
                c.start()
        if pending[k % 2]:
            for c in pending[k % 2]:
                c.wait()

        def tile(j, _):
            n = pl.ds(pl.multiple_of(j * 512, 512), 512)
            v = dot(tg[...], wa[k, :, n], 1, 0) + dot(tu[...], wb[k, :, n], 1, 0)
            total[k % 2, :, n] = v * jnp.exp2(14.0 - expo[:, :1])
            return 0

        lax.fori_loop(0, 2, tile, 0)
        pending[k % 2] = puts(total.at[k % 2], k // 2, pl.ds((k % 2) * DEPTH, DEPTH), so.at[k % 2])
        for c in pending[k % 2]:
            c.start()
    for c in pending[0] + pending[1] + tails:
        c.wait()


def input_sums(acts, was, wbs):
    shape = jax.ShapeDtypeStruct
    own, away = shape((4 * ROWS, HALF + TAIL), F32), shape((3, 4 * ROWS, HALF + TAIL), F32)
    return call(
        input_kernel,
        (own, own, away, away),
        [
            pltpu.VMEM((4, UNITS, DEPTH), BF), pltpu.VMEM((4, UNITS, DEPTH), BF),
            pltpu.VMEM((TOK, UNITS), BF), pltpu.VMEM((TOK, UNITS), BF),
            pltpu.VMEM((2, TOK, DEPTH), F32), pltpu.VMEM((TOK, TAIL), F32),
            pltpu.SemaphoreType.DMA((8,)), pltpu.SemaphoreType.DMA((2, 16)), pltpu.SemaphoreType.DMA((2, 16)),
        ],
        2 * TOK * WIDE * UNITS * 2,
        [VMEM] + [ANY] * 8,
        (ANY,) * 4,
        (acts, *was, *wbs),
        22 << 20,
    )


def join_kernel(own_a, own_b, got, to_a, to_b):
    z, y = place()
    for own, first, to, at in ((own_a, 0, to_a, y), (own_b, 3, to_b, z)):
        for s in range(4):
            r = pl.ds(pl.multiple_of(lax.rem(at + s, 4) * ROWS, ROWS), ROWS)
            v = own[r, :HALF] * jnp.exp2(own[r, HALF:HALF + 1] - 14.0)
            for i in range(first, first + 3):
                v = v + got[i, r, :HALF] * jnp.exp2(got[i, r, HALF:HALF + 1] - 14.0)
            to[s] = v


def joined(own_a, own_b, got):
    out = jax.ShapeDtypeStruct((4, ROWS, HALF), F32)
    return call(join_kernel, (out, out), [], 1 << 30, [VMEM] * 3, (VMEM,) * 2, (own_a, own_b, got), 12 << 20)


def weight_kernel(acts, n_acts, columns, has_base, n_in, *refs):
    ins, outs = refs[:n_in], refs[n_in:n_in + 3]
    a, xc, dc, total, sa, sc, sb, so = refs[n_in + 3:]
    z, y = place()
    stages = [[], [], []]
    n = 0
    for g, pieces in enumerate(acts):
        for i, r0, r1 in pieces:
            for s in range(3):
                lo, hi = max(r0, s * UNITS), min(r1, (s + 1) * UNITS)
                if lo < hi:
                    stages[s].append(pltpu.make_async_copy(
                        ins[i].at[pl.ds(lo - r0, hi - lo)], a.at[pl.ds(lo, hi - lo), pl.ds(g * TOK, TOK)], sa.at[n]))
                    n += 1
    columns(ins[n_acts:], z, y, lambda src, to: stages[0].append(
        pltpu.make_async_copy(src, to, sc.at[0, len(stages[0])])), xc, 0)
    columns(ins[n_acts:], z, y, lambda src, to: stages[2].append(
        pltpu.make_async_copy(src, to, sc.at[1, len(stages[2])])), dc, 1)
    if has_base:
        for s in range(3):
            stages[s].append(pltpu.make_async_copy(ins[n_in - 3 + s], total.at[s], sb.at[s]))

    def begin(s):
        for c in stages[s]:
            c.start()

    begin(0)
    begin(1)
    done = []
    for i in range(3):
        for c in stages[i]:
            c.wait()
        if i == 0:
            begin(2)
        cols = dc if i == 2 else xc
        v = dot(a[i * UNITS:(i + 1) * UNITS, :], cols[...].reshape(len(acts) * TOK, DEPTH), 1, 0)
        total[i] = total[i] + v if has_base else v
        done.append(pltpu.make_async_copy(total.at[i], outs[i], so.at[i]))
        done[-1].start()
    for c in done:
        c.wait()


def near_columns(refs, z, y, add, buf, kind):
    x_own, d_own, side = refs[:3]
    add(d_own if kind else x_own, buf.at[0])
    for h in range(2):
        add(side.at[pl.ds(3 * UNITS + (2 * kind + h) * TOK, TOK)], buf.at[1, :, pl.ds(h * TOK, TOK)])


def plane_columns(first_group, count, refs, z, y, add, buf, kind):
    for i, first, n, off in FROM:
        for j in range(n):
            a, b = lax.rem(z + first + j, 4), lax.rem(y + off, 4)
            if kind:
                a, b = lax.rem(z + off, 4), lax.rem(y + first + j, 4)
            add(refs[5 * kind + i].at[j, pl.ds(first_group, count)], buf.at[:, a * 4 + b])


def weight_sums(groups, columns, arrays, base):
    ins, acts = [], []
    for pieces in groups:
        row, marks = 0, []
        for p, m in pieces:
            marks.append((len(ins), row, row + m))
            ins.append(p)
            row += m
        acts.append(marks)
    n_acts = len(ins)
    ins += list(arrays) + list(base or [])
    n = len(groups)
    col = (n, TOK, DEPTH) if columns is near_columns else (n, 16, ROWS, DEPTH)
    out = jax.ShapeDtypeStruct((UNITS, DEPTH), F32)
    return call(
        functools.partial(weight_kernel, acts, n_acts, columns, base is not None, len(ins)),
        (out,) * 3,
        [
            pltpu.VMEM((3 * UNITS, n * TOK), BF), pltpu.VMEM(col, BF), pltpu.VMEM(col, BF),
            pltpu.VMEM((3, UNITS, DEPTH), F32),
            pltpu.SemaphoreType.DMA((3 * n_acts,)), pltpu.SemaphoreType.DMA((2, 32)),
            pltpu.SemaphoreType.DMA((3,)), pltpu.SemaphoreType.DMA((3,)),
        ],
        2 * 3 * UNITS * DEPTH * n * TOK,
        [ANY] * len(ins),
        (ANY,) * 3,
        ins,
        n * (4 << 20) + (16 << 20),
    )


def block(inputs, w_gate, w_up, w_down, d_out):
    fs = lax.axis_index("fs")

    def relative(v):
        parts = [v[:, i * DEPTH:(i + 1) * DEPTH] for i in range(4)]
        out = []
        for k in range(4):
            w = parts[k]
            for f in range(1, 4):
                w = jnp.where(fs == f, parts[f ^ k], w)
            out.append(w)
        return out

    xp, dp = relative(inputs), relative(d_out)
    x_own, d_own = jnp.concatenate(xp, axis=1), jnp.concatenate(dp, axis=1)

    def spread(own, first, second):
        line = jnp.concatenate(
            [own[None]] + [moved(own[None], **{first: d}) for d in (1, 2, 3)], axis=0)
        up, down = moved(line, **{second: 1}), moved(line, **{second: -1})
        low, high = up[:2], down[2:]
        return line, up, down, moved(low, **{second: 1}), moved(high, **{second: -1})

    xs = spread(x_own, "dz", "dy")
    ds = spread(d_own, "dy", "dz")

    side = moved(jnp.stack([xp[1], dp[1], xp[3], dp[3]]), flip=1)
    far = jnp.stack([xp[0], side[0], dp[0], side[1]])
    near = jnp.stack([xp[2], side[2], dp[2], side[3]])
    got = (moved(near, dx=1), moved(near, dx=-1), moved(far, dx=2))
    xcs = spread(jnp.concatenate([v[:2] for v in got], axis=0), "dz", "dy")
    dcs = spread(jnp.concatenate([v[2:] for v in got], axis=0), "dy", "dz")

    wa = jnp.concatenate([w_gate.T, w_down[:CUT]], axis=0)
    wb = jnp.concatenate([w_up.T, w_down[CUT:]], axis=0)
    wa2, wb2 = moved(wa, dx=1), moved(wb, dx=-1)
    wa1, wb1 = moved(wa, flip=1), moved(wb, flip=1)
    wa3, wb3 = moved(wa2, flip=1), moved(wb2, flip=1)
    was, wbs = (wa, wa1, wa2, wa3), (wb, wb1, wb2, wb3)

    acts, side, x_cols, d_cols = forward(xs, ds, was, wbs)

    am, ap = moved(acts, dx=1), moved(acts, dx=-1)
    side = moved(side, flip=1)
    low, high = am[:LOW], ap[LOW:]
    oa, ob = moved(low, dx=1), moved(high, dx=-1)
    sm, sp = moved(am, flip=1), moved(ap, flip=1)
    soa, sob = moved(oa, flip=1), moved(ob, flip=1)

    own_a, own_b, qa, qb = input_sums(acts, was, wbs)
    qa, qb = qa.astype(F16), qb.astype(F16)
    got = [moved(qa[d - 1], dz=-d) for d in (1, 2, 3)] + [moved(qb[d - 1], dy=-d) for d in (1, 2, 3)]
    got = jnp.stack(got).astype(F32)
    fa, fb = joined(own_a, own_b, got)
    fa = fa[0] + moved(fa[1], dy=-1) + moved(fa[2], dy=-2) + moved(fa[3], dy=-3)
    fb = fb[0] + moved(fb[1], dz=-1) + moved(fb[2], dz=-2) + moved(fb[3], dz=-3)
    grad_inputs = jnp.concatenate(relative(jnp.concatenate([fa, fb], axis=1).astype(BF)), axis=1)

    full = 3 * UNITS
    sums = weight_sums(
        [[(acts, full)], [(side, full)]], near_columns, (x_cols, d_cols, side), None)
    sums = weight_sums(
        [[(am, full)], [(sm, full)], [(ap, full)], [(sp, full)]],
        functools.partial(plane_columns, 0, 4), (*xcs, *dcs), sums)
    sums = weight_sums(
        [[(oa, LOW), (ob, full - LOW)], [(soa, LOW), (sob, full - LOW)]],
        functools.partial(plane_columns, 4, 2), (*xcs, *dcs), sums)
    return grad_inputs, sums[0].T, sums[1].T, sums[2]


def solution(mesh):
    tok = P(AXES, None)
    return jax.shard_map(
        block,
        mesh=mesh,
        in_specs=(tok, P("fs", "tp"), P("fs", "tp"), P("tp", "fs"), tok),
        out_specs=(tok, P("fs", "tp"), P("fs", "tp"), P("tp", "fs")),
        check_vma=False,
    )
```

```python
import functools

import jax
import jax.numpy as jnp
from jax import lax
from jax.experimental import pallas as pl
from jax.experimental.pallas import tpu as pltpu
from jax.sharding import PartitionSpec as P


AXES = ("rep", "fs", "tp")
BF, F32, F16 = jnp.bfloat16, jnp.float32, jnp.float16
W_MAX = 0.09375
ANY = pl.BlockSpec(memory_space=pl.ANY)
VMEM = pl.BlockSpec(memory_space=pltpu.VMEM)
LIMIT = 56 * 1024 * 1024

ROWS, DEPTH, UNITS = 32, 1024, 688
TOK, WIDE = 16 * ROWS, 4 * DEPTH
CUT = 336
LOW = 1040
TAIL = 128


def index_of(x, c, z, y):
    x, z, y = x % 4, z % 4, y % 4
    return (x // 2) * 64 + ((x % 2) * 2 + c) * 16 + z * 4 + y


def moved(array, dx=0, flip=0, dz=0, dy=0):
    pairs = []
    for x in range(4):
        for c in range(2):
            for z in range(4):
                for y in range(4):
                    pairs.append((index_of(x + dx, c ^ flip, z + dz, y + dy), index_of(x, c, z, y)))
    return lax.ppermute(array, AXES, pairs)


def dot(a, b, ca, cb):
    return lax.dot_general(a, b, (((ca,), (cb,)), ((), ())), preferred_element_type=F32)


def place():
    tp = lax.axis_index("tp")
    return tp // 4, tp % 4


def call(body, out_shape, scratch, flops, ins, outs, args, nbytes):
    return pl.pallas_call(
        body,
        out_shape=out_shape,
        in_specs=ins,
        out_specs=outs,
        scratch_shapes=scratch,
        compiler_params=pltpu.CompilerParams(vmem_limit_bytes=LIMIT),
        cost_estimate=pl.CostEstimate(flops=flops, bytes_accessed=nbytes, transcendentals=0),
    )(*args)


FROM = ((0, 0, 4, 0), (1, 0, 4, 1), (2, 0, 4, 3), (3, 0, 2, 2), (4, 2, 2, 2))


def forward_kernel(*refs):
    xs, ds, was, wbs = refs[:5], refs[5:10], refs[10:14], refs[14:18]
    acts, side, x_own, d_own = refs[18:22]
    v, w, sums, act, sx, sd, sw, so = refs[22:]
    z, y = place()
    x_copies, d_copies = [], []
    for i, first, count, off in FROM:
        for j in range(count):
            row = pl.multiple_of((lax.rem(z + first + j, 4) * 4 + lax.rem(y + off, 4)) * ROWS, ROWS)
            x_copies.append(
                pltpu.make_async_copy(xs[i].at[j], v.at[0, pl.ds(row, ROWS)], sx.at[len(x_copies)]))
            row = pl.multiple_of((lax.rem(z + off, 4) * 4 + lax.rem(y + first + j, 4)) * ROWS, ROWS)
            d_copies.append(
                pltpu.make_async_copy(ds[i].at[j], v.at[1, pl.ds(row, ROWS)], sd.at[len(d_copies)]))
    rest = UNITS - CUT
    w_copies = [
        [
            pltpu.make_async_copy(was[k].at[pl.ds(0, UNITS)], w.at[k, 0], sw.at[4 * k]),
            pltpu.make_async_copy(wbs[k].at[pl.ds(0, UNITS)], w.at[k, 1], sw.at[4 * k + 1]),
            pltpu.make_async_copy(was[k].at[pl.ds(UNITS, CUT)], w.at[k, 2, pl.ds(0, CUT)], sw.at[4 * k + 2]),
            pltpu.make_async_copy(wbs[k].at[pl.ds(UNITS, rest)], w.at[k, 2, pl.ds(CUT, rest)], sw.at[4 * k + 3]),
        ]
        for k in range(4)
    ]
    stages = [x_copies + w_copies[0][:2], d_copies + w_copies[0][2:], w_copies[1], w_copies[2], w_copies[3]]

    def begin(n):
        for c in stages[n]:
            c.start()

    def end(n):
        for c in stages[n]:
            c.wait()

    begin(0)
    begin(1)
    end(0)
    begin(2)
    for i in range(2):
        sums[i] = dot(w[0, i], v[0, :, :DEPTH], 1, 1)
    end(1)
    begin(3)
    sums[2] = dot(w[0, 2], v[1, :, :DEPTH], 1, 1)
    end(2)
    begin(4)
    outs = []
    for i, to in enumerate((x_own, d_own)):
        outs.append(pltpu.make_async_copy(v.at[i, :, pl.ds(0, DEPTH)], to, so.at[i]))
        for h in range(2):
            outs.append(pltpu.make_async_copy(
                v.at[i, :, pl.ds(DEPTH + h * TOK, TOK)],
                side.at[pl.ds(3 * UNITS + (2 * i + h) * TOK, TOK)], so.at[2 + 2 * i + h]))
    for k in (1, 2, 3):
        if k > 1:
            end(k + 1)
        if k == 3:
            for c in outs:
                c.start()

        def product(i, _):
            sums[i] = sums[i] + dot(w[k, i], v[i // 2, :, k * DEPTH:(k + 1) * DEPTH], 1, 1)
            return 0

        lax.fori_loop(0, 3, product, 0)

    def unit(i, _):
        r = pl.ds(pl.multiple_of(i * 16, 16), 16)
        g = sums[0, r, :].astype(BF).astype(F32)
        u = sums[1, r, :].astype(BF).astype(F32)
        b = sums[2, r, :].astype(BF).astype(F32)
        sigma = 1.0 / (1.0 + jnp.exp(-g))
        active = g * sigma
        act[r, :] = (b * u * sigma * (1.0 + g * (1.0 - sigma))).astype(BF)
        act[pl.ds(pl.multiple_of(UNITS + i * 16, 16), 16), :] = (b * active).astype(BF)
        act[pl.ds(pl.multiple_of(2 * UNITS + i * 16, 16), 16), :] = (active * u).astype(BF)
        return 0

    lax.fori_loop(0, UNITS // 16, unit, 0)
    outs.append(pltpu.make_async_copy(act, acts, so.at[6]))
    outs.append(pltpu.make_async_copy(act, side.at[pl.ds(0, 3 * UNITS)], so.at[7]))
    for c in outs[-2:]:
        c.start()
    for c in outs:
        c.wait()


def forward(xs, ds, was, wbs):
    shape = jax.ShapeDtypeStruct
    return call(
        forward_kernel,
        (shape((3 * UNITS, TOK), BF), shape((3 * UNITS + 4 * TOK, TOK), BF), shape((TOK, DEPTH), BF), shape((TOK, DEPTH), BF)),
        [
            pltpu.VMEM((2, TOK, WIDE), BF), pltpu.VMEM((4, 3, UNITS, DEPTH), BF), pltpu.VMEM((3, UNITS, TOK), F32),
            pltpu.VMEM((3 * UNITS, TOK), BF),
            pltpu.SemaphoreType.DMA((16,)), pltpu.SemaphoreType.DMA((16,)),
            pltpu.SemaphoreType.DMA((16,)), pltpu.SemaphoreType.DMA((8,)),
        ],
        2 * TOK * WIDE * UNITS * 3,
        [ANY] * 18,
        (ANY,) * 4,
        (*xs, *ds, *was, *wbs),
        34 << 20,
    )


def input_kernel(*refs):
    acts, was, wbs, out = refs[0], refs[1:5], refs[5:9], refs[9]
    wa, wb, tg, tu, total, expo, sw, so = refs[10:]
    copies = [
        (pltpu.make_async_copy(was[k].at[pl.ds(0, UNITS)], wa.at[k], sw.at[2 * k]),
         pltpu.make_async_copy(wbs[k].at[pl.ds(0, UNITS)], wb.at[k], sw.at[2 * k + 1]))
        for k in range(4)
    ]
    for pair in copies[:2]:
        for c in pair:
            c.start()
    tg[...] = acts[:UNITS, :].T
    tu[...] = acts[UNITS:2 * UNITS, :].T
    norm = jnp.sum(jnp.abs(tg[...].astype(F32)), axis=1, keepdims=True)
    norm = norm + jnp.sum(jnp.abs(tu[...].astype(F32)), axis=1, keepdims=True)
    e = jnp.ceil(jnp.log2(jnp.maximum(norm * (1.02 * W_MAX), 1e-30)))
    expo[...] = jnp.broadcast_to(e, (TOK, TAIL))
    puts = [pltpu.make_async_copy(expo, out.at[:, pl.ds(WIDE, TAIL)], so.at[4])]
    puts[0].start()
    for k in range(4):
        for c in copies[k]:
            c.wait()
        if k + 2 < 4:
            for c in copies[k + 2]:
                c.start()
        if k >= 2:
            puts[k - 1].wait()

        def tile(j, _):
            n = pl.ds(pl.multiple_of(j * 512, 512), 512)
            v = dot(tg[...], wa[k, :, n], 1, 0) + dot(tu[...], wb[k, :, n], 1, 0)
            total[k % 2, :, n] = v * jnp.exp2(14.0 - expo[:, :1])
            return 0

        lax.fori_loop(0, 2, tile, 0)
        puts.append(pltpu.make_async_copy(total.at[k % 2], out.at[:, pl.ds(k * DEPTH, DEPTH)], so.at[k]))
        puts[-1].start()
    for c in (puts[0], puts[3], puts[4]):
        c.wait()


def input_sums(acts, was, wbs):
    return call(
        input_kernel,
        jax.ShapeDtypeStruct((TOK, WIDE + TAIL), F32),
        [
            pltpu.VMEM((4, UNITS, DEPTH), BF), pltpu.VMEM((4, UNITS, DEPTH), BF),
            pltpu.VMEM((TOK, UNITS), BF), pltpu.VMEM((TOK, UNITS), BF),
            pltpu.VMEM((2, TOK, DEPTH), F32), pltpu.VMEM((TOK, TAIL), F32),
            pltpu.SemaphoreType.DMA((8,)), pltpu.SemaphoreType.DMA((5,)),
        ],
        2 * TOK * WIDE * UNITS * 2,
        [VMEM] + [ANY] * 8,
        ANY,
        (acts, *was, *wbs),
        22 << 20,
    )


def sum_kernel(got, out):
    v = None
    for i in range(16):
        w = got[i, :, :WIDE] * jnp.exp2(got[i, :, WIDE:WIDE + 1] - 14.0)
        v = w if v is None else v + w
    out[...] = v


def summed(got):
    return pl.pallas_call(
        sum_kernel,
        grid=(ROWS // 8,),
        out_shape=jax.ShapeDtypeStruct((ROWS, WIDE), F32),
        in_specs=[pl.BlockSpec((16, 8, WIDE + TAIL), lambda i: (0, i, 0))],
        out_specs=pl.BlockSpec((8, WIDE), lambda i: (i, 0)),
        compiler_params=pltpu.CompilerParams(vmem_limit_bytes=LIMIT),
        cost_estimate=pl.CostEstimate(flops=1 << 28, bytes_accessed=9 << 20, transcendentals=0),
    )(got)


def weight_kernel(acts, n_acts, columns, has_base, n_in, *refs):
    ins, outs = refs[:n_in], refs[n_in:n_in + 3]
    a, xc, dc, total, sa, sc, sb, so = refs[n_in + 3:]
    z, y = place()
    stages = [[], [], []]
    n = 0
    for g, pieces in enumerate(acts):
        for i, r0, r1 in pieces:
            for s in range(3):
                lo, hi = max(r0, s * UNITS), min(r1, (s + 1) * UNITS)
                if lo < hi:
                    stages[s].append(pltpu.make_async_copy(
                        ins[i].at[pl.ds(lo - r0, hi - lo)], a.at[pl.ds(lo, hi - lo), pl.ds(g * TOK, TOK)], sa.at[n]))
                    n += 1
    columns(ins[n_acts:], z, y, lambda src, to: stages[0].append(
        pltpu.make_async_copy(src, to, sc.at[0, len(stages[0])])), xc, 0)
    columns(ins[n_acts:], z, y, lambda src, to: stages[2].append(
        pltpu.make_async_copy(src, to, sc.at[1, len(stages[2])])), dc, 1)
    if has_base:
        for s in range(3):
            stages[s].append(pltpu.make_async_copy(ins[n_in - 3 + s], total.at[s], sb.at[s]))

    def begin(s):
        for c in stages[s]:
            c.start()

    begin(0)
    begin(1)
    done = []
    for i in range(3):
        for c in stages[i]:
            c.wait()
        if i == 0:
            begin(2)
        cols = dc if i == 2 else xc
        v = dot(a[i * UNITS:(i + 1) * UNITS, :], cols[...].reshape(len(acts) * TOK, DEPTH), 1, 0)
        total[i] = total[i] + v if has_base else v
        done.append(pltpu.make_async_copy(total.at[i], outs[i], so.at[i]))
        done[-1].start()
    for c in done:
        c.wait()


def near_columns(refs, z, y, add, buf, kind):
    x_own, d_own, side = refs[:3]
    add(d_own if kind else x_own, buf.at[0])
    for h in range(2):
        add(side.at[pl.ds(3 * UNITS + (2 * kind + h) * TOK, TOK)], buf.at[1, :, pl.ds(h * TOK, TOK)])


def plane_columns(first_group, count, refs, z, y, add, buf, kind):
    for i, first, n, off in FROM:
        for j in range(n):
            a, b = lax.rem(z + first + j, 4), lax.rem(y + off, 4)
            if kind:
                a, b = lax.rem(z + off, 4), lax.rem(y + first + j, 4)
            add(refs[5 * kind + i].at[j, pl.ds(first_group, count)], buf.at[:, a * 4 + b])


def weight_sums(groups, columns, arrays, base):
    ins, acts = [], []
    for pieces in groups:
        row, marks = 0, []
        for p, m in pieces:
            marks.append((len(ins), row, row + m))
            ins.append(p)
            row += m
        acts.append(marks)
    n_acts = len(ins)
    ins += list(arrays) + list(base or [])
    n = len(groups)
    col = (n, TOK, DEPTH) if columns is near_columns else (n, 16, ROWS, DEPTH)
    out = jax.ShapeDtypeStruct((UNITS, DEPTH), F32)
    return call(
        functools.partial(weight_kernel, acts, n_acts, columns, base is not None, len(ins)),
        (out,) * 3,
        [
            pltpu.VMEM((3 * UNITS, n * TOK), BF), pltpu.VMEM(col, BF), pltpu.VMEM(col, BF),
            pltpu.VMEM((3, UNITS, DEPTH), F32),
            pltpu.SemaphoreType.DMA((3 * n_acts,)), pltpu.SemaphoreType.DMA((2, 32)),
            pltpu.SemaphoreType.DMA((3,)), pltpu.SemaphoreType.DMA((3,)),
        ],
        2 * 3 * UNITS * DEPTH * n * TOK,
        [ANY] * len(ins),
        (ANY,) * 3,
        ins,
        n * (4 << 20) + (16 << 20),
    )


def block(inputs, w_gate, w_up, w_down, d_out):
    fs = lax.axis_index("fs")

    def relative(v):
        parts = [v[:, i * DEPTH:(i + 1) * DEPTH] for i in range(4)]
        out = []
        for k in range(4):
            w = parts[k]
            for f in range(1, 4):
                w = jnp.where(fs == f, parts[f ^ k], w)
            out.append(w)
        return out

    xp, dp = relative(inputs), relative(d_out)
    x_own, d_own = jnp.concatenate(xp, axis=1), jnp.concatenate(dp, axis=1)

    def spread(own, first, second):
        line = jnp.concatenate(
            [own[None]] + [moved(own[None], **{first: d}) for d in (1, 2, 3)], axis=0)
        up, down = moved(line, **{second: 1}), moved(line, **{second: -1})
        low, high = up[:2], down[2:]
        return line, up, down, moved(low, **{second: 1}), moved(high, **{second: -1})

    xs = spread(x_own, "dz", "dy")
    ds = spread(d_own, "dy", "dz")

    side = moved(jnp.stack([xp[1], dp[1], xp[3], dp[3]]), flip=1)
    far = jnp.stack([xp[0], side[0], dp[0], side[1]])
    near = jnp.stack([xp[2], side[2], dp[2], side[3]])
    got = (moved(near, dx=1), moved(near, dx=-1), moved(far, dx=2))
    xcs = spread(jnp.concatenate([v[:2] for v in got], axis=0), "dz", "dy")
    dcs = spread(jnp.concatenate([v[2:] for v in got], axis=0), "dy", "dz")

    wa = jnp.concatenate([w_gate.T, w_down[:CUT]], axis=0)
    wb = jnp.concatenate([w_up.T, w_down[CUT:]], axis=0)
    wa2, wb2 = moved(wa, dx=1), moved(wb, dx=-1)
    wa1, wb1 = moved(wa, flip=1), moved(wb, flip=1)
    wa3, wb3 = moved(wa2, flip=1), moved(wb2, flip=1)
    was, wbs = (wa, wa1, wa2, wa3), (wb, wb1, wb2, wb3)

    acts, side, x_cols, d_cols = forward(xs, ds, was, wbs)

    am, ap = moved(acts, dx=1), moved(acts, dx=-1)
    side = moved(side, flip=1)
    low, high = am[:LOW], ap[LOW:]
    oa, ob = moved(low, dx=1), moved(high, dx=-1)
    sm, sp = moved(am, flip=1), moved(ap, flip=1)
    soa, sob = moved(oa, flip=1), moved(ob, flip=1)

    packed = input_sums(acts, was, wbs).astype(F16)
    got = lax.all_to_all(packed.reshape(16, ROWS, WIDE + TAIL), "tp", 0, 0)
    grad_inputs = jnp.concatenate(relative(summed(got.astype(F32)).astype(BF)), axis=1)

    full = 3 * UNITS
    sums = weight_sums(
        [[(acts, full)], [(side, full)]], near_columns, (x_cols, d_cols, side), None)
    sums = weight_sums(
        [[(am, full)], [(sm, full)], [(ap, full)], [(sp, full)]],
        functools.partial(plane_columns, 0, 4), (*xcs, *dcs), sums)
    sums = weight_sums(
        [[(oa, LOW), (ob, full - LOW)], [(soa, LOW), (sob, full - LOW)]],
        functools.partial(plane_columns, 4, 2), (*xcs, *dcs), sums)
    return grad_inputs, sums[0].T, sums[1].T, sums[2]


def solution(mesh):
    tok = P(AXES, None)
    return jax.shard_map(
        block,
        mesh=mesh,
        in_specs=(tok, P("fs", "tp"), P("fs", "tp"), P("tp", "fs"), tok),
        out_specs=(tok, P("fs", "tp"), P("fs", "tp"), P("tp", "fs")),
        check_vma=False,
    )
```

```python
import functools

import jax
import jax.numpy as jnp
from jax import lax
from jax.experimental import pallas as pl
from jax.experimental.pallas import tpu as pltpu
from jax.sharding import PartitionSpec as P


AXES = ("rep", "fs", "tp")
BF, F32, F16 = jnp.bfloat16, jnp.float32, jnp.float16
W_MAX = 0.09375
ANY = pl.BlockSpec(memory_space=pl.ANY)
VMEM = pl.BlockSpec(memory_space=pltpu.VMEM)
LIMIT = 56 * 1024 * 1024

ROWS, DEPTH, UNITS = 32, 1024, 688
TOK, WIDE = 16 * ROWS, 4 * DEPTH
CUT = 336
LOW, HIGH = 1040, 1024
TAIL = 128


def index_of(x, c, z, y):
    x, z, y = x % 4, z % 4, y % 4
    return (x // 2) * 64 + ((x % 2) * 2 + c) * 16 + z * 4 + y


def moved(array, dx=0, flip=0, dz=0, dy=0):
    pairs = []
    for x in range(4):
        for c in range(2):
            for z in range(4):
                for y in range(4):
                    pairs.append((index_of(x + dx, c ^ flip, z + dz, y + dy), index_of(x, c, z, y)))
    return lax.ppermute(array, AXES, pairs)


def dot(a, b, ca, cb):
    return lax.dot_general(a, b, (((ca,), (cb,)), ((), ())), preferred_element_type=F32)


def place():
    tp = lax.axis_index("tp")
    return tp // 4, tp % 4


def call(body, out_shape, scratch, flops, ins, outs, args, nbytes):
    return pl.pallas_call(
        body,
        out_shape=out_shape,
        in_specs=ins,
        out_specs=outs,
        scratch_shapes=scratch,
        compiler_params=pltpu.CompilerParams(vmem_limit_bytes=LIMIT),
        cost_estimate=pl.CostEstimate(flops=flops, bytes_accessed=nbytes, transcendentals=0),
    )(*args)


FROM = ((0, 0, 4, 0), (1, 0, 4, 1), (2, 0, 4, 3), (3, 0, 2, 2), (4, 2, 2, 2))
WHOLE = ((0, 0, 4, 0), (1, 0, 4, 1), (2, 0, 4, 3), (3, 0, 4, 2))


def forward_kernel(*refs):
    xs, ds, was, wbs = refs[:5], refs[5:10], refs[10:14], refs[14:18]
    acts_l, acts_h, side, x_own, d_own = refs[18:23]
    v, w, sums, act, sx, sd, sw, so = refs[23:]
    z, y = place()
    x_copies, d_copies = [], []
    for i, first, count, off in FROM:
        for j in range(count):
            row = pl.multiple_of((lax.rem(z + first + j, 4) * 4 + lax.rem(y + off, 4)) * ROWS, ROWS)
            x_copies.append(
                pltpu.make_async_copy(xs[i].at[j], v.at[0, pl.ds(row, ROWS)], sx.at[len(x_copies)]))
            row = pl.multiple_of((lax.rem(z + off, 4) * 4 + lax.rem(y + first + j, 4)) * ROWS, ROWS)
            d_copies.append(
                pltpu.make_async_copy(ds[i].at[j], v.at[1, pl.ds(row, ROWS)], sd.at[len(d_copies)]))
    rest = UNITS - CUT
    w_copies = [
        [
            pltpu.make_async_copy(was[k].at[pl.ds(0, UNITS)], w.at[k, 0], sw.at[4 * k]),
            pltpu.make_async_copy(wbs[k].at[pl.ds(0, UNITS)], w.at[k, 1], sw.at[4 * k + 1]),
            pltpu.make_async_copy(was[k].at[pl.ds(UNITS, CUT)], w.at[k, 2, pl.ds(0, CUT)], sw.at[4 * k + 2]),
            pltpu.make_async_copy(wbs[k].at[pl.ds(UNITS, rest)], w.at[k, 2, pl.ds(CUT, rest)], sw.at[4 * k + 3]),
        ]
        for k in range(4)
    ]
    stages = [x_copies + w_copies[0][:2], d_copies + w_copies[0][2:], w_copies[1], w_copies[2], w_copies[3]]

    def begin(n):
        for c in stages[n]:
            c.start()

    def end(n):
        for c in stages[n]:
            c.wait()

    begin(0)
    begin(1)
    end(0)
    begin(2)

    def initial(i, _):
        @pl.when(i == 2)
        def _():
            end(1)
            begin(3)

        sums[i] = dot(w[0, i], v[i // 2, :, :DEPTH], 1, 1)
        return 0

    lax.fori_loop(0, 3, initial, 0)
    end(2)
    begin(4)
    outs = []
    for i, to in enumerate((x_own, d_own)):
        outs.append(pltpu.make_async_copy(v.at[i, :, pl.ds(0, DEPTH)], to, so.at[i]))
        for h in range(2):
            outs.append(pltpu.make_async_copy(
                v.at[i, :, pl.ds(DEPTH + h * TOK, TOK)],
                side.at[pl.ds(3 * UNITS + (2 * i + h) * TOK, TOK)], so.at[2 + 2 * i + h]))
    for k in (1, 2, 3):
        if k > 1:
            end(k + 1)
        if k == 3:
            for c in outs:
                c.start()

        def product(i, _):
            sums[i] = sums[i] + dot(w[k, i], v[i // 2, :, k * DEPTH:(k + 1) * DEPTH], 1, 1)
            return 0

        lax.fori_loop(0, 3, product, 0)

    def unit(i, _):
        r = pl.ds(pl.multiple_of(i * 16, 16), 16)
        g = sums[0, r, :].astype(BF).astype(F32)
        u = sums[1, r, :].astype(BF).astype(F32)
        b = sums[2, r, :].astype(BF).astype(F32)
        sigma = 1.0 / (1.0 + jnp.exp(-g))
        active = g * sigma
        act[r, :] = (b * u * sigma * (1.0 + g * (1.0 - sigma))).astype(BF)
        act[pl.ds(pl.multiple_of(UNITS + i * 16, 16), 16), :] = (b * active).astype(BF)
        act[pl.ds(pl.multiple_of(2 * UNITS + i * 16, 16), 16), :] = (active * u).astype(BF)
        return 0

    lax.fori_loop(0, UNITS // 16, unit, 0)
    outs.append(pltpu.make_async_copy(act.at[pl.ds(0, LOW)], acts_l, so.at[6]))
    outs.append(pltpu.make_async_copy(act.at[pl.ds(LOW, HIGH)], acts_h, so.at[7]))
    outs.append(pltpu.make_async_copy(act, side.at[pl.ds(0, 3 * UNITS)], so.at[8]))
    for c in outs[-3:]:
        c.start()
    for c in outs:
        c.wait()


def forward(xs, ds, was, wbs):
    shape = jax.ShapeDtypeStruct
    return call(
        forward_kernel,
        (shape((LOW, TOK), BF), shape((HIGH, TOK), BF), shape((3 * UNITS + 4 * TOK, TOK), BF),
         shape((TOK, DEPTH), BF), shape((TOK, DEPTH), BF)),
        [
            pltpu.VMEM((2, TOK, WIDE), BF), pltpu.VMEM((4, 3, UNITS, DEPTH), BF), pltpu.VMEM((3, UNITS, TOK), F32),
            pltpu.VMEM((3 * UNITS, TOK), BF),
            pltpu.SemaphoreType.DMA((16,)), pltpu.SemaphoreType.DMA((16,)),
            pltpu.SemaphoreType.DMA((16,)), pltpu.SemaphoreType.DMA((9,)),
        ],
        2 * TOK * WIDE * UNITS * 3,
        [ANY] * 18,
        (ANY,) * 5,
        (*xs, *ds, *was, *wbs),
        34 << 20,
    )


def input_kernel(*refs):
    acts, was, wbs, out = refs[0], refs[1:5], refs[5:9], refs[9]
    act, wa, wb, tg, tu, total, expo, sw, so = refs[10:]
    load = pltpu.make_async_copy(acts.at[pl.ds(0, 2 * UNITS)], act, so.at[5])
    load.start()
    copies = [
        (pltpu.make_async_copy(was[k].at[pl.ds(0, UNITS)], wa.at[k], sw.at[2 * k]),
         pltpu.make_async_copy(wbs[k].at[pl.ds(0, UNITS)], wb.at[k], sw.at[2 * k + 1]))
        for k in range(4)
    ]
    for pair in copies[:2]:
        for c in pair:
            c.start()
    load.wait()
    tg[...] = act[:UNITS, :].T
    tu[...] = act[UNITS:, :].T
    norm = jnp.sum(jnp.abs(tg[...].astype(F32)), axis=1, keepdims=True)
    norm = norm + jnp.sum(jnp.abs(tu[...].astype(F32)), axis=1, keepdims=True)
    e = jnp.ceil(jnp.log2(jnp.maximum(norm * (1.02 * W_MAX), 1e-30)))
    expo[...] = jnp.broadcast_to(e, (TOK, TAIL))
    puts = [pltpu.make_async_copy(expo, out.at[:, pl.ds(WIDE, TAIL)], so.at[4])]
    puts[0].start()
    for k in range(4):
        for c in copies[k]:
            c.wait()
        if k + 2 < 4:
            for c in copies[k + 2]:
                c.start()
        if k >= 2:
            puts[k - 1].wait()

        def tile(j, _):
            n = pl.ds(pl.multiple_of(j * 512, 512), 512)
            v = dot(tg[...], wa[k, :, n], 1, 0) + dot(tu[...], wb[k, :, n], 1, 0)
            total[k % 2, :, n] = v * jnp.exp2(14.0 - expo[:, :1])
            return 0

        lax.fori_loop(0, 2, tile, 0)
        puts.append(pltpu.make_async_copy(total.at[k % 2], out.at[:, pl.ds(k * DEPTH, DEPTH)], so.at[k]))
        puts[-1].start()
    for c in (puts[0], puts[3], puts[4]):
        c.wait()


def input_sums(acts, was, wbs):
    return call(
        input_kernel,
        jax.ShapeDtypeStruct((TOK, WIDE + TAIL), F32),
        [
            pltpu.VMEM((2 * UNITS, TOK), BF),
            pltpu.VMEM((4, UNITS, DEPTH), BF), pltpu.VMEM((4, UNITS, DEPTH), BF),
            pltpu.VMEM((TOK, UNITS), BF), pltpu.VMEM((TOK, UNITS), BF),
            pltpu.VMEM((2, TOK, DEPTH), F32), pltpu.VMEM((TOK, TAIL), F32),
            pltpu.SemaphoreType.DMA((8,)), pltpu.SemaphoreType.DMA((6,)),
        ],
        2 * TOK * WIDE * UNITS * 2,
        [ANY] * 9,
        ANY,
        (acts, *was, *wbs),
        22 << 20,
    )


def sum_kernel(got, out):
    v = None
    for i in range(16):
        w = got[i, :, :WIDE] * jnp.exp2(got[i, :, WIDE:WIDE + 1] - 14.0)
        v = w if v is None else v + w
    out[...] = v


def summed(got):
    return pl.pallas_call(
        sum_kernel,
        grid=(ROWS // 8,),
        out_shape=jax.ShapeDtypeStruct((ROWS, WIDE), F32),
        in_specs=[pl.BlockSpec((16, 8, WIDE + TAIL), lambda i: (0, i, 0))],
        out_specs=pl.BlockSpec((8, WIDE), lambda i: (i, 0)),
        compiler_params=pltpu.CompilerParams(vmem_limit_bytes=LIMIT),
        cost_estimate=pl.CostEstimate(flops=1 << 28, bytes_accessed=9 << 20, transcendentals=0),
    )(got)


def weight_kernel(acts, n_acts, columns, has_base, n_in, *refs):
    ins, outs = refs[:n_in], refs[n_in:n_in + 3]
    a, xc, dc, total, sa, sc, sb, so = refs[n_in + 3:]
    z, y = place()
    stages = [[], [], []]
    n = 0
    for g, pieces in enumerate(acts):
        for i, r0, r1 in pieces:
            for s in range(3):
                lo, hi = max(r0, s * UNITS), min(r1, (s + 1) * UNITS)
                if lo < hi:
                    stages[s].append(pltpu.make_async_copy(
                        ins[i].at[pl.ds(lo - r0, hi - lo)], a.at[pl.ds(lo, hi - lo), pl.ds(g * TOK, TOK)], sa.at[n]))
                    n += 1
    columns(ins[n_acts:], z, y, lambda src, to: stages[0].append(
        pltpu.make_async_copy(src, to, sc.at[0, len(stages[0])])), xc, 0)
    columns(ins[n_acts:], z, y, lambda src, to: stages[2].append(
        pltpu.make_async_copy(src, to, sc.at[1, len(stages[2])])), dc, 1)
    if has_base:
        for s in range(3):
            stages[s].append(pltpu.make_async_copy(ins[n_in - 3 + s], total.at[s], sb.at[s]))

    def begin(s):
        for c in stages[s]:
            c.start()

    begin(0)
    begin(1)
    done = [pltpu.make_async_copy(total.at[i], outs[i], so.at[i]) for i in range(3)]

    def product(i, cols):
        v = dot(a[pl.ds(pl.multiple_of(i * UNITS, 16), UNITS), :], cols[...].reshape(len(acts) * TOK, DEPTH), 1, 0)
        total[i] = total[i] + v if has_base else v

    def pair(i, _):
        @pl.when(i == 0)
        def _():
            for c in stages[0]:
                c.wait()
            begin(2)

        @pl.when(i == 1)
        def _():
            done[0].start()
            for c in stages[1]:
                c.wait()

        product(i, xc)
        return 0

    lax.fori_loop(0, 2, pair, 0)
    done[1].start()
    for c in stages[2]:
        c.wait()
    product(2, dc)
    done[2].start()
    for c in done:
        c.wait()


def near_columns(refs, z, y, add, buf, kind):
    x_own, d_own, side = refs[:3]
    add(d_own if kind else x_own, buf.at[0])
    for h in range(2):
        add(side.at[pl.ds(3 * UNITS + (2 * kind + h) * TOK, TOK)], buf.at[1, :, pl.ds(h * TOK, TOK)])


def plane_columns(first_group, count, refs, z, y, add, buf, kind):
    for i, first, n, off in WHOLE:
        for j in range(n):
            a, b = lax.rem(z + first + j, 4), lax.rem(y + off, 4)
            if kind:
                a, b = lax.rem(z + off, 4), lax.rem(y + first + j, 4)
            add(refs[4 * kind + i].at[j, pl.ds(first_group, count)], buf.at[:, a * 4 + b])


def weight_sums(groups, columns, arrays, base):
    ins, acts = [], []
    for pieces in groups:
        row, marks = 0, []
        for p, m in pieces:
            marks.append((len(ins), row, row + m))
            ins.append(p)
            row += m
        acts.append(marks)
    n_acts = len(ins)
    ins += list(arrays) + list(base or [])
    n = len(groups)
    col = (n, TOK, DEPTH) if columns is near_columns else (n, 16, ROWS, DEPTH)
    out = jax.ShapeDtypeStruct((UNITS, DEPTH), F32)
    return call(
        functools.partial(weight_kernel, acts, n_acts, columns, base is not None, len(ins)),
        (out,) * 3,
        [
            pltpu.VMEM((3 * UNITS, n * TOK), BF), pltpu.VMEM(col, BF), pltpu.VMEM(col, BF),
            pltpu.VMEM((3, UNITS, DEPTH), F32),
            pltpu.SemaphoreType.DMA((3 * n_acts,)), pltpu.SemaphoreType.DMA((2, 32)),
            pltpu.SemaphoreType.DMA((3,)), pltpu.SemaphoreType.DMA((3,)),
        ],
        2 * 3 * UNITS * DEPTH * n * TOK,
        [ANY] * len(ins),
        (ANY,) * 3,
        ins,
        n * (4 << 20) + (16 << 20),
    )


def block(inputs, w_gate, w_up, w_down, d_out):
    fs = lax.axis_index("fs")

    def relative(v):
        parts = [v[:, i * DEPTH:(i + 1) * DEPTH] for i in range(4)]
        out = []
        for k in range(4):
            w = parts[k]
            for f in range(1, 4):
                w = jnp.where(fs == f, parts[f ^ k], w)
            out.append(w)
        return out

    xp, dp = relative(inputs), relative(d_out)
    x_own, d_own = jnp.concatenate(xp, axis=1), jnp.concatenate(dp, axis=1)

    def spread(own, first, second, forward):
        line = jnp.concatenate(
            [own[None]] + [moved(own[None], **{first: d}) for d in (1, 2, 3)], axis=0)
        up, down = moved(line, **{second: 1}), moved(line, **{second: -1})
        if not forward:
            return line, up, down, moved(line, **{second: 2})
        low, high = up[:2], down[2:]
        return line, up, down, moved(low, **{second: 1}), moved(high, **{second: -1})

    xs = spread(x_own, "dz", "dy", True)
    ds = spread(d_own, "dy", "dz", True)

    side = moved(jnp.stack([xp[1], dp[1], xp[3], dp[3]]), flip=1)
    far = jnp.stack([xp[0], side[0], dp[0], side[1]])
    near = jnp.stack([xp[2], side[2], dp[2], side[3]])
    got = (moved(near, dx=1), moved(near, dx=-1), moved(far, dx=2))
    xcs = spread(jnp.concatenate([v[:2] for v in got], axis=0), "dz", "dy", False)
    dcs = spread(jnp.concatenate([v[2:] for v in got], axis=0), "dy", "dz", False)

    wa = jnp.concatenate([w_gate.T, w_down[:CUT]], axis=0)
    wb = jnp.concatenate([w_up.T, w_down[CUT:]], axis=0)
    wa2, wb2 = moved(wa, dx=1), moved(wb, dx=-1)
    wa1, wb1 = moved(wa, flip=1), moved(wb, flip=1)
    wa3, wb3 = moved(wa2, flip=1), moved(wb2, flip=1)
    was, wbs = (wa, wa1, wa2, wa3), (wb, wb1, wb2, wb3)

    acts_l, acts_h, own, x_cols, d_cols = forward(xs, ds, was, wbs)

    aml, aph = moved(acts_l, dx=1), moved(acts_h, dx=-1)
    amh, apl = moved(acts_h, dx=1), moved(acts_l, dx=-1)
    side = moved(own, flip=1)
    oa, ob = moved(aml, dx=1), moved(aph, dx=-1)
    sml, sph = moved(aml, flip=1), moved(aph, flip=1)
    smh, spl = moved(amh, flip=1), moved(apl, flip=1)
    soa, sob = moved(oa, flip=1), moved(ob, flip=1)

    packed = input_sums(own, was, wbs).astype(F16)
    got = lax.all_to_all(packed.reshape(16, ROWS, WIDE + TAIL), "tp", 0, 0)
    grad_inputs = jnp.concatenate(relative(summed(got.astype(F32)).astype(BF)), axis=1)

    full = 3 * UNITS

    def halves(low, high):
        return [(low, LOW), (high, HIGH)]

    sums = weight_sums(
        [[(own, full)], [(side, full)]], near_columns, (x_cols, d_cols, side), None)
    sums = weight_sums(
        [halves(aml, amh), halves(sml, smh), halves(apl, aph), halves(spl, sph)],
        functools.partial(plane_columns, 0, 4), (*xcs, *dcs), sums)
    sums = weight_sums(
        [halves(oa, ob), halves(soa, sob)], functools.partial(plane_columns, 4, 2), (*xcs, *dcs), sums)
    return grad_inputs, sums[0].T, sums[1].T, sums[2]


def solution(mesh):
    tok = P(AXES, None)
    return jax.shard_map(
        block,
        mesh=mesh,
        in_specs=(tok, P("fs", "tp"), P("fs", "tp"), P("tp", "fs"), tok),
        out_specs=(tok, P("fs", "tp"), P("fs", "tp"), P("tp", "fs")),
        check_vma=False,
    )
```

```python
import functools

import jax
import jax.numpy as jnp
from jax import lax
from jax.experimental import pallas as pl
from jax.experimental.pallas import tpu as pltpu
from jax.sharding import PartitionSpec as P


AXES = ("rep", "fs", "tp")
BF, F32, F16 = jnp.bfloat16, jnp.float32, jnp.float16
W_MAX = 0.09375
ANY = pl.BlockSpec(memory_space=pl.ANY)
VMEM = pl.BlockSpec(memory_space=pltpu.VMEM)
LIMIT = 56 * 1024 * 1024

ROWS, DEPTH, UNITS = 32, 1024, 688
TOK, WIDE = 16 * ROWS, 4 * DEPTH
CUT = 336
LOW, HIGH = 1040, 1024
TAIL = 128


def index_of(x, c, z, y):
    x, z, y = x % 4, z % 4, y % 4
    return (x // 2) * 64 + ((x % 2) * 2 + c) * 16 + z * 4 + y


def moved(array, dx=0, flip=0, dz=0, dy=0):
    pairs = []
    for x in range(4):
        for c in range(2):
            for z in range(4):
                for y in range(4):
                    pairs.append((index_of(x + dx, c ^ flip, z + dz, y + dy), index_of(x, c, z, y)))
    return lax.ppermute(array, AXES, pairs)


def dot(a, b, ca, cb):
    return lax.dot_general(a, b, (((ca,), (cb,)), ((), ())), preferred_element_type=F32)


def place():
    tp = lax.axis_index("tp")
    return tp // 4, tp % 4


def call(body, out_shape, scratch, flops, ins, outs, args, nbytes):
    return pl.pallas_call(
        body,
        out_shape=out_shape,
        in_specs=ins,
        out_specs=outs,
        scratch_shapes=scratch,
        compiler_params=pltpu.CompilerParams(vmem_limit_bytes=LIMIT),
        cost_estimate=pl.CostEstimate(flops=flops, bytes_accessed=nbytes, transcendentals=0),
    )(*args)


FROM = ((0, 0), (2, 0), (0, 1), (2, 1), (0, 3), (2, 3), (0, 2), (2, 2))


def forward_kernel(*refs):
    xs, ds, was, wbs = refs[:8], refs[8:16], refs[16:20], refs[20:24]
    acts_l, acts_h, side, x_own, d_own = refs[24:29]
    v, w, sums, act, sx, sd, sw, so = refs[29:]
    z, y = place()
    x_copies, d_copies = [], []
    for i, (first, off) in enumerate(FROM):
        for j in range(2):
            row = pl.multiple_of((lax.rem(z + first + j, 4) * 4 + lax.rem(y + off, 4)) * ROWS, ROWS)
            x_copies.append(
                pltpu.make_async_copy(xs[i].at[j], v.at[0, pl.ds(row, ROWS)], sx.at[len(x_copies)]))
            row = pl.multiple_of((lax.rem(z + off, 4) * 4 + lax.rem(y + first + j, 4)) * ROWS, ROWS)
            d_copies.append(
                pltpu.make_async_copy(ds[i].at[j], v.at[1, pl.ds(row, ROWS)], sd.at[len(d_copies)]))
    rest = UNITS - CUT
    w_copies = [
        [
            pltpu.make_async_copy(was[k].at[pl.ds(0, UNITS)], w.at[k, 0], sw.at[4 * k]),
            pltpu.make_async_copy(wbs[k].at[pl.ds(0, UNITS)], w.at[k, 1], sw.at[4 * k + 1]),
            pltpu.make_async_copy(was[k].at[pl.ds(UNITS, CUT)], w.at[k, 2, pl.ds(0, CUT)], sw.at[4 * k + 2]),
            pltpu.make_async_copy(wbs[k].at[pl.ds(UNITS, rest)], w.at[k, 2, pl.ds(CUT, rest)], sw.at[4 * k + 3]),
        ]
        for k in range(4)
    ]
    stages = [x_copies + w_copies[0][:2], d_copies + w_copies[0][2:], w_copies[1], w_copies[2], w_copies[3]]

    def begin(n):
        for c in stages[n]:
            c.start()

    def end(n):
        for c in stages[n]:
            c.wait()

    begin(0)
    begin(1)
    end(0)
    begin(2)

    def initial(i, _):
        @pl.when(i == 2)
        def _():
            end(1)
            begin(3)

        sums[i] = dot(w[0, i], v[i // 2, :, :DEPTH], 1, 1)
        return 0

    lax.fori_loop(0, 3, initial, 0)
    end(2)
    begin(4)
    outs = []
    for i, to in enumerate((x_own, d_own)):
        outs.append(pltpu.make_async_copy(v.at[i, :, pl.ds(0, DEPTH)], to, so.at[i]))
        for h in range(2):
            outs.append(pltpu.make_async_copy(
                v.at[i, :, pl.ds(DEPTH + h * TOK, TOK)],
                side.at[pl.ds(3 * UNITS + (2 * i + h) * TOK, TOK)], so.at[2 + 2 * i + h]))
    for k in (1, 2, 3):
        if k > 1:
            end(k + 1)
        if k == 3:
            for c in outs:
                c.start()

        def product(i, _):
            sums[i] = sums[i] + dot(w[k, i], v[i // 2, :, k * DEPTH:(k + 1) * DEPTH], 1, 1)
            return 0

        lax.fori_loop(0, 3, product, 0)

    def unit(i, _):
        r = pl.ds(pl.multiple_of(i * 16, 16), 16)
        g = sums[0, r, :].astype(BF).astype(F32)
        u = sums[1, r, :].astype(BF).astype(F32)
        b = sums[2, r, :].astype(BF).astype(F32)
        sigma = 1.0 / (1.0 + jnp.exp(-g))
        active = g * sigma
        act[r, :] = (b * u * sigma * (1.0 + g * (1.0 - sigma))).astype(BF)
        act[pl.ds(pl.multiple_of(UNITS + i * 16, 16), 16), :] = (b * active).astype(BF)
        act[pl.ds(pl.multiple_of(2 * UNITS + i * 16, 16), 16), :] = (active * u).astype(BF)
        return 0

    lax.fori_loop(0, UNITS // 16, unit, 0)
    outs.append(pltpu.make_async_copy(act.at[pl.ds(0, LOW)], acts_l, so.at[6]))
    outs.append(pltpu.make_async_copy(act.at[pl.ds(LOW, HIGH)], acts_h, so.at[7]))
    outs.append(pltpu.make_async_copy(act, side.at[pl.ds(0, 3 * UNITS)], so.at[8]))
    for c in outs[-3:]:
        c.start()
    for c in outs:
        c.wait()


def forward(xs, ds, was, wbs):
    shape = jax.ShapeDtypeStruct
    return call(
        forward_kernel,
        (shape((LOW, TOK), BF), shape((HIGH, TOK), BF), shape((3 * UNITS + 4 * TOK, TOK), BF),
         shape((TOK, DEPTH), BF), shape((TOK, DEPTH), BF)),
        [
            pltpu.VMEM((2, TOK, WIDE), BF), pltpu.VMEM((4, 3, UNITS, DEPTH), BF), pltpu.VMEM((3, UNITS, TOK), F32),
            pltpu.VMEM((3 * UNITS, TOK), BF),
            pltpu.SemaphoreType.DMA((16,)), pltpu.SemaphoreType.DMA((16,)),
            pltpu.SemaphoreType.DMA((16,)), pltpu.SemaphoreType.DMA((9,)),
        ],
        2 * TOK * WIDE * UNITS * 3,
        [ANY] * 24,
        (ANY,) * 5,
        (*xs, *ds, *was, *wbs),
        34 << 20,
    )


def input_kernel(*refs):
    acts, was, wbs, out = refs[0], refs[1:5], refs[5:9], refs[9]
    act, wa, wb, tg, tu, total, expo, sw, so = refs[10:]
    load = pltpu.make_async_copy(acts.at[pl.ds(0, 2 * UNITS)], act, so.at[5])
    load.start()
    copies = [
        (pltpu.make_async_copy(was[k].at[pl.ds(0, UNITS)], wa.at[k], sw.at[2 * k]),
         pltpu.make_async_copy(wbs[k].at[pl.ds(0, UNITS)], wb.at[k], sw.at[2 * k + 1]))
        for k in range(4)
    ]
    for pair in copies[:2]:
        for c in pair:
            c.start()
    load.wait()
    tg[...] = act[:UNITS, :].T
    tu[...] = act[UNITS:, :].T
    norm = jnp.sum(jnp.abs(tg[...].astype(F32)), axis=1, keepdims=True)
    norm = norm + jnp.sum(jnp.abs(tu[...].astype(F32)), axis=1, keepdims=True)
    e = jnp.ceil(jnp.log2(jnp.maximum(jnp.max(norm, axis=0, keepdims=True) * (1.02 * W_MAX), 1e-30)))
    expo[...] = jnp.broadcast_to(e, (TOK, TAIL))
    tail = pltpu.make_async_copy(expo, out.at[:, pl.ds(WIDE, TAIL)], so.at[4])
    tail.start()

    def put(k):
        at = k * DEPTH if isinstance(k, int) else pl.multiple_of(k * DEPTH, DEPTH)
        return pltpu.make_async_copy(total.at[k % 2 if isinstance(k, int) else lax.rem(k, 2)],
                                     out.at[:, pl.ds(at, DEPTH)], so.at[k])

    def part(k, _):
        for n in range(4):
            @pl.when(k == n)
            def _():
                for c in copies[n]:
                    c.wait()
                if n + 2 < 4:
                    for c in copies[n + 2]:
                        c.start()
                if n >= 2:
                    put(n - 2).wait()

        def tile(j, _):
            n = pl.ds(pl.multiple_of(j * 512, 512), 512)
            v = dot(tg[...], wa[k, :, n], 1, 0) + dot(tu[...], wb[k, :, n], 1, 0)
            total[lax.rem(k, 2), :, n] = v * jnp.exp2(14.0 - expo[:, :1])
            return 0

        lax.fori_loop(0, 2, tile, 0)
        put(k).start()
        return 0

    lax.fori_loop(0, 4, part, 0)
    for c in (tail, put(2), put(3)):
        c.wait()


def input_sums(acts, was, wbs):
    return call(
        input_kernel,
        jax.ShapeDtypeStruct((TOK, WIDE + TAIL), F32),
        [
            pltpu.VMEM((2 * UNITS, TOK), BF),
            pltpu.VMEM((4, UNITS, DEPTH), BF), pltpu.VMEM((4, UNITS, DEPTH), BF),
            pltpu.VMEM((TOK, UNITS), BF), pltpu.VMEM((TOK, UNITS), BF),
            pltpu.VMEM((2, TOK, DEPTH), F32), pltpu.VMEM((TOK, TAIL), F32),
            pltpu.SemaphoreType.DMA((8,)), pltpu.SemaphoreType.DMA((6,)),
        ],
        2 * TOK * WIDE * UNITS * 2,
        [ANY] * 9,
        ANY,
        (acts, *was, *wbs),
        22 << 20,
    )


def weight_kernel(acts, n_acts, columns, has_base, n_in, *refs):
    ins, outs = refs[:n_in], refs[n_in:n_in + 3]
    a, cols, total, sa, sc, sb, so = refs[n_in + 3:]
    z, y = place()
    stages = [[], [], []]
    n = 0
    for g, pieces in enumerate(acts):
        for i, r0, r1 in pieces:
            for s in range(3):
                lo, hi = max(r0, s * UNITS), min(r1, (s + 1) * UNITS)
                if lo < hi:
                    stages[s].append(pltpu.make_async_copy(
                        ins[i].at[pl.ds(lo - r0, hi - lo)], a.at[pl.ds(lo, hi - lo), pl.ds(g * TOK, TOK)], sa.at[n]))
                    n += 1
    columns(ins[n_acts:], z, y, lambda src, to: stages[0].append(
        pltpu.make_async_copy(src, to, sc.at[0, len(stages[0])])), cols.at[0], 0)
    columns(ins[n_acts:], z, y, lambda src, to: stages[2].append(
        pltpu.make_async_copy(src, to, sc.at[1, len(stages[2])])), cols.at[1], 1)
    if has_base:
        for s in range(3):
            stages[s].append(pltpu.make_async_copy(ins[n_in - 3 + s], total.at[s], sb.at[s]))

    def begin(s):
        for c in stages[s]:
            c.start()

    begin(0)
    begin(1)
    done = [pltpu.make_async_copy(total.at[i], outs[i], so.at[i]) for i in range(3)]

    def product(i, _):
        for n in range(3):
            @pl.when(i == n)
            def _():
                if n:
                    done[n - 1].start()
                for c in stages[n]:
                    c.wait()
                if n == 0:
                    begin(2)

        rows = pl.ds(pl.multiple_of(i * UNITS, 16), UNITS)
        v = dot(a[rows, :], cols[i // 2].reshape(len(acts) * TOK, DEPTH), 1, 0)
        total[i] = total[i] + v if has_base else v
        return 0

    lax.fori_loop(0, 3, product, 0)
    done[2].start()
    for c in done:
        c.wait()


def near_columns(refs, z, y, add, buf, kind):
    x_own, d_own, side = refs[:3]
    add(d_own if kind else x_own, buf.at[0])
    for h in range(2):
        add(side.at[pl.ds(3 * UNITS + (2 * kind + h) * TOK, TOK)], buf.at[1, :, pl.ds(h * TOK, TOK)])


def plane_columns(first_group, count, refs, z, y, add, buf, kind):
    for i, (first, off) in enumerate(FROM):
        for j in range(2):
            a, b = lax.rem(z + first + j, 4), lax.rem(y + off, 4)
            if kind:
                a, b = lax.rem(z + off, 4), lax.rem(y + first + j, 4)
            add(refs[8 * kind + i].at[j, pl.ds(first_group, count)], buf.at[:, a * 4 + b])


def weight_sums(groups, columns, arrays, base):
    ins, acts = [], []
    for pieces in groups:
        row, marks = 0, []
        for p, m in pieces:
            marks.append((len(ins), row, row + m))
            ins.append(p)
            row += m
        acts.append(marks)
    n_acts = len(ins)
    ins += list(arrays) + list(base or [])
    n = len(groups)
    col = (2, n, TOK, DEPTH) if columns is near_columns else (2, n, 16, ROWS, DEPTH)
    out = jax.ShapeDtypeStruct((UNITS, DEPTH), F32)
    return call(
        functools.partial(weight_kernel, acts, n_acts, columns, base is not None, len(ins)),
        (out,) * 3,
        [
            pltpu.VMEM((3 * UNITS, n * TOK), BF), pltpu.VMEM(col, BF),
            pltpu.VMEM((3, UNITS, DEPTH), F32),
            pltpu.SemaphoreType.DMA((3 * n_acts,)), pltpu.SemaphoreType.DMA((2, 48)),
            pltpu.SemaphoreType.DMA((3,)), pltpu.SemaphoreType.DMA((3,)),
        ],
        2 * 3 * UNITS * DEPTH * n * TOK,
        [ANY] * len(ins),
        (ANY,) * 3,
        ins,
        n * (4 << 20) + (16 << 20),
    )


def block(inputs, w_gate, w_up, w_down, d_out):
    fs = lax.axis_index("fs")

    def relative(v, fs=fs):
        parts = [v[:, i * DEPTH:(i + 1) * DEPTH] for i in range(4)]
        out = []
        for k in range(4):
            w = parts[k]
            for f in range(1, 4):
                w = jnp.where(fs == f, parts[f ^ k], w)
            out.append(w)
        return out

    mark = lax.optimization_barrier(fs) * 3 - 1
    mark = (mark + 1) // 3

    xp, dp = relative(inputs), relative(d_out)
    x_own, d_own = jnp.concatenate(xp, axis=1), jnp.concatenate(dp, axis=1)

    def spread(own, first, second):
        own = own[None]
        one, two, three = (moved(own, **{first: d}) for d in (1, 2, 3))
        low, high = jnp.concatenate([own, one], axis=0), jnp.concatenate([two, three], axis=0)
        up_l, up_h = moved(low, **{second: 1}), moved(high, **{second: 1})
        down_l, down_h = moved(low, **{second: -1}), moved(high, **{second: -1})
        far_l, far_h = moved(up_l, **{second: 1}), moved(down_h, **{second: -1})
        return low, high, up_l, up_h, down_l, down_h, far_l, far_h

    xs = spread(x_own, "dz", "dy")
    ds = spread(d_own, "dy", "dz")

    side = moved(jnp.stack([xp[1], dp[1], xp[3], dp[3]]), flip=1)
    far = jnp.stack([xp[0], side[0], dp[0], side[1]])
    near = jnp.stack([xp[2], side[2], dp[2], side[3]])
    got = (moved(near, dx=1), moved(near, dx=-1), moved(far, dx=2))
    xcs = spread(jnp.concatenate([v[:2] for v in got], axis=0), "dz", "dy")
    dcs = spread(jnp.concatenate([v[2:] for v in got], axis=0), "dy", "dz")

    wa = jnp.concatenate([w_gate.T, w_down[:CUT]], axis=0)
    wb = jnp.concatenate([w_up.T, w_down[CUT:]], axis=0)
    wa2, wb2 = moved(wa, dx=1), moved(wb, dx=-1)
    wa1, wb1 = moved(wa, flip=1), moved(wb, flip=1)
    wa3, wb3 = moved(wa2, flip=1), moved(wb2, flip=1)
    was, wbs = (wa, wa1, wa2, wa3), (wb, wb1, wb2, wb3)

    acts_l, acts_h, own, x_cols, d_cols = forward(xs, ds, was, wbs)

    aml, aph = moved(acts_l, dx=1), moved(acts_h, dx=-1)
    amh, apl = moved(acts_h, dx=1), moved(acts_l, dx=-1)
    side = moved(own, flip=1)
    oa, ob = moved(aml, dx=1), moved(aph, dx=-1)
    sml, sph = moved(aml, flip=1), moved(aph, flip=1)
    smh, spl = moved(amh, flip=1), moved(apl, flip=1)
    soa, sob = moved(oa, flip=1), moved(ob, flip=1)

    packed = input_sums(own, was, wbs).astype(F16)
    got = lax.all_to_all(packed.reshape(16, ROWS, WIDE + TAIL), "tp", 0, 0)
    back = lax.optimization_barrier(jnp.exp2(got[:, 0, WIDE].astype(F32) - 14.0))
    total = 0.0
    for i in range(16):
        total = total + got[i, :, :WIDE].astype(F32) * back[i]
    grad_inputs = jnp.concatenate(relative(total.astype(BF), mark), axis=1)

    full = 3 * UNITS

    def halves(low, high):
        return [(low, LOW), (high, HIGH)]

    sums = weight_sums(
        [[(own, full)], [(side, full)]], near_columns, (x_cols, d_cols, side), None)
    sums = weight_sums(
        [halves(aml, amh), halves(sml, smh), halves(apl, aph), halves(spl, sph)],
        functools.partial(plane_columns, 0, 4), (*xcs, *dcs), sums)
    sums = weight_sums(
        [halves(oa, ob), halves(soa, sob)], functools.partial(plane_columns, 4, 2), (*xcs, *dcs), sums)
    return grad_inputs, sums[0].T, sums[1].T, sums[2]


def solution(mesh):
    tok = P(AXES, None)
    return jax.shard_map(
        block,
        mesh=mesh,
        in_specs=(tok, P("fs", "tp"), P("fs", "tp"), P("tp", "fs"), tok),
        out_specs=(tok, P("fs", "tp"), P("fs", "tp"), P("tp", "fs")),
        check_vma=False,
    )
```

```python
import functools

import jax
import jax.numpy as jnp
from jax import lax
from jax.experimental import pallas as pl
from jax.experimental.pallas import tpu as pltpu
from jax.sharding import PartitionSpec as P


AXES = ("rep", "fs", "tp")
BF, F32, F16 = jnp.bfloat16, jnp.float32, jnp.float16
W_MAX = 0.09375
ANY = pl.BlockSpec(memory_space=pl.ANY)
VMEM = pl.BlockSpec(memory_space=pltpu.VMEM)
LIMIT = 56 * 1024 * 1024

ROWS, DEPTH, UNITS = 32, 1024, 688
TOK, WIDE = 16 * ROWS, 4 * DEPTH
CUT = 336
LOW, HIGH = 1040, 1024
TAIL = 128


def index_of(x, c, z, y):
    x, z, y = x % 4, z % 4, y % 4
    return (x // 2) * 64 + ((x % 2) * 2 + c) * 16 + z * 4 + y


def moved(array, dx=0, flip=0, dz=0, dy=0):
    pairs = []
    for x in range(4):
        for c in range(2):
            for z in range(4):
                for y in range(4):
                    pairs.append((index_of(x + dx, c ^ flip, z + dz, y + dy), index_of(x, c, z, y)))
    return lax.ppermute(array, AXES, pairs)


def dot(a, b, ca, cb):
    return lax.dot_general(a, b, (((ca,), (cb,)), ((), ())), preferred_element_type=F32)


def place():
    tp = lax.axis_index("tp")
    return tp // 4, tp % 4


def call(body, out_shape, scratch, flops, ins, outs, args, nbytes):
    return pl.pallas_call(
        body,
        out_shape=out_shape,
        in_specs=ins,
        out_specs=outs,
        scratch_shapes=scratch,
        compiler_params=pltpu.CompilerParams(vmem_limit_bytes=LIMIT),
        cost_estimate=pl.CostEstimate(flops=flops, bytes_accessed=nbytes, transcendentals=0),
    )(*args)


FROM = ((0, 0), (2, 0), (0, 1), (2, 1), (0, 3), (2, 3), (0, 2), (2, 2))
WHOLE = (0, 1, 3, 2)


def forward_kernel(*refs):
    xs, ds, was, wbs = refs[:8], refs[8:16], refs[16:20], refs[20:24]
    acts_l, acts_h, side, x_own, d_own = refs[24:29]
    v, w, sums, act, sx, sd, sw, so = refs[29:]
    z, y = place()
    x_copies, d_copies = [], []
    for i, (first, off) in enumerate(FROM):
        for j in range(2):
            row = pl.multiple_of((lax.rem(z + first + j, 4) * 4 + lax.rem(y + off, 4)) * ROWS, ROWS)
            x_copies.append(
                pltpu.make_async_copy(xs[i].at[j], v.at[0, pl.ds(row, ROWS)], sx.at[len(x_copies)]))
            row = pl.multiple_of((lax.rem(z + off, 4) * 4 + lax.rem(y + first + j, 4)) * ROWS, ROWS)
            d_copies.append(
                pltpu.make_async_copy(ds[i].at[j], v.at[1, pl.ds(row, ROWS)], sd.at[len(d_copies)]))
    rest = UNITS - CUT
    w_copies = [
        [
            pltpu.make_async_copy(was[k].at[pl.ds(0, UNITS)], w.at[k, 0], sw.at[4 * k]),
            pltpu.make_async_copy(wbs[k].at[pl.ds(0, UNITS)], w.at[k, 1], sw.at[4 * k + 1]),
            pltpu.make_async_copy(was[k].at[pl.ds(UNITS, CUT)], w.at[k, 2, pl.ds(0, CUT)], sw.at[4 * k + 2]),
            pltpu.make_async_copy(wbs[k].at[pl.ds(UNITS, rest)], w.at[k, 2, pl.ds(CUT, rest)], sw.at[4 * k + 3]),
        ]
        for k in range(4)
    ]
    stages = [x_copies + w_copies[0][:2], d_copies + w_copies[0][2:], w_copies[1], w_copies[2], w_copies[3]]

    def begin(n):
        for c in stages[n]:
            c.start()

    def end(n):
        for c in stages[n]:
            c.wait()

    begin(0)
    begin(1)
    end(0)
    begin(2)

    def initial(i, _):
        @pl.when(i == 2)
        def _():
            end(1)
            begin(3)

        sums[i] = dot(w[0, i], v[i // 2, :, :DEPTH], 1, 1)
        return 0

    lax.fori_loop(0, 3, initial, 0)
    end(2)
    begin(4)
    outs = []
    for i, to in enumerate((x_own, d_own)):
        outs.append(pltpu.make_async_copy(v.at[i, :, pl.ds(0, DEPTH)], to, so.at[i]))
        for h in range(2):
            outs.append(pltpu.make_async_copy(
                v.at[i, :, pl.ds(DEPTH + h * TOK, TOK)],
                side.at[pl.ds(3 * UNITS + (2 * i + h) * TOK, TOK)], so.at[2 + 2 * i + h]))
    for k in (1, 2, 3):
        if k > 1:
            end(k + 1)
        if k == 3:
            for c in outs:
                c.start()

        def product(i, _):
            sums[i] = sums[i] + dot(w[k, i], v[i // 2, :, k * DEPTH:(k + 1) * DEPTH], 1, 1)
            return 0

        lax.fori_loop(0, 3, product, 0)

    def unit(i, _):
        r = pl.ds(pl.multiple_of(i * 16, 16), 16)
        g = sums[0, r, :].astype(BF).astype(F32)
        u = sums[1, r, :].astype(BF).astype(F32)
        b = sums[2, r, :].astype(BF).astype(F32)
        sigma = 1.0 / (1.0 + jnp.exp(-g))
        active = g * sigma
        act[r, :] = (b * u * sigma * (1.0 + g * (1.0 - sigma))).astype(BF)
        act[pl.ds(pl.multiple_of(UNITS + i * 16, 16), 16), :] = (b * active).astype(BF)
        act[pl.ds(pl.multiple_of(2 * UNITS + i * 16, 16), 16), :] = (active * u).astype(BF)
        return 0

    lax.fori_loop(0, UNITS // 16, unit, 0)
    outs.append(pltpu.make_async_copy(act.at[pl.ds(0, LOW)], acts_l, so.at[6]))
    outs.append(pltpu.make_async_copy(act.at[pl.ds(LOW, HIGH)], acts_h, so.at[7]))
    outs.append(pltpu.make_async_copy(act, side.at[pl.ds(0, 3 * UNITS)], so.at[8]))
    for c in outs[-3:]:
        c.start()
    for c in outs:
        c.wait()


def forward(xs, ds, was, wbs):
    shape = jax.ShapeDtypeStruct
    return call(
        forward_kernel,
        (shape((LOW, TOK), BF), shape((HIGH, TOK), BF), shape((3 * UNITS + 4 * TOK, TOK), BF),
         shape((TOK, DEPTH), BF), shape((TOK, DEPTH), BF)),
        [
            pltpu.VMEM((2, TOK, WIDE), BF), pltpu.VMEM((4, 3, UNITS, DEPTH), BF), pltpu.VMEM((3, UNITS, TOK), F32),
            pltpu.VMEM((3 * UNITS, TOK), BF),
            pltpu.SemaphoreType.DMA((16,)), pltpu.SemaphoreType.DMA((16,)),
            pltpu.SemaphoreType.DMA((16,)), pltpu.SemaphoreType.DMA((9,)),
        ],
        2 * TOK * WIDE * UNITS * 3,
        [ANY] * 24,
        (ANY,) * 5,
        (*xs, *ds, *was, *wbs),
        34 << 20,
    )


def input_kernel(*refs):
    acts, was, wbs, out = refs[0], refs[1:5], refs[5:9], refs[9]
    act, wa, wb, tg, tu, total, expo, sw, so = refs[10:]
    load = pltpu.make_async_copy(acts.at[pl.ds(0, 2 * UNITS)], act, so.at[5])
    load.start()
    copies = [
        (pltpu.make_async_copy(was[k].at[pl.ds(0, UNITS)], wa.at[k], sw.at[2 * k]),
         pltpu.make_async_copy(wbs[k].at[pl.ds(0, UNITS)], wb.at[k], sw.at[2 * k + 1]))
        for k in range(4)
    ]
    for pair in copies[:2]:
        for c in pair:
            c.start()
    load.wait()
    tg[...] = act[:UNITS, :].T
    tu[...] = act[UNITS:, :].T
    norm = jnp.sum(jnp.abs(tg[...].astype(F32)), axis=1, keepdims=True)
    norm = norm + jnp.sum(jnp.abs(tu[...].astype(F32)), axis=1, keepdims=True)
    e = jnp.ceil(jnp.log2(jnp.maximum(jnp.max(norm, axis=0, keepdims=True) * (1.02 * W_MAX), 1e-30)))
    expo[...] = jnp.broadcast_to(e, (TOK, TAIL))
    tail = pltpu.make_async_copy(expo, out.at[:, pl.ds(WIDE, TAIL)], so.at[4])
    tail.start()

    def put(k):
        at = k * DEPTH if isinstance(k, int) else pl.multiple_of(k * DEPTH, DEPTH)
        return pltpu.make_async_copy(total.at[k % 2 if isinstance(k, int) else lax.rem(k, 2)],
                                     out.at[:, pl.ds(at, DEPTH)], so.at[k])

    def part(k, _):
        for n in range(4):
            @pl.when(k == n)
            def _():
                for c in copies[n]:
                    c.wait()
                if n + 2 < 4:
                    for c in copies[n + 2]:
                        c.start()
                if n >= 2:
                    put(n - 2).wait()

        def tile(j, _):
            n = pl.ds(pl.multiple_of(j * 512, 512), 512)
            v = dot(tg[...], wa[k, :, n], 1, 0) + dot(tu[...], wb[k, :, n], 1, 0)
            total[lax.rem(k, 2), :, n] = v * jnp.exp2(14.0 - expo[:, :1])
            return 0

        lax.fori_loop(0, 2, tile, 0)
        put(k).start()
        return 0

    lax.fori_loop(0, 4, part, 0)
    for c in (tail, put(2), put(3)):
        c.wait()


def input_sums(acts, was, wbs):
    return call(
        input_kernel,
        jax.ShapeDtypeStruct((TOK, WIDE + TAIL), F32),
        [
            pltpu.VMEM((2 * UNITS, TOK), BF),
            pltpu.VMEM((4, UNITS, DEPTH), BF), pltpu.VMEM((4, UNITS, DEPTH), BF),
            pltpu.VMEM((TOK, UNITS), BF), pltpu.VMEM((TOK, UNITS), BF),
            pltpu.VMEM((2, TOK, DEPTH), F32), pltpu.VMEM((TOK, TAIL), F32),
            pltpu.SemaphoreType.DMA((8,)), pltpu.SemaphoreType.DMA((6,)),
        ],
        2 * TOK * WIDE * UNITS * 2,
        [ANY] * 9,
        ANY,
        (acts, *was, *wbs),
        22 << 20,
    )


def weight_kernel(acts, n_acts, columns, has_base, n_in, *refs):
    ins, outs = refs[:n_in], refs[n_in:n_in + 3]
    a, cols, total, sa, sc, sb, so = refs[n_in + 3:]
    z, y = place()
    stages = [[], [], []]
    n = 0
    for g, pieces in enumerate(acts):
        for i, r0, r1 in pieces:
            for s in range(3):
                lo, hi = max(r0, s * UNITS), min(r1, (s + 1) * UNITS)
                if lo < hi:
                    stages[s].append(pltpu.make_async_copy(
                        ins[i].at[pl.ds(lo - r0, hi - lo)], a.at[pl.ds(lo, hi - lo), pl.ds(g * TOK, TOK)], sa.at[n]))
                    n += 1
    columns(ins[n_acts:], z, y, lambda src, to: stages[0].append(
        pltpu.make_async_copy(src, to, sc.at[0, len(stages[0])])), cols.at[0], 0)
    columns(ins[n_acts:], z, y, lambda src, to: stages[2].append(
        pltpu.make_async_copy(src, to, sc.at[1, len(stages[2])])), cols.at[1], 1)
    if has_base:
        for s in range(3):
            stages[s].append(pltpu.make_async_copy(ins[n_in - 3 + s], total.at[s], sb.at[s]))

    def begin(s):
        for c in stages[s]:
            c.start()

    begin(0)
    begin(1)
    done = [pltpu.make_async_copy(total.at[i], outs[i], so.at[i]) for i in range(3)]

    def product(i, _):
        for n in range(3):
            @pl.when(i == n)
            def _():
                if n:
                    done[n - 1].start()
                for c in stages[n]:
                    c.wait()
                if n == 0:
                    begin(2)

        rows = pl.ds(pl.multiple_of(i * UNITS, 16), UNITS)
        v = dot(a[rows, :], cols[i // 2].reshape(len(acts) * TOK, DEPTH), 1, 0)
        total[i] = total[i] + v if has_base else v
        return 0

    lax.fori_loop(0, 3, product, 0)
    done[2].start()
    for c in done:
        c.wait()


def near_columns(refs, z, y, add, buf, kind):
    x_own, d_own, side = refs[:3]
    add(d_own if kind else x_own, buf.at[0])
    for h in range(2):
        add(side.at[pl.ds(3 * UNITS + (2 * kind + h) * TOK, TOK)], buf.at[1, :, pl.ds(h * TOK, TOK)])


def plane_columns(first_group, count, refs, z, y, add, buf, kind):
    for i, off in enumerate(WHOLE):
        for j in range(4):
            a, b = lax.rem(z + j, 4), lax.rem(y + off, 4)
            if kind:
                a, b = lax.rem(z + off, 4), lax.rem(y + j, 4)
            add(refs[4 * kind + i].at[j, pl.ds(first_group, count)], buf.at[:, a * 4 + b])


def weight_sums(groups, columns, arrays, base):
    ins, acts = [], []
    for pieces in groups:
        row, marks = 0, []
        for p, m in pieces:
            marks.append((len(ins), row, row + m))
            ins.append(p)
            row += m
        acts.append(marks)
    n_acts = len(ins)
    ins += list(arrays) + list(base or [])
    n = len(groups)
    col = (2, n, TOK, DEPTH) if columns is near_columns else (2, n, 16, ROWS, DEPTH)
    out = jax.ShapeDtypeStruct((UNITS, DEPTH), F32)
    return call(
        functools.partial(weight_kernel, acts, n_acts, columns, base is not None, len(ins)),
        (out,) * 3,
        [
            pltpu.VMEM((3 * UNITS, n * TOK), BF), pltpu.VMEM(col, BF),
            pltpu.VMEM((3, UNITS, DEPTH), F32),
            pltpu.SemaphoreType.DMA((3 * n_acts,)), pltpu.SemaphoreType.DMA((2, 48)),
            pltpu.SemaphoreType.DMA((3,)), pltpu.SemaphoreType.DMA((3,)),
        ],
        2 * 3 * UNITS * DEPTH * n * TOK,
        [ANY] * len(ins),
        (ANY,) * 3,
        ins,
        n * (4 << 20) + (16 << 20),
    )


def block(inputs, w_gate, w_up, w_down, d_out):
    fs = lax.axis_index("fs")

    def relative(v, fs=fs):
        parts = [v[:, i * DEPTH:(i + 1) * DEPTH] for i in range(4)]
        out = []
        for k in range(4):
            w = parts[k]
            for f in range(1, 4):
                w = jnp.where(fs == f, parts[f ^ k], w)
            out.append(w)
        return out

    mark = lax.optimization_barrier(fs) * 3 - 1
    mark = (mark + 1) // 3

    xp, dp = relative(inputs), relative(d_out)
    x_own, d_own = jnp.concatenate(xp, axis=1), jnp.concatenate(dp, axis=1)

    def spread(own, first, second, whole=False):
        own = own[None]
        one, two, three = (moved(own, **{first: d}) for d in (1, 2, 3))
        if whole:
            line = jnp.concatenate([own, one, two, three], axis=0)
            return (line, *(moved(line, **{second: d}) for d in (1, -1, 2)))
        low, high = jnp.concatenate([own, one], axis=0), jnp.concatenate([two, three], axis=0)
        up_l, up_h = moved(low, **{second: 1}), moved(high, **{second: 1})
        down_l, down_h = moved(low, **{second: -1}), moved(high, **{second: -1})
        far_l, far_h = moved(up_l, **{second: 1}), moved(down_h, **{second: -1})
        return low, high, up_l, up_h, down_l, down_h, far_l, far_h

    xs = spread(x_own, "dz", "dy")
    ds = spread(d_own, "dy", "dz")

    side = moved(jnp.stack([xp[1], dp[1], xp[3], dp[3]]), flip=1)
    far = jnp.stack([xp[0], side[0], dp[0], side[1]])
    near = jnp.stack([xp[2], side[2], dp[2], side[3]])
    got = (moved(near, dx=1), moved(near, dx=-1), moved(far, dx=2))
    xcs = spread(jnp.concatenate([v[:2] for v in got], axis=0), "dz", "dy", True)
    dcs = spread(jnp.concatenate([v[2:] for v in got], axis=0), "dy", "dz", True)

    wa = jnp.concatenate([w_gate.T, w_down[:CUT]], axis=0)
    wb = jnp.concatenate([w_up.T, w_down[CUT:]], axis=0)
    wa2, wb2 = moved(wa, dx=1), moved(wb, dx=-1)
    wa1, wb1 = moved(wa, flip=1), moved(wb, flip=1)
    wa3, wb3 = moved(wa2, flip=1), moved(wb2, flip=1)
    was, wbs = (wa, wa1, wa2, wa3), (wb, wb1, wb2, wb3)

    acts_l, acts_h, own, x_cols, d_cols = forward(xs, ds, was, wbs)

    aml, aph = moved(acts_l, dx=1), moved(acts_h, dx=-1)
    amh, apl = moved(acts_h, dx=1), moved(acts_l, dx=-1)
    side = moved(own, flip=1)
    oa, ob = moved(aml, dx=1), moved(aph, dx=-1)
    sml, sph = moved(aml, flip=1), moved(aph, flip=1)
    smh, spl = moved(amh, flip=1), moved(apl, flip=1)
    soa, sob = moved(oa, flip=1), moved(ob, flip=1)

    packed = input_sums(own, was, wbs).astype(F16)
    got = lax.all_to_all(packed.reshape(16, ROWS, WIDE + TAIL), "tp", 0, 0)
    back = lax.optimization_barrier(jnp.exp2(got[:, 0, WIDE].astype(F32) - 14.0))
    total = 0.0
    for i in range(16):
        total = total + got[i, :, :WIDE].astype(F32) * back[i]
    grad_inputs = jnp.concatenate(relative(total.astype(BF), mark), axis=1)

    full = 3 * UNITS

    def halves(low, high):
        return [(low, LOW), (high, HIGH)]

    sums = weight_sums(
        [[(own, full)], [(side, full)]], near_columns, (x_cols, d_cols, side), None)
    sums = weight_sums(
        [halves(aml, amh), halves(sml, smh), halves(apl, aph), halves(spl, sph)],
        functools.partial(plane_columns, 0, 4), (*xcs, *dcs), sums)
    sums = weight_sums(
        [halves(oa, ob), halves(soa, sob)], functools.partial(plane_columns, 4, 2), (*xcs, *dcs), sums)
    return grad_inputs, sums[0].T, sums[1].T, sums[2]


def solution(mesh):
    tok = P(AXES, None)
    return jax.shard_map(
        block,
        mesh=mesh,
        in_specs=(tok, P("fs", "tp"), P("fs", "tp"), P("tp", "fs"), tok),
        out_specs=(tok, P("fs", "tp"), P("fs", "tp"), P("tp", "fs")),
        check_vma=False,
    )
```

```python
import functools

import jax
import jax.numpy as jnp
from jax import lax
from jax.experimental import pallas as pl
from jax.experimental.pallas import tpu as pltpu
from jax.sharding import PartitionSpec as P


AXES = ("rep", "fs", "tp")
BF, F32, F16 = jnp.bfloat16, jnp.float32, jnp.float16
W_MAX = 0.09375
ANY = pl.BlockSpec(memory_space=pl.ANY)
VMEM = pl.BlockSpec(memory_space=pltpu.VMEM)
LIMIT = 56 * 1024 * 1024

ROWS, DEPTH, UNITS = 32, 1024, 688
TOK, WIDE = 16 * ROWS, 4 * DEPTH
CUT = 336
LOW, HIGH = 1040, 1024
HALF = 2 * DEPTH
TAIL = 128


def index_of(x, c, z, y):
    x, z, y = x % 4, z % 4, y % 4
    return (x // 2) * 64 + ((x % 2) * 2 + c) * 16 + z * 4 + y


def moved(array, dx=0, flip=0, dz=0, dy=0):
    pairs = []
    for x in range(4):
        for c in range(2):
            for z in range(4):
                for y in range(4):
                    pairs.append((index_of(x + dx, c ^ flip, z + dz, y + dy), index_of(x, c, z, y)))
    return lax.ppermute(array, AXES, pairs)


def dot(a, b, ca, cb):
    return lax.dot_general(a, b, (((ca,), (cb,)), ((), ())), preferred_element_type=F32)


def place():
    tp = lax.axis_index("tp")
    return tp // 4, tp % 4


def call(body, out_shape, scratch, flops, ins, outs, args, nbytes):
    return pl.pallas_call(
        body,
        out_shape=out_shape,
        in_specs=ins,
        out_specs=outs,
        scratch_shapes=scratch,
        compiler_params=pltpu.CompilerParams(vmem_limit_bytes=LIMIT),
        cost_estimate=pl.CostEstimate(flops=flops, bytes_accessed=nbytes, transcendentals=0),
    )(*args)


FROM = ((0, 0), (2, 0), (0, 1), (2, 1), (0, 3), (2, 3), (0, 2), (2, 2))
WHOLE = (0, 1, 3, 2)


def forward_kernel(*refs):
    xs, ds, was, wbs = refs[:8], refs[8:16], refs[16:20], refs[20:24]
    acts_l, acts_h, side, x_own, d_own = refs[24:29]
    v, w, sums, act, sx, sd, sw, so = refs[29:]
    z, y = place()
    x_copies, d_copies = [], []
    for i, (first, off) in enumerate(FROM):
        for j in range(2):
            row = pl.multiple_of((lax.rem(z + first + j, 4) * 4 + lax.rem(y + off, 4)) * ROWS, ROWS)
            x_copies.append(
                pltpu.make_async_copy(xs[i].at[j], v.at[0, pl.ds(row, ROWS)], sx.at[len(x_copies)]))
            row = pl.multiple_of((lax.rem(z + off, 4) * 4 + lax.rem(y + first + j, 4)) * ROWS, ROWS)
            d_copies.append(
                pltpu.make_async_copy(ds[i].at[j], v.at[1, pl.ds(row, ROWS)], sd.at[len(d_copies)]))
    rest = UNITS - CUT
    w_copies = [
        [
            pltpu.make_async_copy(was[k].at[pl.ds(0, UNITS)], w.at[k, 0], sw.at[4 * k]),
            pltpu.make_async_copy(wbs[k].at[pl.ds(0, UNITS)], w.at[k, 1], sw.at[4 * k + 1]),
            pltpu.make_async_copy(was[k].at[pl.ds(UNITS, CUT)], w.at[k, 2, pl.ds(0, CUT)], sw.at[4 * k + 2]),
            pltpu.make_async_copy(wbs[k].at[pl.ds(UNITS, rest)], w.at[k, 2, pl.ds(CUT, rest)], sw.at[4 * k + 3]),
        ]
        for k in range(4)
    ]
    stages = [x_copies + w_copies[0][:2], d_copies + w_copies[0][2:], w_copies[1], w_copies[2], w_copies[3]]

    def begin(n):
        for c in stages[n]:
            c.start()

    def end(n):
        for c in stages[n]:
            c.wait()

    begin(0)
    begin(1)
    sums[...] = jnp.zeros_like(sums)
    end(0)
    begin(2)

    outs = []
    for i, to in enumerate((x_own, d_own)):
        outs.append(pltpu.make_async_copy(v.at[i, :, pl.ds(0, DEPTH)], to, so.at[i]))
        for h in range(2):
            outs.append(pltpu.make_async_copy(
                v.at[i, :, pl.ds(DEPTH + h * TOK, TOK)],
                side.at[pl.ds(3 * UNITS + (2 * i + h) * TOK, TOK)], so.at[2 + 2 * i + h]))

    def product(n, _):
        k, i = n // 3, lax.rem(n, 3)

        @pl.when(n == 2)
        def _():
            end(1)
            begin(3)

        @pl.when(n == 3)
        def _():
            end(2)
            begin(4)

        @pl.when(n == 6)
        def _():
            end(3)

        @pl.when(n == 9)
        def _():
            end(4)
            for c in outs:
                c.start()

        sums[i] = sums[i] + dot(w[k, i], v[i // 2, :, pl.ds(pl.multiple_of(k * DEPTH, DEPTH), DEPTH)], 1, 1)
        return 0

    lax.fori_loop(0, 12, product, 0)

    def unit(i, _):
        r = pl.ds(pl.multiple_of(i * 16, 16), 16)
        g = sums[0, r, :].astype(BF).astype(F32)
        u = sums[1, r, :].astype(BF).astype(F32)
        b = sums[2, r, :].astype(BF).astype(F32)
        sigma = 1.0 / (1.0 + jnp.exp(-g))
        active = g * sigma
        act[r, :] = (b * u * sigma * (1.0 + g * (1.0 - sigma))).astype(BF)
        act[pl.ds(pl.multiple_of(UNITS + i * 16, 16), 16), :] = (b * active).astype(BF)
        act[pl.ds(pl.multiple_of(2 * UNITS + i * 16, 16), 16), :] = (active * u).astype(BF)
        return 0

    lax.fori_loop(0, UNITS // 16, unit, 0)
    outs.append(pltpu.make_async_copy(act.at[pl.ds(0, LOW)], acts_l, so.at[6]))
    outs.append(pltpu.make_async_copy(act.at[pl.ds(LOW, HIGH)], acts_h, so.at[7]))
    outs.append(pltpu.make_async_copy(act, side.at[pl.ds(0, 3 * UNITS)], so.at[8]))
    for c in outs[-3:]:
        c.start()
    for c in outs:
        c.wait()


def forward(xs, ds, was, wbs):
    shape = jax.ShapeDtypeStruct
    return call(
        forward_kernel,
        (shape((LOW, TOK), BF), shape((HIGH, TOK), BF), shape((3 * UNITS + 4 * TOK, TOK), BF),
         shape((TOK, DEPTH), BF), shape((TOK, DEPTH), BF)),
        [
            pltpu.VMEM((2, TOK, WIDE), BF), pltpu.VMEM((4, 3, UNITS, DEPTH), BF), pltpu.VMEM((3, UNITS, TOK), F32),
            pltpu.VMEM((3 * UNITS, TOK), BF),
            pltpu.SemaphoreType.DMA((16,)), pltpu.SemaphoreType.DMA((16,)),
            pltpu.SemaphoreType.DMA((16,)), pltpu.SemaphoreType.DMA((9,)),
        ],
        2 * TOK * WIDE * UNITS * 3,
        [ANY] * 24,
        (ANY,) * 5,
        (*xs, *ds, *was, *wbs),
        34 << 20,
    )


def input_kernel(*refs):
    acts, was, wbs = refs[0], refs[1:5], refs[5:9]
    own, away = refs[9:11], refs[11:13]
    act, wa, wb, tg, tu, total, expo, sw, so, st, sl = refs[13:]
    z, y = place()
    load = pltpu.make_async_copy(acts.at[pl.ds(0, 2 * UNITS)], act, sl.at[0])
    load.start()
    copies = [
        (pltpu.make_async_copy(was[k].at[pl.ds(0, UNITS)], wa.at[k], sw.at[2 * k]),
         pltpu.make_async_copy(wbs[k].at[pl.ds(0, UNITS)], wb.at[k], sw.at[2 * k + 1]))
        for k in range(4)
    ]
    for pair in copies[:2]:
        for c in pair:
            c.start()
    load.wait()
    tg[...] = act[:UNITS, :].T
    tu[...] = act[UNITS:, :].T
    norm = jnp.sum(jnp.abs(tg[...].astype(F32)), axis=1, keepdims=True)
    norm = norm + jnp.sum(jnp.abs(tu[...].astype(F32)), axis=1, keepdims=True)
    e = jnp.ceil(jnp.log2(jnp.maximum(jnp.max(norm, axis=0, keepdims=True) * (1.02 * W_MAX), 1e-30)))
    expo[...] = jnp.broadcast_to(e, (TOK, TAIL))

    def puts(src, side, cols, sems):
        out = []
        for s in range(4):
            to = own[side] if s == 0 else away[side].at[s - 1]
            if side == 0:
                r = pl.ds(pl.multiple_of(lax.rem(z + s, 4) * (4 * ROWS), 4 * ROWS), 4 * ROWS)
                out.append(pltpu.make_async_copy(src.at[r], to.at[:, cols], sems.at[s]))
            else:
                for i in range(4):
                    r = pl.ds(pl.multiple_of((i * 4 + lax.rem(y + s, 4)) * ROWS, ROWS), ROWS)
                    out.append(pltpu.make_async_copy(src.at[r], to.at[pl.ds(i * ROWS, ROWS), cols], sems.at[4 * s + i]))
        return out

    tails = [c for side in range(2) for c in puts(expo, side, pl.ds(HALF, TAIL), st.at[side])]
    for c in tails:
        c.start()
    parts = [puts(total.at[k % 2], k // 2, pl.ds((k % 2) * DEPTH, DEPTH), so.at[k]) for k in range(4)]

    def part(k, _):
        for n in range(4):
            @pl.when(k == n)
            def _():
                for c in copies[n]:
                    c.wait()
                if n + 2 < 4:
                    for c in copies[n + 2]:
                        c.start()
                if n >= 2:
                    for c in parts[n - 2]:
                        c.wait()

        def tile(j, _):
            n = pl.ds(pl.multiple_of(j * 512, 512), 512)
            v = dot(tg[...], wa[k, :, n], 1, 0) + dot(tu[...], wb[k, :, n], 1, 0)
            total[lax.rem(k, 2), :, n] = v * jnp.exp2(14.0 - expo[:, :1])
            return 0

        lax.fori_loop(0, 2, tile, 0)
        for n in range(4):
            @pl.when(k == n)
            def _():
                for c in parts[n]:
                    c.start()
        return 0

    lax.fori_loop(0, 4, part, 0)
    for c in parts[2] + parts[3] + tails:
        c.wait()


def input_sums(acts, was, wbs):
    shape = jax.ShapeDtypeStruct
    own, away = shape((4 * ROWS, HALF + TAIL), F32), shape((3, 4 * ROWS, HALF + TAIL), F32)
    return call(
        input_kernel,
        (own, own, away, away),
        [
            pltpu.VMEM((2 * UNITS, TOK), BF),
            pltpu.VMEM((4, UNITS, DEPTH), BF), pltpu.VMEM((4, UNITS, DEPTH), BF),
            pltpu.VMEM((TOK, UNITS), BF), pltpu.VMEM((TOK, UNITS), BF),
            pltpu.VMEM((2, TOK, DEPTH), F32), pltpu.VMEM((TOK, TAIL), F32),
            pltpu.SemaphoreType.DMA((8,)), pltpu.SemaphoreType.DMA((4, 16)), pltpu.SemaphoreType.DMA((2, 16)),
            pltpu.SemaphoreType.DMA((1,)),
        ],
        2 * TOK * WIDE * UNITS * 2,
        [ANY] * 9,
        (ANY,) * 4,
        (acts, *was, *wbs),
        22 << 20,
    )


def join_kernel(own_a, own_b, got, to_a, to_b):
    z, y = place()
    for own, first, to, at in ((own_a, 0, to_a, y), (own_b, 3, to_b, z)):
        for s in range(4):
            r = pl.ds(pl.multiple_of(lax.rem(at + s, 4) * ROWS, ROWS), ROWS)
            v = own[r, :HALF] * jnp.exp2(own[r, HALF:HALF + 1] - 14.0)
            for i in range(first, first + 3):
                v = v + got[i, r, :HALF] * jnp.exp2(got[i, r, HALF:HALF + 1] - 14.0)
            to[s] = v


def joined(own_a, own_b, got):
    out = jax.ShapeDtypeStruct((4, ROWS, HALF), F32)
    return call(join_kernel, (out, out), [], 1 << 30, [VMEM] * 3, (VMEM,) * 2, (own_a, own_b, got), 12 << 20)


def weight_kernel(acts, n_acts, columns, has_base, n_in, *refs):
    ins, outs = refs[:n_in], refs[n_in:n_in + 3]
    a, cols, total, sa, sc, sb, so = refs[n_in + 3:]
    z, y = place()
    stages = [[], [], []]
    n = 0
    for g, pieces in enumerate(acts):
        for i, r0, r1 in pieces:
            for s in range(3):
                lo, hi = max(r0, s * UNITS), min(r1, (s + 1) * UNITS)
                if lo < hi:
                    stages[s].append(pltpu.make_async_copy(
                        ins[i].at[pl.ds(lo - r0, hi - lo)], a.at[pl.ds(lo, hi - lo), pl.ds(g * TOK, TOK)], sa.at[n]))
                    n += 1
    columns(ins[n_acts:], z, y, lambda src, to: stages[0].append(
        pltpu.make_async_copy(src, to, sc.at[0, len(stages[0])])), cols.at[0], 0)
    columns(ins[n_acts:], z, y, lambda src, to: stages[2].append(
        pltpu.make_async_copy(src, to, sc.at[1, len(stages[2])])), cols.at[1], 1)
    if has_base:
        for s in range(3):
            stages[s].append(pltpu.make_async_copy(ins[n_in - 3 + s], total.at[s], sb.at[s]))

    def begin(s):
        for c in stages[s]:
            c.start()

    begin(0)
    begin(1)
    done = [pltpu.make_async_copy(total.at[i], outs[i], so.at[i]) for i in range(3)]

    def product(i, _):
        for n in range(3):
            @pl.when(i == n)
            def _():
                if n:
                    done[n - 1].start()
                for c in stages[n]:
                    c.wait()
                if n == 0:
                    begin(2)

        rows = pl.ds(pl.multiple_of(i * UNITS, 16), UNITS)
        v = dot(a[rows, :], cols[i // 2].reshape(len(acts) * TOK, DEPTH), 1, 0)
        total[i] = total[i] + v if has_base else v
        return 0

    lax.fori_loop(0, 3, product, 0)
    done[2].start()
    for c in done:
        c.wait()


def near_columns(refs, z, y, add, buf, kind):
    x_own, d_own, side = refs[:3]
    add(d_own if kind else x_own, buf.at[0])
    for h in range(2):
        add(side.at[pl.ds(3 * UNITS + (2 * kind + h) * TOK, TOK)], buf.at[1, :, pl.ds(h * TOK, TOK)])


def plane_columns(first_group, count, refs, z, y, add, buf, kind):
    for i, off in enumerate(WHOLE):
        for j in range(4):
            a, b = lax.rem(z + j, 4), lax.rem(y + off, 4)
            if kind:
                a, b = lax.rem(z + off, 4), lax.rem(y + j, 4)
            add(refs[4 * kind + i].at[j, pl.ds(first_group, count)], buf.at[:, a * 4 + b])


def weight_sums(groups, columns, arrays, base):
    ins, acts = [], []
    for pieces in groups:
        row, marks = 0, []
        for p, m in pieces:
            marks.append((len(ins), row, row + m))
            ins.append(p)
            row += m
        acts.append(marks)
    n_acts = len(ins)
    ins += list(arrays) + list(base or [])
    n = len(groups)
    col = (2, n, TOK, DEPTH) if columns is near_columns else (2, n, 16, ROWS, DEPTH)
    out = jax.ShapeDtypeStruct((UNITS, DEPTH), F32)
    return call(
        functools.partial(weight_kernel, acts, n_acts, columns, base is not None, len(ins)),
        (out,) * 3,
        [
            pltpu.VMEM((3 * UNITS, n * TOK), BF), pltpu.VMEM(col, BF),
            pltpu.VMEM((3, UNITS, DEPTH), F32),
            pltpu.SemaphoreType.DMA((3 * n_acts,)), pltpu.SemaphoreType.DMA((2, 48)),
            pltpu.SemaphoreType.DMA((3,)), pltpu.SemaphoreType.DMA((3,)),
        ],
        2 * 3 * UNITS * DEPTH * n * TOK,
        [ANY] * len(ins),
        (ANY,) * 3,
        ins,
        n * (4 << 20) + (16 << 20),
    )


def block(inputs, w_gate, w_up, w_down, d_out):
    fs = lax.axis_index("fs")

    def relative(v, fs=fs):
        parts = [v[:, i * DEPTH:(i + 1) * DEPTH] for i in range(4)]
        out = []
        for k in range(4):
            w = parts[k]
            for f in range(1, 4):
                w = jnp.where(fs == f, parts[f ^ k], w)
            out.append(w)
        return out

    mark = lax.optimization_barrier(fs) * 3 - 1
    mark = (mark + 1) // 3

    xp, dp = relative(inputs), relative(d_out)
    x_own, d_own = jnp.concatenate(xp, axis=1), jnp.concatenate(dp, axis=1)

    def spread(own, first, second, whole=False):
        own = own[None]
        one, two, three = (moved(own, **{first: d}) for d in (1, 2, 3))
        if whole:
            line = jnp.concatenate([own, one, two, three], axis=0)
            return (line, *(moved(line, **{second: d}) for d in (1, -1, 2)))
        low, high = jnp.concatenate([own, one], axis=0), jnp.concatenate([two, three], axis=0)
        up_l, up_h = moved(low, **{second: 1}), moved(high, **{second: 1})
        down_l, down_h = moved(low, **{second: -1}), moved(high, **{second: -1})
        far_l, far_h = moved(up_l, **{second: 1}), moved(down_h, **{second: -1})
        return low, high, up_l, up_h, down_l, down_h, far_l, far_h

    xs = spread(x_own, "dz", "dy")
    ds = spread(d_own, "dy", "dz")

    side = moved(jnp.stack([xp[1], dp[1], xp[3], dp[3]]), flip=1)
    far = jnp.stack([xp[0], side[0], dp[0], side[1]])
    near = jnp.stack([xp[2], side[2], dp[2], side[3]])
    got = (moved(near, dx=1), moved(near, dx=-1), moved(far, dx=2))
    xcs = spread(jnp.concatenate([v[:2] for v in got], axis=0), "dz", "dy", True)
    dcs = spread(jnp.concatenate([v[2:] for v in got], axis=0), "dy", "dz", True)

    wa = jnp.concatenate([w_gate.T, w_down[:CUT]], axis=0)
    wb = jnp.concatenate([w_up.T, w_down[CUT:]], axis=0)
    wa2, wb2 = moved(wa, dx=1), moved(wb, dx=-1)
    wa1, wb1 = moved(wa, flip=1), moved(wb, flip=1)
    wa3, wb3 = moved(wa2, flip=1), moved(wb2, flip=1)
    was, wbs = (wa, wa1, wa2, wa3), (wb, wb1, wb2, wb3)

    acts_l, acts_h, own, x_cols, d_cols = forward(xs, ds, was, wbs)

    aml, aph = moved(acts_l, dx=1), moved(acts_h, dx=-1)
    amh, apl = moved(acts_h, dx=1), moved(acts_l, dx=-1)
    side = moved(own, flip=1)
    oa, ob = moved(aml, dx=1), moved(aph, dx=-1)
    sml, sph = moved(aml, flip=1), moved(aph, flip=1)
    smh, spl = moved(amh, flip=1), moved(apl, flip=1)
    soa, sob = moved(oa, flip=1), moved(ob, flip=1)

    own_a, own_b, qa, qb = input_sums(own, was, wbs)
    qa, qb = qa.astype(F16), qb.astype(F16)
    got = [moved(qa[d - 1], dz=-d) for d in (1, 2, 3)] + [moved(qb[d - 1], dy=-d) for d in (1, 2, 3)]
    fa, fb = joined(own_a, own_b, jnp.stack(got).astype(F32))
    fa = fa[0] + moved(fa[1], dy=-1) + moved(fa[2], dy=-2) + moved(fa[3], dy=-3)
    fb = fb[0] + moved(fb[1], dz=-1) + moved(fb[2], dz=-2) + moved(fb[3], dz=-3)
    total = jnp.concatenate([fa, fb], axis=1)
    grad_inputs = jnp.concatenate(relative(total.astype(BF), mark), axis=1)

    full = 3 * UNITS

    def halves(low, high):
        return [(low, LOW), (high, HIGH)]

    sums = weight_sums(
        [[(own, full)], [(side, full)]], near_columns, (x_cols, d_cols, side), None)
    sums = weight_sums(
        [halves(aml, amh), halves(sml, smh), halves(apl, aph), halves(spl, sph)],
        functools.partial(plane_columns, 0, 4), (*xcs, *dcs), sums)
    sums = weight_sums(
        [halves(oa, ob), halves(soa, sob)], functools.partial(plane_columns, 4, 2), (*xcs, *dcs), sums)
    return grad_inputs, sums[0].T, sums[1].T, sums[2]


def solution(mesh):
    tok = P(AXES, None)
    return jax.shard_map(
        block,
        mesh=mesh,
        in_specs=(tok, P("fs", "tp"), P("fs", "tp"), P("tp", "fs"), tok),
        out_specs=(tok, P("fs", "tp"), P("fs", "tp"), P("tp", "fs")),
        check_vma=False,
    )
```

```python
import functools

import jax
import jax.numpy as jnp
from jax import lax
from jax.experimental import pallas as pl
from jax.experimental.pallas import tpu as pltpu
from jax.sharding import PartitionSpec as P


AXES = ("rep", "fs", "tp")
BF, F32, F16 = jnp.bfloat16, jnp.float32, jnp.float16
W_MAX = 0.09375
ANY = pl.BlockSpec(memory_space=pl.ANY)
VMEM = pl.BlockSpec(memory_space=pltpu.VMEM)
LIMIT = 56 * 1024 * 1024

ROWS, DEPTH, UNITS = 32, 1024, 688
TOK, WIDE = 16 * ROWS, 4 * DEPTH
CUT = 336
LOW, HIGH = 1040, 1024
HALF = 2 * DEPTH
TAIL = 128


def index_of(x, c, z, y):
    x, z, y = x % 4, z % 4, y % 4
    return (x // 2) * 64 + ((x % 2) * 2 + c) * 16 + z * 4 + y


def moved(array, dx=0, flip=0, dz=0, dy=0):
    pairs = []
    for x in range(4):
        for c in range(2):
            for z in range(4):
                for y in range(4):
                    pairs.append((index_of(x + dx, c ^ flip, z + dz, y + dy), index_of(x, c, z, y)))
    return lax.ppermute(array, AXES, pairs)


def dot(a, b, ca, cb):
    return lax.dot_general(a, b, (((ca,), (cb,)), ((), ())), preferred_element_type=F32)


def place():
    tp = lax.axis_index("tp")
    return tp // 4, tp % 4


def call(body, out_shape, scratch, flops, ins, outs, args, nbytes):
    return pl.pallas_call(
        body,
        out_shape=out_shape,
        in_specs=ins,
        out_specs=outs,
        scratch_shapes=scratch,
        compiler_params=pltpu.CompilerParams(vmem_limit_bytes=LIMIT),
        cost_estimate=pl.CostEstimate(flops=flops, bytes_accessed=nbytes, transcendentals=0),
    )(*args)


FROM = ((0, 0), (2, 0), (0, 1), (2, 1), (0, 3), (2, 3), (0, 2), (2, 2))
WHOLE = (0, 1, 3, 2)


def forward_kernel(*refs):
    xs, ds, was, wbs = refs[:8], refs[8:16], refs[16:20], refs[20:24]
    acts_l, acts_h, side, x_own, d_own = refs[24:29]
    v, w, sums, act, sx, sd, sw, so = refs[29:]
    z, y = place()
    x_copies, d_copies = [], []
    for i, (first, off) in enumerate(FROM):
        for j in range(2):
            row = pl.multiple_of((lax.rem(z + first + j, 4) * 4 + lax.rem(y + off, 4)) * ROWS, ROWS)
            x_copies.append(
                pltpu.make_async_copy(xs[i].at[j], v.at[0, pl.ds(row, ROWS)], sx.at[len(x_copies)]))
            row = pl.multiple_of((lax.rem(z + off, 4) * 4 + lax.rem(y + first + j, 4)) * ROWS, ROWS)
            d_copies.append(
                pltpu.make_async_copy(ds[i].at[j], v.at[1, pl.ds(row, ROWS)], sd.at[len(d_copies)]))
    rest = UNITS - CUT
    w_copies = [
        [
            pltpu.make_async_copy(was[k].at[pl.ds(0, UNITS)], w.at[k, 0], sw.at[4 * k]),
            pltpu.make_async_copy(wbs[k].at[pl.ds(0, UNITS)], w.at[k, 1], sw.at[4 * k + 1]),
            pltpu.make_async_copy(was[k].at[pl.ds(UNITS, CUT)], w.at[k, 2, pl.ds(0, CUT)], sw.at[4 * k + 2]),
            pltpu.make_async_copy(wbs[k].at[pl.ds(UNITS, rest)], w.at[k, 2, pl.ds(CUT, rest)], sw.at[4 * k + 3]),
        ]
        for k in range(4)
    ]
    stages = [x_copies + w_copies[0][:2], d_copies + w_copies[0][2:], w_copies[1], w_copies[2], w_copies[3]]

    def begin(n):
        for c in stages[n]:
            c.start()

    def end(n):
        for c in stages[n]:
            c.wait()

    begin(0)
    begin(1)
    sums[...] = jnp.zeros_like(sums)
    end(0)
    begin(2)

    outs = []
    for i, to in enumerate((x_own, d_own)):
        outs.append(pltpu.make_async_copy(v.at[i, :, pl.ds(0, DEPTH)], to, so.at[i]))
        for h in range(2):
            outs.append(pltpu.make_async_copy(
                v.at[i, :, pl.ds(DEPTH + h * TOK, TOK)],
                side.at[pl.ds(3 * UNITS + (2 * i + h) * TOK, TOK)], so.at[2 + 2 * i + h]))

    def product(n, _):
        k, i = n // 3, lax.rem(n, 3)

        @pl.when(n == 2)
        def _():
            end(1)
            begin(3)

        @pl.when(n == 3)
        def _():
            end(2)
            begin(4)

        @pl.when(n == 6)
        def _():
            end(3)

        @pl.when(n == 9)
        def _():
            end(4)
            for c in outs:
                c.start()

        sums[i] = sums[i] + dot(w[k, i], v[i // 2, :, pl.ds(pl.multiple_of(k * DEPTH, DEPTH), DEPTH)], 1, 1)
        return 0

    lax.fori_loop(0, 12, product, 0)

    def unit(i, _):
        r = pl.ds(pl.multiple_of(i * 16, 16), 16)
        g = sums[0, r, :].astype(BF).astype(F32)
        u = sums[1, r, :].astype(BF).astype(F32)
        b = sums[2, r, :].astype(BF).astype(F32)
        sigma = 1.0 / (1.0 + jnp.exp(-g))
        active = g * sigma
        act[r, :] = (b * u * sigma * (1.0 + g * (1.0 - sigma))).astype(BF)
        act[pl.ds(pl.multiple_of(UNITS + i * 16, 16), 16), :] = (b * active).astype(BF)
        act[pl.ds(pl.multiple_of(2 * UNITS + i * 16, 16), 16), :] = (active * u).astype(BF)
        return 0

    lax.fori_loop(0, UNITS // 16, unit, 0)
    outs.append(pltpu.make_async_copy(act.at[pl.ds(0, LOW)], acts_l, so.at[6]))
    outs.append(pltpu.make_async_copy(act.at[pl.ds(LOW, HIGH)], acts_h, so.at[7]))
    outs.append(pltpu.make_async_copy(act, side.at[pl.ds(0, 3 * UNITS)], so.at[8]))
    for c in outs[-3:]:
        c.start()
    for c in outs:
        c.wait()


def forward(xs, ds, was, wbs):
    shape = jax.ShapeDtypeStruct
    return call(
        forward_kernel,
        (shape((LOW, TOK), BF), shape((HIGH, TOK), BF), shape((3 * UNITS + 4 * TOK, TOK), BF),
         shape((TOK, DEPTH), BF), shape((TOK, DEPTH), BF)),
        [
            pltpu.VMEM((2, TOK, WIDE), BF), pltpu.VMEM((4, 3, UNITS, DEPTH), BF), pltpu.VMEM((3, UNITS, TOK), F32),
            pltpu.VMEM((3 * UNITS, TOK), BF),
            pltpu.SemaphoreType.DMA((16,)), pltpu.SemaphoreType.DMA((16,)),
            pltpu.SemaphoreType.DMA((16,)), pltpu.SemaphoreType.DMA((9,)),
        ],
        2 * TOK * WIDE * UNITS * 3,
        [ANY] * 24,
        (ANY,) * 5,
        (*xs, *ds, *was, *wbs),
        34 << 20,
    )


def input_kernel(*refs):
    acts, was, wbs = refs[0], refs[1:5], refs[5:9]
    own, away = refs[9:11], refs[11:13]
    act, wa, wb, tg, tu, total, expo, sw, so, st, sl = refs[13:]
    z, y = place()
    load = pltpu.make_async_copy(acts.at[pl.ds(0, 2 * UNITS)], act, sl.at[0])
    load.start()
    copies = [
        (pltpu.make_async_copy(was[k].at[pl.ds(0, UNITS)], wa.at[k], sw.at[2 * k]),
         pltpu.make_async_copy(wbs[k].at[pl.ds(0, UNITS)], wb.at[k], sw.at[2 * k + 1]))
        for k in range(4)
    ]
    for pair in copies[:2]:
        for c in pair:
            c.start()
    load.wait()
    tg[...] = act[:UNITS, :].T
    tu[...] = act[UNITS:, :].T
    norm = jnp.sum(jnp.abs(tg[...].astype(F32)), axis=1, keepdims=True)
    norm = norm + jnp.sum(jnp.abs(tu[...].astype(F32)), axis=1, keepdims=True)
    e = jnp.ceil(jnp.log2(jnp.maximum(jnp.max(norm, axis=0, keepdims=True) * (1.02 * W_MAX), 1e-30)))
    expo[...] = jnp.broadcast_to(e, (TOK, TAIL))

    def puts(src, side, cols, sems):
        out = []
        for s in range(4):
            to = own[side] if s == 0 else away[side].at[s - 1]
            if side == 0:
                r = pl.ds(pl.multiple_of(lax.rem(z + s, 4) * (4 * ROWS), 4 * ROWS), 4 * ROWS)
                out.append(pltpu.make_async_copy(src.at[r], to.at[:, cols], sems.at[s]))
            else:
                for i in range(4):
                    r = pl.ds(pl.multiple_of((i * 4 + lax.rem(y + s, 4)) * ROWS, ROWS), ROWS)
                    out.append(pltpu.make_async_copy(src.at[r], to.at[pl.ds(i * ROWS, ROWS), cols], sems.at[4 * s + i]))
        return out

    tails = [c for side in range(2) for c in puts(expo, side, pl.ds(HALF, TAIL), st.at[side])]
    for c in tails:
        c.start()
    parts = [puts(total.at[k % 2], k // 2, pl.ds((k % 2) * DEPTH, DEPTH), so.at[k]) for k in range(4)]

    def part(k, _):
        for n in range(4):
            @pl.when(k == n)
            def _():
                for c in copies[n]:
                    c.wait()
                if n + 2 < 4:
                    for c in copies[n + 2]:
                        c.start()
                if n >= 2:
                    for c in parts[n - 2]:
                        c.wait()

        def tile(j, _):
            n = pl.ds(pl.multiple_of(j * 512, 512), 512)
            v = dot(tg[...], wa[k, :, n], 1, 0) + dot(tu[...], wb[k, :, n], 1, 0)
            total[lax.rem(k, 2), :, n] = v * jnp.exp2(14.0 - expo[:, :1])
            return 0

        lax.fori_loop(0, 2, tile, 0)
        for n in range(4):
            @pl.when(k == n)
            def _():
                for c in parts[n]:
                    c.start()
        return 0

    lax.fori_loop(0, 4, part, 0)
    for c in parts[2] + parts[3] + tails:
        c.wait()


def input_sums(acts, was, wbs):
    shape = jax.ShapeDtypeStruct
    own, away = shape((4 * ROWS, HALF + TAIL), F32), shape((3, 4 * ROWS, HALF + TAIL), F32)
    return call(
        input_kernel,
        (own, own, away, away),
        [
            pltpu.VMEM((2 * UNITS, TOK), BF),
            pltpu.VMEM((4, UNITS, DEPTH), BF), pltpu.VMEM((4, UNITS, DEPTH), BF),
            pltpu.VMEM((TOK, UNITS), BF), pltpu.VMEM((TOK, UNITS), BF),
            pltpu.VMEM((2, TOK, DEPTH), F32), pltpu.VMEM((TOK, TAIL), F32),
            pltpu.SemaphoreType.DMA((8,)), pltpu.SemaphoreType.DMA((4, 16)), pltpu.SemaphoreType.DMA((2, 16)),
            pltpu.SemaphoreType.DMA((1,)),
        ],
        2 * TOK * WIDE * UNITS * 2,
        [ANY] * 9,
        (ANY,) * 4,
        (acts, *was, *wbs),
        22 << 20,
    )


def join_kernel(*refs):
    z, y = place()
    for side, at in ((0, y), (1, z)):
        own, got, out = refs[side], refs[2 + 3 * side:5 + 3 * side], refs[8 + 4 * side:12 + 4 * side]
        for s in range(4):
            r = pl.ds(pl.multiple_of(lax.rem(at + s, 4) * ROWS, ROWS), ROWS)
            v = own[r, :HALF] * jnp.exp2(own[r, HALF:HALF + 1] - 14.0)
            for g in got:
                v = v + g[r, :HALF] * jnp.exp2(g[r, HALF:HALF + 1] - 14.0)
            out[s][...] = v


def joined(own_a, own_b, got):
    out = jax.ShapeDtypeStruct((ROWS, HALF), F32)
    kept = call(join_kernel, (out,) * 8, [], 1 << 30, [VMEM] * 8, (VMEM,) * 8, (own_a, own_b, *got), 12 << 20)
    return kept[:4], kept[4:]


def weight_kernel(acts, n_acts, columns, has_base, n_in, *refs):
    ins, outs = refs[:n_in], refs[n_in:n_in + 3]
    a, cols, total, sa, sc, sb, so = refs[n_in + 3:]
    z, y = place()
    stages = [[], [], []]
    n = 0
    for g, pieces in enumerate(acts):
        for i, r0, r1 in pieces:
            for s in range(3):
                lo, hi = max(r0, s * UNITS), min(r1, (s + 1) * UNITS)
                if lo < hi:
                    stages[s].append(pltpu.make_async_copy(
                        ins[i].at[pl.ds(lo - r0, hi - lo)], a.at[pl.ds(lo, hi - lo), pl.ds(g * TOK, TOK)], sa.at[n]))
                    n += 1
    columns(ins[n_acts:], z, y, lambda src, to: stages[0].append(
        pltpu.make_async_copy(src, to, sc.at[0, len(stages[0])])), cols.at[0], 0)
    columns(ins[n_acts:], z, y, lambda src, to: stages[2].append(
        pltpu.make_async_copy(src, to, sc.at[1, len(stages[2])])), cols.at[1], 1)
    if has_base:
        for s in range(3):
            stages[s].append(pltpu.make_async_copy(ins[n_in - 3 + s], total.at[s], sb.at[s]))

    def begin(s):
        for c in stages[s]:
            c.start()

    begin(0)
    begin(1)
    done = [pltpu.make_async_copy(total.at[i], outs[i], so.at[i]) for i in range(3)]

    def product(i, _):
        for n in range(3):
            @pl.when(i == n)
            def _():
                if n:
                    done[n - 1].start()
                for c in stages[n]:
                    c.wait()
                if n == 0:
                    begin(2)

        rows = pl.ds(pl.multiple_of(i * UNITS, 16), UNITS)
        v = dot(a[rows, :], cols[i // 2].reshape(len(acts) * TOK, DEPTH), 1, 0)
        total[i] = total[i] + v if has_base else v
        return 0

    lax.fori_loop(0, 3, product, 0)
    done[2].start()
    for c in done:
        c.wait()


def near_columns(refs, z, y, add, buf, kind):
    x_own, d_own, side = refs[:3]
    add(d_own if kind else x_own, buf.at[0])
    for h in range(2):
        add(side.at[pl.ds(3 * UNITS + (2 * kind + h) * TOK, TOK)], buf.at[1, :, pl.ds(h * TOK, TOK)])


def plane_columns(first_group, count, refs, z, y, add, buf, kind):
    for i, off in enumerate(WHOLE):
        for j in range(4):
            a, b = lax.rem(z + j, 4), lax.rem(y + off, 4)
            if kind:
                a, b = lax.rem(z + off, 4), lax.rem(y + j, 4)
            add(refs[4 * kind + i].at[j, pl.ds(first_group, count)], buf.at[:, a * 4 + b])


def weight_sums(groups, columns, arrays, base):
    ins, acts = [], []
    for pieces in groups:
        row, marks = 0, []
        for p, m in pieces:
            marks.append((len(ins), row, row + m))
            ins.append(p)
            row += m
        acts.append(marks)
    n_acts = len(ins)
    ins += list(arrays) + list(base or [])
    n = len(groups)
    col = (2, n, TOK, DEPTH) if columns is near_columns else (2, n, 16, ROWS, DEPTH)
    out = jax.ShapeDtypeStruct((UNITS, DEPTH), F32)
    return call(
        functools.partial(weight_kernel, acts, n_acts, columns, base is not None, len(ins)),
        (out,) * 3,
        [
            pltpu.VMEM((3 * UNITS, n * TOK), BF), pltpu.VMEM(col, BF),
            pltpu.VMEM((3, UNITS, DEPTH), F32),
            pltpu.SemaphoreType.DMA((3 * n_acts,)), pltpu.SemaphoreType.DMA((2, 48)),
            pltpu.SemaphoreType.DMA((3,)), pltpu.SemaphoreType.DMA((3,)),
        ],
        2 * 3 * UNITS * DEPTH * n * TOK,
        [ANY] * len(ins),
        (ANY,) * 3,
        ins,
        n * (4 << 20) + (16 << 20),
    )


def block(inputs, w_gate, w_up, w_down, d_out):
    fs = lax.axis_index("fs")

    def relative(v, fs=fs):
        parts = [v[:, i * DEPTH:(i + 1) * DEPTH] for i in range(4)]
        out = []
        for k in range(4):
            w = parts[k]
            for f in range(1, 4):
                w = jnp.where(fs == f, parts[f ^ k], w)
            out.append(w)
        return out

    mark = lax.optimization_barrier(fs) * 3 - 1
    mark = (mark + 1) // 3

    xp, dp = relative(inputs), relative(d_out)
    x_own, d_own = jnp.concatenate(xp, axis=1), jnp.concatenate(dp, axis=1)

    def spread(own, first, second, whole=False):
        own = own[None]
        one, two, three = (moved(own, **{first: d}) for d in (1, 2, 3))
        if whole:
            line = jnp.concatenate([own, one, two, three], axis=0)
            return (line, *(moved(line, **{second: d}) for d in (1, -1, 2)))
        low, high = jnp.concatenate([own, one], axis=0), jnp.concatenate([two, three], axis=0)
        up_l, up_h = moved(low, **{second: 1}), moved(high, **{second: 1})
        down_l, down_h = moved(low, **{second: -1}), moved(high, **{second: -1})
        far_l, far_h = moved(up_l, **{second: 1}), moved(down_h, **{second: -1})
        return low, high, up_l, up_h, down_l, down_h, far_l, far_h

    xs = spread(x_own, "dz", "dy")
    ds = spread(d_own, "dy", "dz")

    side = moved(jnp.stack([xp[1], dp[1], xp[3], dp[3]]), flip=1)
    far = jnp.stack([xp[0], side[0], dp[0], side[1]])
    near = jnp.stack([xp[2], side[2], dp[2], side[3]])
    got = (moved(near, dx=1), moved(near, dx=-1), moved(far, dx=2))
    xcs = spread(jnp.concatenate([v[:2] for v in got], axis=0), "dz", "dy", True)
    dcs = spread(jnp.concatenate([v[2:] for v in got], axis=0), "dy", "dz", True)

    wa = jnp.concatenate([w_gate.T, w_down[:CUT]], axis=0)
    wb = jnp.concatenate([w_up.T, w_down[CUT:]], axis=0)
    wa2, wb2 = moved(wa, dx=1), moved(wb, dx=-1)
    wa1, wb1 = moved(wa, flip=1), moved(wb, flip=1)
    wa3, wb3 = moved(wa2, flip=1), moved(wb2, flip=1)
    was, wbs = (wa, wa1, wa2, wa3), (wb, wb1, wb2, wb3)

    acts_l, acts_h, own, x_cols, d_cols = forward(xs, ds, was, wbs)

    aml, aph = moved(acts_l, dx=1), moved(acts_h, dx=-1)
    amh, apl = moved(acts_h, dx=1), moved(acts_l, dx=-1)
    side = moved(own, flip=1)
    oa, ob = moved(aml, dx=1), moved(aph, dx=-1)
    sml, sph = moved(aml, flip=1), moved(aph, flip=1)
    smh, spl = moved(amh, flip=1), moved(apl, flip=1)
    soa, sob = moved(oa, flip=1), moved(ob, flip=1)

    own_a, own_b, qa, qb = input_sums(own, was, wbs)
    qa, qb = qa.astype(F16), qb.astype(F16)
    got = [moved(qa[d - 1], dz=-d) for d in (1, 2, 3)] + [moved(qb[d - 1], dy=-d) for d in (1, 2, 3)]
    fa, fb = joined(own_a, own_b, [g.astype(F32) for g in got])
    fa = fa[0] + moved(fa[1], dy=-1) + moved(fa[2], dy=-2) + moved(fa[3], dy=-3)
    fb = fb[0] + moved(fb[1], dz=-1) + moved(fb[2], dz=-2) + moved(fb[3], dz=-3)
    total = jnp.concatenate([fa, fb], axis=1)
    grad_inputs = jnp.concatenate(relative(total.astype(BF), mark), axis=1)

    full = 3 * UNITS

    def halves(low, high):
        return [(low, LOW), (high, HIGH)]

    sums = weight_sums(
        [[(own, full)], [(side, full)]], near_columns, (x_cols, d_cols, side), None)
    sums = weight_sums(
        [halves(aml, amh), halves(sml, smh), halves(apl, aph), halves(spl, sph)],
        functools.partial(plane_columns, 0, 4), (*xcs, *dcs), sums)
    sums = weight_sums(
        [halves(oa, ob), halves(soa, sob)], functools.partial(plane_columns, 4, 2), (*xcs, *dcs), sums)
    return grad_inputs, sums[0].T, sums[1].T, sums[2]


def solution(mesh):
    tok = P(AXES, None)
    return jax.shard_map(
        block,
        mesh=mesh,
        in_specs=(tok, P("fs", "tp"), P("fs", "tp"), P("tp", "fs"), tok),
        out_specs=(tok, P("fs", "tp"), P("fs", "tp"), P("tp", "fs")),
        check_vma=False,
    )
```

```python
import functools

import jax
import jax.numpy as jnp
from jax import lax
from jax.experimental import pallas as pl
from jax.experimental.pallas import tpu as pltpu
from jax.sharding import PartitionSpec as P


AXES = ("rep", "fs", "tp")
BF, F32, F16 = jnp.bfloat16, jnp.float32, jnp.float16
W_MAX = 0.09375
ANY = pl.BlockSpec(memory_space=pl.ANY)
VMEM = pl.BlockSpec(memory_space=pltpu.VMEM)
LIMIT = 56 * 1024 * 1024

ROWS, DEPTH, UNITS = 32, 1024, 688
TOK, WIDE = 16 * ROWS, 4 * DEPTH
CUT = 336
LOW, HIGH = 1040, 1024
HALF = 2 * DEPTH
TAIL = 128


def index_of(x, c, z, y):
    x, z, y = x % 4, z % 4, y % 4
    return (x // 2) * 64 + ((x % 2) * 2 + c) * 16 + z * 4 + y


def moved(array, dx=0, flip=0, dz=0, dy=0):
    pairs = []
    for x in range(4):
        for c in range(2):
            for z in range(4):
                for y in range(4):
                    pairs.append((index_of(x + dx, c ^ flip, z + dz, y + dy), index_of(x, c, z, y)))
    return lax.ppermute(array, AXES, pairs)


def dot(a, b, ca, cb):
    return lax.dot_general(a, b, (((ca,), (cb,)), ((), ())), preferred_element_type=F32)


def place():
    tp = lax.axis_index("tp")
    return tp // 4, tp % 4


def call(name, body, out_shape, scratch, flops, ins, outs, args, nbytes):
    return pl.pallas_call(
        body,
        out_shape=out_shape,
        in_specs=ins,
        out_specs=outs,
        scratch_shapes=scratch,
        compiler_params=pltpu.CompilerParams(vmem_limit_bytes=LIMIT if name != "k_join" else 24 << 20),
        cost_estimate=pl.CostEstimate(flops=flops, bytes_accessed=nbytes, transcendentals=0),
    )(*args)


FROM = ((0, 0), (2, 0), (0, 1), (2, 1), (0, 3), (2, 3), (0, 2), (2, 2))
WHOLE = (0, 1, 3, 2)


def forward_kernel(*refs):
    xs, ds, was, wbs = refs[:8], refs[8:16], refs[16:20], refs[20:24]
    acts_l, acts_h, side, x_own, d_own = refs[24:29]
    v, w, sums, act, sx, sd, sw, so = refs[29:]
    z, y = place()
    x_copies, d_copies = [], []
    for i, (first, off) in enumerate(FROM):
        for j in range(2):
            row = pl.multiple_of((lax.rem(z + first + j, 4) * 4 + lax.rem(y + off, 4)) * ROWS, ROWS)
            x_copies.append(
                pltpu.make_async_copy(xs[i].at[j], v.at[0, pl.ds(row, ROWS)], sx.at[len(x_copies)]))
            row = pl.multiple_of((lax.rem(z + off, 4) * 4 + lax.rem(y + first + j, 4)) * ROWS, ROWS)
            d_copies.append(
                pltpu.make_async_copy(ds[i].at[j], v.at[1, pl.ds(row, ROWS)], sd.at[len(d_copies)]))
    rest = UNITS - CUT
    w_copies = [
        [
            pltpu.make_async_copy(was[k].at[pl.ds(0, UNITS)], w.at[k, 0], sw.at[4 * k]),
            pltpu.make_async_copy(wbs[k].at[pl.ds(0, UNITS)], w.at[k, 1], sw.at[4 * k + 1]),
            pltpu.make_async_copy(was[k].at[pl.ds(UNITS, CUT)], w.at[k, 2, pl.ds(0, CUT)], sw.at[4 * k + 2]),
            pltpu.make_async_copy(wbs[k].at[pl.ds(UNITS, rest)], w.at[k, 2, pl.ds(CUT, rest)], sw.at[4 * k + 3]),
        ]
        for k in range(4)
    ]
    stages = [x_copies + w_copies[0][:2], d_copies + w_copies[0][2:], w_copies[1], w_copies[2], w_copies[3]]

    def begin(n):
        for c in stages[n]:
            c.start()

    def end(n):
        for c in stages[n]:
            c.wait()

    begin(0)
    begin(1)
    sums[...] = jnp.zeros_like(sums)
    end(0)
    begin(2)

    outs = []
    for i, to in enumerate((x_own, d_own)):
        outs.append(pltpu.make_async_copy(v.at[i, :, pl.ds(0, DEPTH)], to, so.at[i]))
        for h in range(2):
            outs.append(pltpu.make_async_copy(
                v.at[i, :, pl.ds(DEPTH + h * TOK, TOK)],
                side.at[pl.ds(3 * UNITS + (2 * i + h) * TOK, TOK)], so.at[2 + 2 * i + h]))

    def product(n, _):
        k, i = n // 3, lax.rem(n, 3)

        @pl.when(n == 2)
        def _():
            end(1)
            begin(3)

        @pl.when(n == 3)
        def _():
            end(2)
            begin(4)

        @pl.when(n == 6)
        def _():
            end(3)

        @pl.when(n == 9)
        def _():
            end(4)
            for c in outs:
                c.start()

        sums[i] = sums[i] + dot(w[k, i], v[i // 2, :, pl.ds(pl.multiple_of(k * DEPTH, DEPTH), DEPTH)], 1, 1)
        return 0

    lax.fori_loop(0, 12, product, 0)

    def unit(i, _):
        r = pl.ds(pl.multiple_of(i * 16, 16), 16)
        g = sums[0, r, :].astype(BF).astype(F32)
        u = sums[1, r, :].astype(BF).astype(F32)
        b = sums[2, r, :].astype(BF).astype(F32)
        sigma = 1.0 / (1.0 + jnp.exp(-g))
        active = g * sigma
        act[r, :] = (b * u * sigma * (1.0 + g * (1.0 - sigma))).astype(BF)
        act[pl.ds(pl.multiple_of(UNITS + i * 16, 16), 16), :] = (b * active).astype(BF)
        act[pl.ds(pl.multiple_of(2 * UNITS + i * 16, 16), 16), :] = (active * u).astype(BF)
        return 0

    lax.fori_loop(0, UNITS // 16, unit, 0)
    outs.append(pltpu.make_async_copy(act.at[pl.ds(0, LOW)], acts_l, so.at[6]))
    outs.append(pltpu.make_async_copy(act.at[pl.ds(LOW, HIGH)], acts_h, so.at[7]))
    outs.append(pltpu.make_async_copy(act, side.at[pl.ds(0, 3 * UNITS)], so.at[8]))
    for c in outs[-3:]:
        c.start()
    for c in outs:
        c.wait()


def forward(xs, ds, was, wbs):
    shape = jax.ShapeDtypeStruct
    return call(
        "k_fwd",
        forward_kernel,
        (shape((LOW, TOK), BF), shape((HIGH, TOK), BF), shape((3 * UNITS + 4 * TOK, TOK), BF),
         shape((TOK, DEPTH), BF), shape((TOK, DEPTH), BF)),
        [
            pltpu.VMEM((2, TOK, WIDE), BF), pltpu.VMEM((4, 3, UNITS, DEPTH), BF), pltpu.VMEM((3, UNITS, TOK), F32),
            pltpu.VMEM((3 * UNITS, TOK), BF),
            pltpu.SemaphoreType.DMA((16,)), pltpu.SemaphoreType.DMA((16,)),
            pltpu.SemaphoreType.DMA((16,)), pltpu.SemaphoreType.DMA((9,)),
        ],
        2 * TOK * WIDE * UNITS * 3,
        [ANY] * 24,
        (ANY,) * 5,
        (*xs, *ds, *was, *wbs),
        34 << 20,
    )


def input_kernel(*refs):
    acts, was, wbs = refs[0], refs[1:5], refs[5:9]
    own, away = refs[9:11], refs[11:13]
    act, wa, wb, tg, tu, total, expo, sw, so, st, sl = refs[13:]
    z, y = place()
    load = pltpu.make_async_copy(acts.at[pl.ds(0, 2 * UNITS)], act, sl.at[0])
    load.start()
    copies = [
        (pltpu.make_async_copy(was[k].at[pl.ds(0, UNITS)], wa.at[k], sw.at[2 * k]),
         pltpu.make_async_copy(wbs[k].at[pl.ds(0, UNITS)], wb.at[k], sw.at[2 * k + 1]))
        for k in range(4)
    ]
    for pair in copies[:2]:
        for c in pair:
            c.start()
    load.wait()
    tg[...] = act[:UNITS, :].T
    tu[...] = act[UNITS:, :].T
    norm = jnp.sum(jnp.abs(tg[...].astype(F32)), axis=1, keepdims=True)
    norm = norm + jnp.sum(jnp.abs(tu[...].astype(F32)), axis=1, keepdims=True)
    e = jnp.ceil(jnp.log2(jnp.maximum(jnp.max(norm, axis=0, keepdims=True) * (1.02 * W_MAX), 1e-30)))
    expo[...] = jnp.broadcast_to(e, (TOK, TAIL))

    def puts(src, side, cols, sems):
        out = []
        for s in range(4):
            to = own[side] if s == 0 else away[side].at[s - 1]
            if side == 0:
                r = pl.ds(pl.multiple_of(lax.rem(z + s, 4) * (4 * ROWS), 4 * ROWS), 4 * ROWS)
                out.append(pltpu.make_async_copy(src.at[r], to.at[:, cols], sems.at[s]))
            else:
                for i in range(4):
                    r = pl.ds(pl.multiple_of((i * 4 + lax.rem(y + s, 4)) * ROWS, ROWS), ROWS)
                    out.append(pltpu.make_async_copy(src.at[r], to.at[pl.ds(i * ROWS, ROWS), cols], sems.at[4 * s + i]))
        return out

    tails = [c for side in range(2) for c in puts(expo, side, pl.ds(HALF, TAIL), st.at[side])]
    for c in tails:
        c.start()
    parts = [puts(total.at[k % 2], k // 2, pl.ds((k % 2) * DEPTH, DEPTH), so.at[k]) for k in range(4)]

    def part(k, _):
        for n in range(4):
            @pl.when(k == n)
            def _():
                for c in copies[n]:
                    c.wait()
                if n + 2 < 4:
                    for c in copies[n + 2]:
                        c.start()
                if n >= 2:
                    for c in parts[n - 2]:
                        c.wait()

        def tile(j, _):
            n = pl.ds(pl.multiple_of(j * 512, 512), 512)
            v = dot(tg[...], wa[k, :, n], 1, 0) + dot(tu[...], wb[k, :, n], 1, 0)
            total[lax.rem(k, 2), :, n] = v * jnp.exp2(14.0 - expo[:, :1])
            return 0

        lax.fori_loop(0, 2, tile, 0)
        for n in range(4):
            @pl.when(k == n)
            def _():
                for c in parts[n]:
                    c.start()
        return 0

    lax.fori_loop(0, 4, part, 0)
    for c in parts[2] + parts[3] + tails:
        c.wait()


def input_sums(acts, was, wbs):
    shape = jax.ShapeDtypeStruct
    own, away = shape((4 * ROWS, HALF + TAIL), F32), shape((3, 4 * ROWS, HALF + TAIL), F32)
    return call(
        "k_in",
        input_kernel,
        (own, own, away, away),
        [
            pltpu.VMEM((2 * UNITS, TOK), BF),
            pltpu.VMEM((4, UNITS, DEPTH), BF), pltpu.VMEM((4, UNITS, DEPTH), BF),
            pltpu.VMEM((TOK, UNITS), BF), pltpu.VMEM((TOK, UNITS), BF),
            pltpu.VMEM((2, TOK, DEPTH), F32), pltpu.VMEM((TOK, TAIL), F32),
            pltpu.SemaphoreType.DMA((8,)), pltpu.SemaphoreType.DMA((4, 16)), pltpu.SemaphoreType.DMA((2, 16)),
            pltpu.SemaphoreType.DMA((1,)),
        ],
        2 * TOK * WIDE * UNITS * 2,
        [ANY] * 9,
        (ANY,) * 4,
        (acts, *was, *wbs),
        22 << 20,
    )


def join_kernel(*refs):
    z, y = place()
    for side, at in ((0, y), (1, z)):
        own, got, out = refs[side], refs[2 + 3 * side:5 + 3 * side], refs[8 + 4 * side:12 + 4 * side]
        for s in range(4):
            r = pl.ds(pl.multiple_of(lax.rem(at + s, 4) * ROWS, ROWS), ROWS)
            v = own[r, :HALF] * jnp.exp2(own[r, HALF:HALF + 1] - 14.0)
            for g in got:
                v = v + g[r, :HALF] * jnp.exp2(g[r, HALF:HALF + 1] - 14.0)
            out[s][...] = v


def joined(own_a, own_b, got):
    out = jax.ShapeDtypeStruct((ROWS, HALF), F32)
    kept = call("k_join", join_kernel, (out,) * 8, [], 1 << 30, [VMEM] * 8, (VMEM,) * 8, (own_a, own_b, *got), 12 << 20)
    return kept[:4], kept[4:]


def weight_kernel(acts, n_acts, columns, has_base, n_in, *refs):
    ins, outs = refs[:n_in], refs[n_in:n_in + 3]
    a, cols, total, sa, sc, sb, so = refs[n_in + 3:]
    z, y = place()
    stages = [[], [], []]
    n = 0
    for g, pieces in enumerate(acts):
        for i, r0, r1 in pieces:
            for s in range(3):
                lo, hi = max(r0, s * UNITS), min(r1, (s + 1) * UNITS)
                if lo < hi:
                    stages[s].append(pltpu.make_async_copy(
                        ins[i].at[pl.ds(lo - r0, hi - lo)], a.at[pl.ds(lo, hi - lo), pl.ds(g * TOK, TOK)], sa.at[n]))
                    n += 1
    columns(ins[n_acts:], z, y, lambda src, to: stages[0].append(
        pltpu.make_async_copy(src, to, sc.at[0, len(stages[0])])), cols.at[0], 0)
    columns(ins[n_acts:], z, y, lambda src, to: stages[2].append(
        pltpu.make_async_copy(src, to, sc.at[1, len(stages[2])])), cols.at[1], 1)
    if has_base:
        for s in range(3):
            stages[s].append(pltpu.make_async_copy(ins[n_in - 3 + s], total.at[s], sb.at[s]))

    def begin(s):
        for c in stages[s]:
            c.start()

    begin(0)
    begin(1)
    done = [pltpu.make_async_copy(total.at[i], outs[i], so.at[i]) for i in range(3)]

    def product(i, _):
        for n in range(3):
            @pl.when(i == n)
            def _():
                if n:
                    done[n - 1].start()
                for c in stages[n]:
                    c.wait()
                if n == 0:
                    begin(2)

        rows = pl.ds(pl.multiple_of(i * UNITS, 16), UNITS)
        v = dot(a[rows, :], cols[i // 2].reshape(len(acts) * TOK, DEPTH), 1, 0)
        total[i] = total[i] + v if has_base else v
        return 0

    lax.fori_loop(0, 3, product, 0)
    done[2].start()
    for c in done:
        c.wait()


def near_columns(refs, z, y, add, buf, kind):
    x_own, d_own, side = refs[:3]
    add(d_own if kind else x_own, buf.at[0])
    for h in range(2):
        add(side.at[pl.ds(3 * UNITS + (2 * kind + h) * TOK, TOK)], buf.at[1, :, pl.ds(h * TOK, TOK)])


def plane_columns(first_group, count, refs, z, y, add, buf, kind):
    for i, off in enumerate(WHOLE):
        for j in range(4):
            a, b = lax.rem(z + j, 4), lax.rem(y + off, 4)
            if kind:
                a, b = lax.rem(z + off, 4), lax.rem(y + j, 4)
            add(refs[4 * kind + i].at[j, pl.ds(first_group, count)], buf.at[:, a * 4 + b])


def weight_sums(name, groups, columns, arrays, base):
    ins, acts = [], []
    for pieces in groups:
        row, marks = 0, []
        for p, m in pieces:
            marks.append((len(ins), row, row + m))
            ins.append(p)
            row += m
        acts.append(marks)
    n_acts = len(ins)
    ins += list(arrays) + list(base or [])
    n = len(groups)
    col = (2, n, TOK, DEPTH) if columns is near_columns else (2, n, 16, ROWS, DEPTH)
    out = jax.ShapeDtypeStruct((UNITS, DEPTH), F32)
    return call(
        name,
        functools.partial(weight_kernel, acts, n_acts, columns, base is not None, len(ins)),
        (out,) * 3,
        [
            pltpu.VMEM((3 * UNITS, n * TOK), BF), pltpu.VMEM(col, BF),
            pltpu.VMEM((3, UNITS, DEPTH), F32),
            pltpu.SemaphoreType.DMA((3 * n_acts,)), pltpu.SemaphoreType.DMA((2, 48)),
            pltpu.SemaphoreType.DMA((3,)), pltpu.SemaphoreType.DMA((3,)),
        ],
        2 * 3 * UNITS * DEPTH * n * TOK,
        [ANY] * len(ins),
        (ANY,) * 3,
        ins,
        n * (4 << 20) + (16 << 20),
    )


def block(inputs, w_gate, w_up, w_down, d_out):
    fs = lax.axis_index("fs")

    def relative(v, fs=fs):
        parts = [v[:, i * DEPTH:(i + 1) * DEPTH] for i in range(4)]
        out = []
        for k in range(4):
            w = parts[k]
            for f in range(1, 4):
                w = jnp.where(fs == f, parts[f ^ k], w)
            out.append(w)
        return out

    mark = lax.optimization_barrier(fs) * 3 - 1
    mark = (mark + 1) // 3

    xp, dp = relative(inputs), relative(d_out)
    x_own, d_own = jnp.concatenate(xp, axis=1), jnp.concatenate(dp, axis=1)

    def spread(own, first, second, whole=False):
        own = own[None]
        one, two, three = (moved(own, **{first: d}) for d in (1, 2, 3))
        if whole:
            line = jnp.concatenate([own, one, two, three], axis=0)
            return (line, *(moved(line, **{second: d}) for d in (1, -1, 2)))
        low, high = jnp.concatenate([own, one], axis=0), jnp.concatenate([two, three], axis=0)
        up_l, up_h = moved(low, **{second: 1}), moved(high, **{second: 1})
        down_l, down_h = moved(low, **{second: -1}), moved(high, **{second: -1})
        far_l, far_h = moved(up_l, **{second: 1}), moved(down_h, **{second: -1})
        return low, high, up_l, up_h, down_l, down_h, far_l, far_h

    xs = spread(x_own, "dz", "dy")
    ds = spread(d_own, "dy", "dz")

    side = moved(jnp.stack([xp[1], dp[1], xp[3], dp[3]]), flip=1)
    far = jnp.stack([xp[0], side[0], dp[0], side[1]])
    near = jnp.stack([xp[2], side[2], dp[2], side[3]])
    got = (moved(near, dx=1), moved(near, dx=-1), moved(far, dx=2))
    xcs = spread(jnp.concatenate([v[:2] for v in got], axis=0), "dz", "dy", True)
    dcs = spread(jnp.concatenate([v[2:] for v in got], axis=0), "dy", "dz", True)

    wa = jnp.concatenate([w_gate.T, w_down[:CUT]], axis=0)
    wb = jnp.concatenate([w_up.T, w_down[CUT:]], axis=0)
    wa2, wb2 = moved(wa, dx=1), moved(wb, dx=-1)
    wa1, wb1 = moved(wa, flip=1), moved(wb, flip=1)
    wa3, wb3 = moved(wa2, flip=1), moved(wb2, flip=1)
    was, wbs = (wa, wa1, wa2, wa3), (wb, wb1, wb2, wb3)

    acts_l, acts_h, own, x_cols, d_cols = forward(xs, ds, was, wbs)

    aml, aph = moved(acts_l, dx=1), moved(acts_h, dx=-1)
    amh, apl = moved(acts_h, dx=1), moved(acts_l, dx=-1)
    side = moved(own, flip=1)
    oa, ob = moved(aml, dx=1), moved(aph, dx=-1)
    sml, sph = moved(aml, flip=1), moved(aph, flip=1)
    smh, spl = moved(amh, flip=1), moved(apl, flip=1)
    soa, sob = moved(oa, flip=1), moved(ob, flip=1)

    own_a, own_b, qa, qb = input_sums(own, was, wbs)
    qa, qb = qa.astype(F16), qb.astype(F16)
    got = [moved(qa[d - 1], dz=-d) for d in (1, 2, 3)] + [moved(qb[d - 1], dy=-d) for d in (1, 2, 3)]
    fa, fb = joined(own_a, own_b, [g.astype(F32) for g in got])
    fa = fa[0] + moved(fa[1], dy=-1) + moved(fa[2], dy=-2) + moved(fa[3], dy=-3)
    fb = fb[0] + moved(fb[1], dz=-1) + moved(fb[2], dz=-2) + moved(fb[3], dz=-3)
    total = jnp.concatenate([fa, fb], axis=1)
    grad_inputs = jnp.concatenate(relative(total.astype(BF), mark), axis=1)

    full = 3 * UNITS

    def halves(low, high):
        return [(low, LOW), (high, HIGH)]

    sums = weight_sums(
        "k_near", [[(own, full)], [(side, full)]], near_columns, (x_cols, d_cols, side), None)
    sums = weight_sums(
        "k_mid", [halves(aml, amh), halves(sml, smh), halves(apl, aph), halves(spl, sph)],
        functools.partial(plane_columns, 0, 4), (*xcs, *dcs), sums)
    sums = weight_sums(
        "k_far", [halves(oa, ob), halves(soa, sob)], functools.partial(plane_columns, 4, 2), (*xcs, *dcs), sums)
    return grad_inputs, sums[0].T, sums[1].T, sums[2]


def solution(mesh):
    tok = P(AXES, None)
    return jax.shard_map(
        block,
        mesh=mesh,
        in_specs=(tok, P("fs", "tp"), P("fs", "tp"), P("tp", "fs"), tok),
        out_specs=(tok, P("fs", "tp"), P("fs", "tp"), P("tp", "fs")),
        check_vma=False,
    )
```
